512 devices in a mesh: rep: 2 (over z_hi), fs: 32 (over z_lo, y), tp: 8 (over x, core).
Axes of the slice: x: 4, y: 4, z: 16 (z_hi: 2, z_lo: 8; z = z_hi * 8 + z_lo), core: 2. Of those that a mesh axis runs over, the one named last changes fastest.
Arguments:
- inputs: bfloat16 [2, 12288, 2048], P('rep', 'fs', 'tp'), may hold values from -6 to 6
- gate_proj: bfloat16 [2048, 2816], P('fs', 'tp'), may hold values from -0.125 to 0.125
- value_proj: bfloat16 [2048, 2816], P('fs', 'tp'), may hold values from -0.125 to 0.125
- gate_taps: float32 [3, 2816], replicated, may hold values from -3 to 3
- value_taps: float32 [3, 2816], replicated, may hold values from -3 to 3
- out_grad: bfloat16 [2, 12288, 2816], P('rep', 'fs', 'tp'), may hold values from -6 to 6
Outputs:
- in_grad: bfloat16 [2, 12288, 2048], P('rep', 'fs', 'tp')
- gate_proj_grad: float32 [2048, 2816], P('fs', 'tp')
- value_proj_grad: float32 [2048, 2816], P('fs', 'tp')
- gate_taps_grad: float32 [3, 2816], replicated
- value_taps_grad: float32 [3, 2816], replicated
The draws below stay inside these ranges and needn't reach their ends.
All inputs are finite; a program needn't handle non-finite values.
Results may differ from the reference program's by a relative error of at most 0.013.
Values may be sent and summed in bfloat16 or wider, within the bound.
A program may use at most 64 MiB of HBM per device.

```python
import jax
import jax.numpy as jnp
from jax import lax

D = 2048
FF = 2816
CONV = 3
HID_DEV = 352
BATCH = 2
SEQ = 12288
ALL_TOKENS = 24576


def raised(drawn, rng, source, target, shards_of, factor):
    owner, partner = [(jnp.arange(drawn.shape[axis_at]) // (drawn.shape[axis_at] // shards_of)).reshape([-1 if axis == axis_at else 1 for axis in range(drawn.ndim)]) for axis_at in (source, target)]
    chosen = jax.random.permutation(rng, shards_of)[partner]
    strong = (owner == chosen) | (owner == (partner + shards_of // 2) % shards_of)
    return jnp.where(strong, factor * drawn, drawn)


def block_scale(stream_key, extent, shards, least, largest):
    def one(position, blocks):
        draws = jax.random.uniform(jax.random.fold_in(jax.random.fold_in(stream_key, 6), position), (blocks,), jnp.float32, least / len(shards), largest / len(shards))
        return jnp.repeat(jnp.exp(draws), extent[position] // blocks).reshape((-1,) + (1,) * (len(extent) - position - 1))

    factor_of = one(*shards[0])
    for cut in shards[1:]:
        factor_of = factor_of * one(*cut)
    return factor_of


def centred(stream_key, extent, deviation, limit, split=(), kind=jnp.bfloat16):
    level = block_scale(stream_key, extent, split, -0.22, 0.18) if split else 1.0
    result = jax.random.normal(stream_key, extent, jnp.float32) * deviation * level
    return jnp.minimum(jnp.maximum(result, -limit), limit).astype(kind)


def bell_draw_with(key, dims, deviation, bound, split, heavy, kind=jnp.bfloat16):
    array = deviation * jax.random.normal(key, dims, jnp.float32)
    if split:
        array = array * block_scale(key, dims, split, -0.22, 0.18)
    return jnp.clip(raised(array, jax.random.fold_in(key, 3), *heavy), -bound, bound).astype(kind)


def setup_inputs(seed: int = 0) -> dict:
    arg_keys = jax.random.split(jax.random.key(seed), 7)
    inputs = bell_draw_with(arg_keys[0], (BATCH, SEQ, D), 1.0, 6.0, ((0, 2), (1, 32), (2, 8)), (1, 2, 32, 2.75))
    gate_proj = centred(arg_keys[1], (D, FF), D ** -0.5, 0.125, ((0, 32), (1, 8)))
    value_proj = centred(arg_keys[2], (D, FF), D ** -0.5, 0.125, ((0, 32), (1, 8)))
    gate_taps = centred(arg_keys[3], (CONV, FF), 0.577, 3.0, (), jnp.float32)
    value_taps = centred(arg_keys[4], (CONV, FF), 0.577, 3.0, (), jnp.float32)
    out_grad = bell_draw_with(arg_keys[5], (BATCH, SEQ, FF), 1.0, 6.0, ((0, 2), (1, 32), (2, 8)), (1, 2, 32, 2.75))
    return dict(inputs=inputs, gate_proj=gate_proj, value_proj=value_proj, gate_taps=gate_taps, value_taps=value_taps, out_grad=out_grad)


def conv_fwd(pre_acts, taps):
    seq_len = pre_acts.shape[0]
    padded = jnp.pad(pre_acts, ((1, 1), (0, 0)))
    return taps[0] * padded[0:seq_len] + taps[1] * padded[1:seq_len + 1] + taps[2] * padded[2:seq_len + 2]


def conv_back(cot_rows, taps):
    seq_len = cot_rows.shape[0]
    padded = jnp.pad(cot_rows, ((1, 1), (0, 0)))
    return taps[0] * padded[2:seq_len + 2] + taps[1] * padded[1:seq_len + 1] + taps[2] * padded[0:seq_len]


def cotangents(gate_mix, value_mix, cot_in):
    sigmoid_gate = jax.nn.sigmoid(gate_mix)
    gate_cot = cot_in * value_mix * (sigmoid_gate * (1.0 + gate_mix * (1.0 - sigmoid_gate)))
    value_cot = cot_in * (gate_mix * sigmoid_gate)
    return gate_cot, value_cot


def reference(inputs, gate_proj, value_proj, gate_taps, value_taps, out_grad):
    contract_cols = (((1,), (1,)), ((), ()))
    contract_rows = (((0,), (0,)), ((), ()))

    def one_sequence(pair):
        seq_inputs, seq_cot = pair
        seq_len = seq_inputs.shape[0]
        gate_pre = jnp.dot(seq_inputs, gate_proj, preferred_element_type=jnp.float32).astype(jnp.bfloat16)
        value_pre = jnp.dot(seq_inputs, value_proj, preferred_element_type=jnp.float32).astype(jnp.bfloat16)
        gate_mix = conv_fwd(gate_pre.astype(jnp.float32), gate_taps)
        value_mix = conv_fwd(value_pre.astype(jnp.float32), value_taps)
        gate_cot, value_cot = cotangents(gate_mix, value_mix, seq_cot.astype(jnp.float32))
        gate_pre_cot = conv_back(gate_cot, gate_taps).astype(jnp.bfloat16)
        value_pre_cot = conv_back(value_cot, value_taps).astype(jnp.bfloat16)

        def add_block(total, block_index):
            first_col = (block_index * HID_DEV).astype(jnp.int32)
            gate_cols = lax.dynamic_slice_in_dim(gate_pre_cot, first_col, HID_DEV, 1)
            value_cols = lax.dynamic_slice_in_dim(value_pre_cot, first_col, HID_DEV, 1)
            gate_block = lax.dynamic_slice_in_dim(gate_proj, first_col, HID_DEV, 1)
            value_block = lax.dynamic_slice_in_dim(value_proj, first_col, HID_DEV, 1)
            partial_value = lax.dot_general(gate_cols, gate_block, contract_cols, preferred_element_type=jnp.float32)
            partial_value = partial_value + lax.dot_general(value_cols, value_block, contract_cols, preferred_element_type=jnp.float32)
            rounded = lax.optimization_barrier(partial_value.astype(jnp.bfloat16))
            return total + rounded.astype(jnp.float32), None

        in_sum, _ = lax.scan(add_block, jnp.zeros((seq_len, D), jnp.float32), jnp.arange(FF // HID_DEV).astype(jnp.int32))
        in_grad = in_sum.astype(jnp.bfloat16)
        gate_grad = lax.dot_general(seq_inputs, gate_pre_cot, contract_rows, preferred_element_type=jnp.float32)
        value_grad = lax.dot_general(seq_inputs, value_pre_cot, contract_rows, preferred_element_type=jnp.float32)
        gate_padded = jnp.pad(gate_pre.astype(jnp.float32), ((1, 1), (0, 0)))
        value_padded = jnp.pad(value_pre.astype(jnp.float32), ((1, 1), (0, 0)))
        gate_tgrad = jnp.stack([jnp.sum(gate_padded[offset:offset + seq_len] * gate_cot, axis=0) for offset in range(3)])
        value_tgrad = jnp.stack([jnp.sum(value_padded[offset:offset + seq_len] * value_cot, axis=0) for offset in range(3)])
        return in_grad, gate_grad, value_grad, gate_tgrad, value_tgrad

    results = lax.map(one_sequence, (inputs, out_grad))
    factor = float(ALL_TOKENS) ** -0.5
    return (results[0], jnp.sum(results[1], axis=0) * factor, jnp.sum(results[2], axis=0) * factor,
            jnp.sum(results[3], axis=0) * factor, jnp.sum(results[4], axis=0) * factor)
```

```python
import functools

import jax
import jax.numpy as jnp
from jax import lax
from jax.experimental import pallas as pl
from jax.experimental.pallas import tpu as pltpu
from jax.sharding import PartitionSpec as P

MESH = pl.DeviceIdType.MESH
BF16 = jnp.bfloat16
F32 = jnp.float32

NX, NC, NY, NZ = 4, 2, 4, 16
ZL = 8
TOK = 384
COLS = 352
FEAT = 256
EDGE = 16
EXT = TOK + 2 * EDGE


def right_reach(r):
    return 4 if r < 2 else 3


class Wires:
    def __init__(self, send_sems, recv_sems):
        self.send_sems, self.recv_sems = send_sems, recv_sems
        self.index = {}
        self.sent = []

    def at(self, key):
        return self.index.setdefault(key, len(self.index))

    def send(self, key, src, dst, to):
        i = self.at(key)
        copy = pltpu.make_async_remote_copy(
            src_ref=src,
            dst_ref=dst,
            send_sem=self.send_sems.at[i],
            recv_sem=self.recv_sems.at[i],
            device_id=to,
            device_id_type=MESH,
        )
        copy.start()
        self.sent.append(copy)

    def wait(self, key, dst, to):
        i = self.at(key)
        pltpu.make_async_remote_copy(
            src_ref=dst,
            dst_ref=dst,
            send_sem=self.send_sems.at[i],
            recv_sem=self.recv_sems.at[i],
            device_id=to,
            device_id_type=MESH,
        ).wait_recv()

    def drain(self):
        for copy in self.sent:
            copy.wait_send()


def kernel(
    factor,
    x_hbm, wg_hbm, wv_hbm, ogt_hbm, taps_ref,
    din_ref, dg_ref, dv_ref, tout_ref,
    X, WG, WV, OGT, OG, PG, PV, KG, KV, CG, CV, GG, GV,
    FARG, FARV, DIRG, DIRV, MIDG, MIDV, ENDG, ENDV, RG, RV,
    ZRG, ZLG, ZRV, ZLV, TRG, TLG, TRV, TLV,
    IP, IR, IS, ISR, TY, TZ1, TB, TT,
    send_sems, recv_sems, local_sems,
):
    rep, fs, tp = lax.axis_index("rep"), lax.axis_index("fs"), lax.axis_index("tp")
    zl, y = lax.div(fs, NY), lax.rem(fs, NY)
    x, c = lax.div(tp, NC), lax.rem(tp, NC)
    zg = rep * ZL + zl

    def dev(x=x, c=c, y=y, z=zg):
        z = lax.rem(z + NZ, NZ)
        return (
            lax.div(z, ZL),
            lax.rem(z, ZL) * NY + lax.rem(y + NY, NY),
            lax.rem(x + NX, NX) * NC + c,
        )

    def blk(dz, dy):
        return lax.rem(zl + dz + ZL, ZL) * NY + lax.rem(y + dy + NY, NY)

    def zrow(dz):
        return lax.rem(zl + dz + 2 * ZL, ZL)

    me = dev()
    right, left = dev(z=zg + 1), dev(z=zg - 1)
    up, down = dev(y=y + 1), dev(y=y - 1)
    partner = dev(c=1 - c)
    after_z = zg + lax.div(y + 1, NY)
    after = dev(y=y + 1, z=after_z)
    before_z = zg - 1 + lax.div(y + NY - 1, NY)
    before = dev(y=y - 1, z=before_z)

    def tp_peer(k):
        return (rep, fs, lax.rem(tp + k + 8, 8))

    zq, zo = lax.div(zg, 4), lax.rem(zg, 4)
    side = 4 * (1 - 2 * lax.rem(zq, 2))

    def z_near(k):
        return dev(z=zq * 4 + lax.rem(zo + k, 4))

    own = blk(0, 0)
    loads = [
        pltpu.make_async_copy(wg_hbm, WG.at[own], local_sems.at[0]),
        pltpu.make_async_copy(wv_hbm, WV.at[own], local_sems.at[1]),
        pltpu.make_async_copy(x_hbm, X.at[tp, pl.ds(EDGE, TOK)], local_sems.at[2]),
        pltpu.make_async_copy(ogt_hbm, OGT.at[pl.ds(0, COLS)], local_sems.at[3]),
    ]
    for load in loads:
        load.start()

    barrier = pltpu.get_barrier_semaphore()
    peers = [tp_peer(k) for k in range(1, 8)]
    peers += [dev(y=y + k) for k in (1, 2, 3)]
    peers += [right, left, after, before]
    peers += [z_near(k) for k in (1, 2, 3)]
    peers += [dev(z=zg + 4), dev(z=zg - 4)]
    for peer in peers:
        pl.semaphore_signal(barrier, inc=1, device_id=peer, device_id_type=MESH)
    pl.semaphore_wait(barrier, len(peers))

    w = Wires(send_sems, recv_sems)

    loads[0].wait()
    for dy in (1, 3, 2):
        w.send(("gy", dy), WG.at[own], WG.at[own], dev(y=y + dy))
    loads[1].wait()
    w.send(("vz", 1, 1), WV.at[own], WV.at[own], right)
    w.send(("vz", -1, 1), WV.at[own], WV.at[own], left)
    w.send(("gz", 0, 1, 1), WG.at[own], WG.at[own], right)
    w.send(("gz", 0, -1, 1), WG.at[own], WG.at[own], left)
    loads[2].wait()
    mine = X.at[tp, pl.ds(EDGE, TOK)]
    for dx in (1, 3, 2):
        w.send(("x", dx), mine, mine, dev(x=x + dx))
    w.send(("xp", 0), mine, mine, partner)
    head, tail = X.at[tp, pl.ds(EDGE, EDGE)], X.at[tp, pl.ds(TOK, EDGE)]
    lo, hi = pl.ds(0, EDGE), pl.ds(TOK + EDGE, EDGE)
    w.send(("hx", 1), tail, X.at[tp, lo], after)
    w.send(("hx", -1), head, X.at[tp, hi], before)
    w.send(("vy", 0, 1), WV.at[own], WV.at[own], up)
    w.send(("vy", 0, -1), WV.at[own], WV.at[own], down)

    for r in (3, 1, 2):
        unit = WG.at[blk(0, r)]
        w.wait(("gy", 4 - r), unit, me)
        w.send(("gz", r, 1, 1), unit, unit, right)
        w.send(("gz", r, -1, 1), unit, unit, left)

    def out_grad_rows():
        loads[3].wait()
        for i in range(3):
            for j in range(3):
                block = OGT[128 * i : 128 * i + 128, 128 * j : 128 * j + 128].astype(F32)
                cols = min(128, COLS - 128 * i)
                OG[EDGE + 128 * j : EDGE + 128 * j + 128, 128 * i : 128 * i + cols] = (
                    block.T[:, :cols].astype(BF16)
                )

    def gate_chunk(z, first=False):
        part = jnp.dot(
            X[z],
            WG[pl.ds(z * NY, NY)].reshape(FEAT, COLS),
            preferred_element_type=F32,
        )
        if first:
            PG[8 : 8 + EXT] = part
        else:
            PG[8 : 8 + EXT] += part

    def value_chunk(z, first=False):
        part = jnp.dot(
            X[z],
            WV[pl.ds(z * NY, NY)].reshape(FEAT, COLS),
            preferred_element_type=F32,
        )
        if first:
            PV[8 : 8 + EXT] = part
        else:
            PV[8 : 8 + EXT] += part

    def x_arrived(dx):
        slot = X.at[lax.rem(x - dx + NX, NX) * NC + c, pl.ds(EDGE, TOK)]
        w.wait(("x", dx), slot, me)
        w.send(("xp", dx), slot, slot, partner)

    def xp_arrived(dx):
        slot = X.at[lax.rem(x - dx + NX, NX) * NC + 1 - c, pl.ds(EDGE, TOK)]
        w.wait(("xp", dx), slot, me)

    def value_row_sent(dz):
        unit = WV.at[blk(dz, 0)]
        w.send(("vy", dz, 1), unit, unit, up)
        w.send(("vy", dz, -1), unit, unit, down)

    def value_row_arrived(dz):
        from_down, from_up = WV.at[blk(dz, -1)], WV.at[blk(dz, 1)]
        w.wait(("vy", dz, 1), from_down, me)
        if dz % 2 == 0:
            w.send(("vf", dz), from_down, from_down, up)
        w.wait(("vy", dz, -1), from_up, me)
        if dz % 2 == 1:
            w.send(("vf", dz), from_up, from_up, down)

    def value_row_done(dz):
        w.wait(("vf", dz), WV.at[blk(dz, 2)], me)

    rows_sent = [[0]]
    for d in range(1, 5):
        sent = []
        for way, reach, to in ((1, 4, right), (-1, 3, left)):
            if d <= reach:
                unit = WV.at[blk(-way * d, 0)]
                w.wait(("vz", way, d), unit, me)
                if d < reach:
                    w.send(("vz", way, d + 1), unit, unit, to)
                value_row_sent(-way * d)
                sent.append(-way * d)
        for r in (0, 3, 1, 2):
            for way, reach, to in ((1, right_reach(r), right), (-1, 7 - right_reach(r), left)):
                if d <= reach:
                    unit = WG.at[blk(-way * d, r)]
                    w.wait(("gz", r, way, d), unit, me)
                    if d < reach:
                        w.send(("gz", r, way, d + 1), unit, unit, to)
        for dz in rows_sent[-1]:
            value_row_arrived(dz)
        rows_sent.append(sent)
        if d == 1:
            w.wait(("hx", 1), X.at[tp, lo], me)
            w.wait(("hx", -1), X.at[tp, hi], me)
            for k in range(1, 8):
                w.send(("hl", k), X.at[tp, lo], X.at[tp, lo], tp_peer(k))
                w.send(("hr", k), X.at[tp, hi], X.at[tp, hi], tp_peer(k))
            x_arrived(1)
            x_arrived(3)
            out_grad_rows()
        if d == 2:
            w.send(("og", 1), OG.at[pl.ds(TOK, EDGE)], OG.at[lo], after)
            w.send(("og", -1), OG.at[pl.ds(EDGE, EDGE)], OG.at[hi], before)
            x_arrived(2)
            for dx in (0, 1, 3, 2):
                xp_arrived(dx)
            for k in range(1, 8):
                t = lax.rem(tp - k + 8, 8)
                w.wait(("hl", k), X.at[t, lo], me)
                w.wait(("hr", k), X.at[t, hi], me)
            gate_chunk(zrow(0), first=True)
            gate_chunk(zrow(1))
            gate_chunk(zrow(-1))
        if d == 3:
            gate_chunk(zrow(2))
            gate_chunk(zrow(-2))
            for dz in rows_sent[0] + rows_sent[1]:
                value_row_done(dz)
            value_chunk(zrow(0), first=True)
            value_chunk(zrow(1))
            value_chunk(zrow(-1))
    for dz in rows_sent[-1]:
        value_row_arrived(dz)
    gate_chunk(zrow(3))
    gate_chunk(zrow(-3))
    gate_chunk(zrow(4))
    for dz in rows_sent[2] + rows_sent[3] + rows_sent[4]:
        value_row_done(dz)
        value_chunk(zrow(dz))
    w.wait(("og", 1), OG.at[lo], me)
    w.wait(("og", -1), OG.at[hi], me)

    not_first, not_last = fs > 0, fs < NY * ZL - 1
    for ref in (PG, PV):
        ref[8 : 8 + EDGE] = jnp.where(not_first, ref[8 : 8 + EDGE], 0.0)
        ref[8 + EDGE + TOK : 8 + EXT] = jnp.where(not_last, ref[8 + EDGE + TOK : 8 + EXT], 0.0)
    OG[:EDGE] = jnp.where(not_first, OG[:EDGE].astype(F32), 0.0).astype(BF16)
    OG[EDGE + TOK :] = jnp.where(not_last, OG[EDGE + TOK :].astype(F32), 0.0).astype(BF16)

    g0, g1, g2 = (taps_ref[0, k : k + 1, :] for k in range(3))
    v0, v1, v2 = (taps_ref[1, k : k + 1, :] for k in range(3))

    def rounded(value):
        return value.astype(BF16).astype(F32)

    def cot_rows(i):
        base = pl.multiple_of(i * 16, 16)
        gate = rounded(PG[pl.ds(base, 32)])
        value = rounded(PV[pl.ds(base, 32)])
        gm, gz, gp = gate[7:23], gate[8:24], gate[9:25]
        vm, vz, vp = value[7:23], value[8:24], value[9:25]
        gate_mix = g0 * gm + g1 * gz + g2 * gp
        value_mix = v0 * vm + v1 * vz + v2 * vp
        grad = OG[pl.ds(base, 16)].astype(F32)
        s = jax.nn.sigmoid(gate_mix)
        gate_cot = grad * value_mix * (s * (1.0 + gate_mix * (1.0 - s)))
        value_cot = grad * (gate_mix * s)
        KG[pl.ds(base + 8, 16)] = gate_cot
        KV[pl.ds(base + 8, 16)] = value_cot
        return [
            (p * k).reshape(2, 8, COLS).sum(axis=0)
            for p, k in (
                (gm, gate_cot), (gz, gate_cot), (gp, gate_cot),
                (vm, value_cot), (vz, value_cot), (vp, value_cot),
            )
        ]

    cot_rows(0)
    cot_rows(TOK // 16 + 1)
    zero = jnp.zeros((8, COLS), F32)
    tap_sums = lax.fori_loop(
        1, TOK // 16 + 1,
        lambda i, sums: tuple(a + b for a, b in zip(sums, cot_rows(i))),
        (zero,) * 6,
    )

    def back_rows(i, carry):
        base = pl.multiple_of(i * 16, 16)
        out = pl.ds(pl.multiple_of(i * 16 - 16, 16), 16)
        for source, target, (t0, t1, t2) in ((KG, CG, (g0, g1, g2)), (KV, CV, (v0, v1, v2))):
            cot = source[pl.ds(base, 32)]
            target[out] = (t0 * cot[9:25] + t1 * cot[8:24] + t2 * cot[7:23]).astype(BF16)
        return carry

    lax.fori_loop(1, TOK // 16 + 1, back_rows, 0)

    rows = [jnp.sum(part, axis=0, keepdims=True) for part in tap_sums]
    TY[y] = jnp.concatenate(rows + [jnp.zeros((2, COLS), F32)], axis=0)

    order = (0, 1, -1, 2, -2, 3, -3, 4)
    place = {dz % ZL: k for k, dz in enumerate(order)}

    def make_blocks(k):
        z = zrow(order[k])
        acts = X[z, EDGE : EDGE + TOK, :]
        for cot, terms in ((CG, GG), (CV, GV)):
            block = lax.dot_general(
                acts, cot[...], (((0,), (0,)), ((), ())), preferred_element_type=F32
            )
            terms[pl.ds(z * NY, NY)] = block.astype(BF16).reshape(NY, 64, COLS)
        dz = order[k]
        w.send(("far_g", k), GG.at[blk(dz, 2)], FARG.at[k], up)
        w.send(("far_v", k), GV.at[blk(dz, 2)], FARV.at[k], down)
        w.send(("dir_g", k), GG.at[blk(dz, -1)], DIRG.at[k], down)
        w.send(("dir_v", k), GV.at[blk(dz, 1)], DIRV.at[k], up)

    def total(*parts):
        acc = parts[0].astype(F32)
        for part in parts[1:]:
            acc = acc + part.astype(F32)
        return acc

    def pass_on(k):
        dz = order[k]
        w.wait(("far_g", k), FARG.at[k], me)
        MIDG[k] = total(FARG[k], GG[blk(dz, 1)]).astype(BF16)
        w.send(("mid_g", k), MIDG.at[k], ENDG.at[k], up)
        w.wait(("far_v", k), FARV.at[k], me)
        MIDV[k] = total(FARV[k], GV[blk(dz, -1)]).astype(BF16)
        w.send(("mid_v", k), MIDV.at[k], ENDV.at[k], down)

    def row_done(k):
        own = blk(order[k], 0)
        w.wait(("dir_g", k), DIRG.at[k], me)
        w.wait(("mid_g", k), ENDG.at[k], me)
        RG[k] = total(GG[own], DIRG[k], ENDG[k]).astype(BF16)
        w.wait(("dir_v", k), DIRV.at[k], me)
        w.wait(("mid_v", k), ENDV.at[k], me)
        RV[k] = total(GV[own], DIRV[k], ENDV[k]).astype(BF16)

    chains = {
        "gr": (RG, ZRG, TRG, -1, 0, 8, right),
        "gl": (RG, ZLG, TLG, 1, 1, 7, left),
        "vr": (RV, ZRV, TRV, -1, 1, 7, right),
        "vl": (RV, ZLV, TLV, 1, 0, 8, left),
    }

    def hop(name, s):
        terms, landing, sums, way, start, length, to = chains[name]
        k = place[(way * (start + s)) % ZL]
        if s == 0:
            w.send((name, 0), terms.at[k], landing.at[0], to)
            return
        w.wait((name, s - 1), landing.at[s - 1], me)
        sums[s] = total(landing[s - 1], terms[k]).astype(BF16)
        w.send((name, s), sums.at[s], landing.at[s], to)

    hops = {
        0: [("gr", 0), ("vl", 0)],
        1: [("gl", 0), ("vl", 1)],
        2: [("gr", 1), ("vr", 0)],
        3: [("gl", 1), ("vl", 2)],
        4: [("gr", 2), ("vr", 1)],
        5: [("gl", 2), ("vl", 3)],
        6: [("gr", 3), ("vr", 2)],
        7: [("gr", 4), ("gl", 3), ("vl", 4), ("vr", 3)],
    }

    def input_terms(j):
        part = lax.dot_general(
            CG[...], WG[NY * j : NY * j + NY].reshape(FEAT, COLS),
            (((1,), (1,)), ((), ())), preferred_element_type=F32,
        ) + lax.dot_general(
            CV[...], WV[NY * j : NY * j + NY].reshape(FEAT, COLS),
            (((1,), (1,)), ((), ())), preferred_element_type=F32,
        )
        IP[j % 2, j // 2] = part.astype(BF16)

    def input_swap():
        for i in range(NX):
            w.send(("ip", i), IP.at[1 - c, i], IR.at[i], partner)

    def input_sums():
        for i in range(NX):
            w.wait(("ip", i), IR.at[i], me)
            IS[i] = total(IP[c, i], IR[i]).astype(BF16)
        for dx in (1, 3, 2):
            w.send(("is", dx), IS.at[lax.rem(x + dx, NX)], ISR.at[dx - 1], dev(x=x + dx))

    def input_done():
        for dx in (1, 3, 2):
            w.wait(("is", dx), ISR.at[dx - 1], me)
        din_ref[...] = total(IP[c, x], IR[x], ISR[0], ISR[1], ISR[2]).astype(BF16)

    def taps_y():
        for dy in (1, 2, 3):
            w.send(("ty", dy), TY.at[y], TY.at[y], dev(y=y + dy))

    def taps_z():
        for dy in (1, 2, 3):
            w.wait(("ty", dy), TY.at[lax.rem(y - dy + NY, NY)], me)
        TZ1[zo] = TY[0] + TY[1] + TY[2] + TY[3]
        for k in (1, 2, 3):
            w.send(("tz", k), TZ1.at[zo], TZ1.at[zo], z_near(k))

    def taps_pair(stage):
        if stage == 0:
            for k in (1, 2, 3):
                w.wait(("tz", k), TZ1.at[lax.rem(zo - k + 4, 4)], me)
            TB[0] = TZ1[0] + TZ1[1] + TZ1[2] + TZ1[3]
            w.send(("tb", 0), TB.at[0], TB.at[1], dev(z=zg + side))
        else:
            w.wait(("tb", 0), TB.at[1], me)
            TB[2] = TB[0] + TB[1]
            w.send(("tb", 1), TB.at[2], TB.at[3], dev(z=zg - side))

    def taps_spread():
        w.wait(("tb", 1), TB.at[3], me)
        TT[tp] = (TB[2] + TB[3]) * factor
        for k in range(1, 8):
            w.send(("tt", k), TT.at[tp], TT.at[tp], tp_peer(k))

    def taps_done():
        for k in range(1, 8):
            w.wait(("tt", k), TT.at[lax.rem(tp - k + 8, 8)], me)
        tout_ref[...] = TT[...]

    make_blocks(0)
    make_blocks(1)
    make_blocks(2)
    taps_y()
    pass_on(0)
    make_blocks(3)
    pass_on(1)
    row_done(0)
    for h in hops[0]:
        hop(*h)
    make_blocks(4)
    for j in range(4):
        input_terms(j)
    pass_on(2)
    row_done(1)
    for h in hops[1]:
        hop(*h)
    make_blocks(5)
    for j in range(4, 8):
        input_terms(j)
    input_swap()
    taps_z()
    pass_on(3)
    row_done(2)
    for h in hops[2]:
        hop(*h)
    make_blocks(6)
    make_blocks(7)
    input_sums()
    pass_on(4)
    row_done(3)
    for h in hops[3]:
        hop(*h)
    taps_pair(0)
    pass_on(5)
    row_done(4)
    for h in hops[4]:
        hop(*h)
    pass_on(6)
    row_done(5)
    for h in hops[5]:
        hop(*h)
    taps_pair(1)
    pass_on(7)
    row_done(6)
    for h in hops[6]:
        hop(*h)
    taps_spread()
    row_done(7)
    for h in hops[7]:
        hop(*h)
    input_done()
    for s in (5, 6, 7):
        for name in ("gr", "gl", "vl", "vr"):
            hop(name, s if chains[name][5] == 8 else s - 1)
    taps_done()
    own_k = place[0]
    w.wait(("gr", 7), ZRG.at[7], me)
    w.wait(("gl", 6), ZLG.at[6], me)
    dg_ref[...] = total(RG[own_k], ZRG[7], ZLG[6]) * factor
    w.wait(("vl", 7), ZLV.at[7], me)
    w.wait(("vr", 6), ZRV.at[6], me)
    dv_ref[...] = total(RV[own_k], ZLV[7], ZRV[6]) * factor
    w.drain()


COPIES = 320


def shards(inputs, gate_proj, value_proj, gate_taps, value_taps, out_grad):
    rows, cols = gate_proj.shape
    start = lax.axis_index("tp") * cols
    taps = jnp.stack(
        [
            lax.dynamic_slice_in_dim(gate_taps, start, cols, 1),
            lax.dynamic_slice_in_dim(value_taps, start, cols, 1),
        ]
    )
    factor = float(TOK * NY * NZ) ** (-0.5)
    unit = (rows, cols)
    vm = pltpu.VMEM
    scratch = [
        vm((8, EXT, FEAT), BF16),
        vm((32, *unit), BF16),
        vm((32, *unit), BF16),
        vm((384, TOK), BF16),
        vm((EXT, cols), BF16),
        vm((EXT + 16, cols), F32),
        vm((EXT + 16, cols), F32),
        vm((EXT + 16, cols), F32),
        vm((EXT + 16, cols), F32),
        vm((TOK, cols), BF16),
        vm((TOK, cols), BF16),
        vm((32, *unit), BF16),
        vm((32, *unit), BF16),
    ]
    scratch += [vm((8, *unit), BF16) for _ in range(10)]
    scratch += [vm((8, *unit), BF16) for _ in range(8)]
    scratch += [
        vm((2, NX, TOK, FEAT), BF16),
        vm((NX, TOK, FEAT), BF16),
        vm((NX, TOK, FEAT), BF16),
        vm((3, TOK, FEAT), BF16),
        vm((4, 8, cols), F32),
        vm((4, 8, cols), F32),
        vm((4, 8, cols), F32),
        vm((8, 8, cols), F32),
        pltpu.SemaphoreType.DMA((COPIES,)),
        pltpu.SemaphoreType.DMA((COPIES,)),
        pltpu.SemaphoreType.DMA((4,)),
    ]
    hbm = pl.BlockSpec(memory_space=pl.ANY)
    vmem = pl.BlockSpec(memory_space=pltpu.VMEM)
    din, dg, dv, tout = pl.pallas_call(
        functools.partial(kernel, factor),
        out_shape=(
            jax.ShapeDtypeStruct((TOK, FEAT), BF16),
            jax.ShapeDtypeStruct(unit, F32),
            jax.ShapeDtypeStruct(unit, F32),
            jax.ShapeDtypeStruct((8, 8, cols), F32),
        ),
        in_specs=[hbm, hbm, hbm, hbm, vmem],
        out_specs=(vmem, vmem, vmem, vmem),
        scratch_shapes=scratch,
        compiler_params=pltpu.CompilerParams(
            collective_id=0, has_side_effects=True, vmem_limit_bytes=56 * 1024 * 1024
        ),
    )(inputs[0], gate_proj, value_proj, jnp.swapaxes(out_grad[0], 0, 1), taps)
    taps_all = jnp.moveaxis(tout[:, :6], 0, 1).reshape(6, 8 * cols)
    return din[None], dg, dv, taps_all[:3], taps_all[3:]


def solution(mesh):
    return jax.shard_map(
        shards,
        mesh=mesh,
        in_specs=(P("rep", "fs", "tp"), P("fs", "tp"), P("fs", "tp"), P(), P(), P("rep", "fs", "tp")),
        out_specs=(P("rep", "fs", "tp"), P("fs", "tp"), P("fs", "tp"), P(), P()),
        check_vma=False,
    )
```

```python
import functools

import jax
import jax.numpy as jnp
from jax import lax
from jax.experimental import pallas as pl
from jax.experimental.pallas import tpu as pltpu
from jax.sharding import PartitionSpec as P

MESH = pl.DeviceIdType.MESH
BF16 = jnp.bfloat16
F32 = jnp.float32

NX, NC, NY, NZ = 4, 2, 4, 16
ZL = 8
TOK = 384
COLS = 352
FEAT = 256
EDGE = 16
EXT = TOK + 2 * EDGE


def right_reach(r):
    return 4 if r < 2 else 3


class Wires:
    def __init__(self, send_sems, recv_sems):
        self.send_sems, self.recv_sems = send_sems, recv_sems
        self.index = {}
        self.count = dict.fromkeys(("unit", "tile", "edge", "og", "taps"), 0)

    def at(self, key):
        return self.index.setdefault(key, len(self.index))

    def copy(self, key, src, dst, to, kind):
        return pltpu.make_async_remote_copy(
            src_ref=src,
            dst_ref=dst,
            send_sem=self.send_sems.at[list(self.count).index(kind)],
            recv_sem=self.recv_sems.at[self.at(key)],
            device_id=to,
            device_id_type=MESH,
        )

    def send(self, key, src, dst, to, kind="unit"):
        self.count[kind] += 1
        self.copy(key, src, dst, to, kind).start()

    def wait(self, key, dst, to, kind="unit"):
        self.copy(key, dst, dst, to, kind).wait_recv()

    def drain(self, spans, to):
        for kind, span in spans.items():
            whole = span(self.count[kind])
            self.copy(("drain",), whole, whole, to, kind).wait_send()


def kernel(
    factor,
    x_hbm, wg_hbm, wv_hbm, gt_hbm, vt_hbm, ogt_hbm,
    din_hbm, dg_hbm, dv_hbm, tout_hbm,
    X, U, XB, TS, GT, VT, OGT, OG, PG, PV, KG, KV, CG, CV, DIN, DG, DV,
    send_sems, recv_sems, local_sems,
):
    def parts_of(pool, sizes):
        first, parts = 0, []
        for size in sizes:
            parts.append(pool.at[pl.ds(first, size)])
            first += size
        return parts

    WG, WV, GG, GV, *rest = parts_of(U, [32] * 4 + [8] * 18)
    FAR, DIR, MID, END, RED = ({"g": rest[2 * i], "v": rest[2 * i + 1]} for i in range(5))
    ZRG, ZLG, ZRV, ZLV = rest[10:14]
    SUMS = dict(zip(("gr", "gl", "vr", "vl"), rest[14:18]))
    IP, IR, IS, ISR = parts_of(XB, [2 * NX, NX, NX, 3])
    TY, TZ1, TB, TT = parts_of(TS, [4, 4, 4, 8])
    rep, fs, tp = lax.axis_index("rep"), lax.axis_index("fs"), lax.axis_index("tp")
    zl, y = lax.div(fs, NY), lax.rem(fs, NY)
    x, c = lax.div(tp, NC), lax.rem(tp, NC)
    zg = rep * ZL + zl

    def dev(x=x, c=c, y=y, z=zg):
        z = lax.rem(z + NZ, NZ)
        return (
            lax.div(z, ZL),
            lax.rem(z, ZL) * NY + lax.rem(y + NY, NY),
            lax.rem(x + NX, NX) * NC + c,
        )

    def blk(dz, dy):
        return lax.rem(zl + dz + ZL, ZL) * NY + lax.rem(y + dy + NY, NY)

    def zrow(dz):
        return lax.rem(zl + dz + 2 * ZL, ZL)

    me = dev()
    right, left = dev(z=zg + 1), dev(z=zg - 1)
    up, down = dev(y=y + 1), dev(y=y - 1)
    partner = dev(c=1 - c)
    after_z = zg + lax.div(y + 1, NY)
    after = dev(y=y + 1, z=after_z)
    before_z = zg - 1 + lax.div(y + NY - 1, NY)
    before = dev(y=y - 1, z=before_z)

    def tp_peer(k):
        return (rep, fs, lax.rem(tp + k + 8, 8))

    zq, zo = lax.div(zg, 4), lax.rem(zg, 4)
    side = 4 * (1 - 2 * lax.rem(zq, 2))

    def z_near(k):
        return dev(z=zq * 4 + lax.rem(zo + k, 4))

    own = blk(0, 0)
    loads = [
        pltpu.make_async_copy(wg_hbm, WG.at[own], local_sems.at[0]),
        pltpu.make_async_copy(wv_hbm, WV.at[own], local_sems.at[1]),
        pltpu.make_async_copy(x_hbm, X.at[tp, pl.ds(EDGE, TOK)], local_sems.at[2]),
        pltpu.make_async_copy(ogt_hbm, OGT.at[pl.ds(0, COLS)], local_sems.at[3]),
        pltpu.make_async_copy(gt_hbm, GT, local_sems.at[4]),
        pltpu.make_async_copy(vt_hbm, VT, local_sems.at[5]),
    ]
    for load in loads:
        load.start()

    barrier = pltpu.get_barrier_semaphore()
    peers = [tp_peer(k) for k in range(1, 8)]
    peers += [dev(y=y + k) for k in (1, 2, 3)]
    peers += [right, left, after, before]
    peers += [z_near(k) for k in (1, 2, 3)]
    peers += [dev(z=zg + 4), dev(z=zg - 4)]
    for peer in peers:
        pl.semaphore_signal(barrier, inc=1, device_id=peer, device_id_type=MESH)
    pl.semaphore_wait(barrier, len(peers))

    w = Wires(send_sems, recv_sems)

    loads[0].wait()
    for dy in (1, 3, 2):
        w.send(("gy", dy), WG.at[own], WG.at[own], dev(y=y + dy))
    loads[1].wait()
    w.send(("vz", 1, 1), WV.at[own], WV.at[own], right)
    w.send(("vz", -1, 1), WV.at[own], WV.at[own], left)
    w.send(("gz", 0, 1, 1), WG.at[own], WG.at[own], right)
    w.send(("gz", 0, -1, 1), WG.at[own], WG.at[own], left)
    loads[2].wait()
    head, tail = X.at[tp, pl.ds(EDGE, EDGE)], X.at[tp, pl.ds(TOK, EDGE)]
    lo, hi = pl.ds(0, EDGE), pl.ds(TOK + EDGE, EDGE)
    w.send(("hx", 1), tail, X.at[tp, lo], after, "edge")
    w.send(("hx", -1), head, X.at[tp, hi], before, "edge")
    mine = X.at[tp, pl.ds(EDGE, TOK)]
    for dx in (1, 3, 2):
        w.send(("x", dx), mine, mine, dev(x=x + dx), "tile")
    w.send(("xp", 0), mine, mine, partner, "tile")
    w.send(("vy", 0, 1), WV.at[own], WV.at[own], up)
    w.send(("vy", 0, -1), WV.at[own], WV.at[own], down)

    def out_grad_rows():
        loads[3].wait()
        for i in range(3):
            for j in range(3):
                block = OGT[128 * i : 128 * i + 128, 128 * j : 128 * j + 128].astype(F32)
                cols = min(128, COLS - 128 * i)
                OG[EDGE + 128 * j : EDGE + 128 * j + 128, 128 * i : 128 * i + cols] = (
                    block.T[:, :cols].astype(BF16)
                )

    def gate_chunk(z, first=False):
        part = jnp.dot(
            X[z],
            WG[pl.ds(z * NY, NY)].reshape(FEAT, COLS),
            preferred_element_type=F32,
        )
        if first:
            PG[8 : 8 + EXT] = part
        else:
            PG[8 : 8 + EXT] += part

    def value_chunk(z, first=False):
        part = jnp.dot(
            X[z],
            WV[pl.ds(z * NY, NY)].reshape(FEAT, COLS),
            preferred_element_type=F32,
        )
        if first:
            PV[8 : 8 + EXT] = part
        else:
            PV[8 : 8 + EXT] += part

    def x_arrived(dx):
        slot = X.at[lax.rem(x - dx + NX, NX) * NC + c, pl.ds(EDGE, TOK)]
        w.wait(("x", dx), slot, me, "tile")
        w.send(("xp", dx), slot, slot, partner, "tile")

    def xp_arrived(dx):
        slot = X.at[lax.rem(x - dx + NX, NX) * NC + 1 - c, pl.ds(EDGE, TOK)]
        w.wait(("xp", dx), slot, me, "tile")

    def edges_spread():
        w.wait(("hx", 1), X.at[tp, lo], me, "edge")
        w.wait(("hx", -1), X.at[tp, hi], me, "edge")
        for k in range(1, 8):
            w.send(("hl",), X.at[tp, lo], X.at[tp, lo], tp_peer(k), "edge")
            w.send(("hl",), X.at[tp, hi], X.at[tp, hi], tp_peer(k), "edge")

    def edges_done():
        w.wait(("hl",), X.at[0, pl.ds(0, 14 * EDGE)], me, "edge")

    def gate_y(dy):
        unit = WG.at[blk(0, -dy)]
        w.wait(("gy", dy), unit, me)
        w.send(("gz", 4 - dy, 1, 1), unit, unit, right)
        w.send(("gz", 4 - dy, -1, 1), unit, unit, left)

    def gate_z(r, d):
        for way, reach, to in ((1, right_reach(r), right), (-1, 7 - right_reach(r), left)):
            if d <= reach:
                unit = WG.at[blk(-way * d, r)]
                w.wait(("gz", r, way, d), unit, me)
                if d < reach:
                    w.send(("gz", r, way, d + 1), unit, unit, to)

    def value_z(d):
        for way, reach, to in ((1, 4, right), (-1, 3, left)):
            if d <= reach:
                dz = -way * d
                unit = WV.at[blk(dz, 0)]
                w.wait(("vz", way, d), unit, me)
                if d < reach:
                    w.send(("vz", way, d + 1), unit, unit, to)
                w.send(("vy", dz, 1), unit, unit, up)
                w.send(("vy", dz, -1), unit, unit, down)

    def value_y(dz):
        from_down, from_up = WV.at[blk(dz, -1)], WV.at[blk(dz, 1)]
        w.wait(("vy", dz, 1), from_down, me)
        if dz % 2 == 0:
            w.send(("vf", dz), from_down, from_down, up)
        w.wait(("vy", dz, -1), from_up, me)
        if dz % 2 == 1:
            w.send(("vf", dz), from_up, from_up, down)

    def value_row(dz, first=False):
        w.wait(("vf", dz), WV.at[blk(dz, 2)], me)
        value_chunk(zrow(dz), first)

    value_z(1)
    gate_y(1)
    gate_y(3)
    edges_spread()
    gate_y(2)
    gate_z(0, 1)
    value_y(0)
    value_z(2)
    gate_z(3, 1)
    gate_z(1, 1)
    gate_z(2, 1)
    value_y(1)
    value_y(-1)
    out_grad_rows()
    gate_z(0, 2)
    value_z(3)
    w.send(("og", 1), OG.at[pl.ds(TOK, EDGE)], OG.at[lo], after, "og")
    w.send(("og", -1), OG.at[pl.ds(EDGE, EDGE)], OG.at[hi], before, "og")
    x_arrived(1)
    x_arrived(3)
    gate_z(3, 2)
    value_y(2)
    value_y(-2)
    gate_z(1, 2)
    gate_z(2, 2)
    gate_z(0, 3)
    value_z(4)
    x_arrived(2)
    gate_z(3, 3)
    value_y(3)
    value_y(-3)
    gate_z(1, 3)
    for dx in (0, 1, 3, 2):
        xp_arrived(dx)
    edges_done()
    gate_chunk(zrow(0), first=True)
    gate_chunk(zrow(1))
    gate_z(2, 3)
    gate_chunk(zrow(-1))
    value_row(0, first=True)
    gate_z(0, 4)
    gate_chunk(zrow(2))
    gate_chunk(zrow(-2))
    value_y(-4)
    gate_z(3, 4)
    value_row(1)
    value_row(-1)
    gate_z(1, 4)
    value_row(2)
    value_row(-2)
    gate_z(2, 4)
    gate_chunk(zrow(3))
    gate_chunk(zrow(-3))
    gate_chunk(zrow(4))
    value_row(3)
    value_row(-3)
    value_row(-4)
    w.wait(("og", 1), OG.at[lo], me, "og")
    w.wait(("og", -1), OG.at[hi], me, "og")

    not_first, not_last = fs > 0, fs < NY * ZL - 1
    for ref in (PG, PV):
        ref[8 : 8 + EDGE] = jnp.where(not_first, ref[8 : 8 + EDGE], 0.0)
        ref[8 + EDGE + TOK : 8 + EXT] = jnp.where(not_last, ref[8 + EDGE + TOK : 8 + EXT], 0.0)
    OG[:EDGE] = jnp.where(not_first, OG[:EDGE].astype(F32), 0.0).astype(BF16)
    OG[EDGE + TOK :] = jnp.where(not_last, OG[EDGE + TOK :].astype(F32), 0.0).astype(BF16)

    loads[4].wait()
    loads[5].wait()
    taps = jnp.concatenate([GT[...], VT[...], jnp.zeros((2, 8 * COLS), F32)], axis=0)
    taps = pltpu.roll(taps, lax.rem((8 - tp) * COLS, 8 * COLS), axis=1)[:, :COLS]
    g0, g1, g2, v0, v1, v2 = (taps[k : k + 1] for k in range(6))

    def rounded(value):
        return value.astype(BF16).astype(F32)

    def cot_rows(i):
        base = pl.multiple_of(i * 16, 16)
        gate = rounded(PG[pl.ds(base, 32)])
        value = rounded(PV[pl.ds(base, 32)])
        gm, gz, gp = gate[7:23], gate[8:24], gate[9:25]
        vm, vz, vp = value[7:23], value[8:24], value[9:25]
        gate_mix = g0 * gm + g1 * gz + g2 * gp
        value_mix = v0 * vm + v1 * vz + v2 * vp
        grad = OG[pl.ds(base, 16)].astype(F32)
        s = jax.nn.sigmoid(gate_mix)
        gate_cot = grad * value_mix * (s * (1.0 + gate_mix * (1.0 - s)))
        value_cot = grad * (gate_mix * s)
        KG[pl.ds(base + 8, 16)] = gate_cot
        KV[pl.ds(base + 8, 16)] = value_cot
        return [
            (p * k).reshape(2, 8, COLS).sum(axis=0)
            for p, k in (
                (gm, gate_cot), (gz, gate_cot), (gp, gate_cot),
                (vm, value_cot), (vz, value_cot), (vp, value_cot),
            )
        ]

    cot_rows(0)
    cot_rows(TOK // 16 + 1)
    zero = jnp.zeros((8, COLS), F32)
    tap_sums = lax.fori_loop(
        1, TOK // 16 + 1,
        lambda i, sums: tuple(a + b for a, b in zip(sums, cot_rows(i))),
        (zero,) * 6,
    )

    def back_rows(i, carry):
        base = pl.multiple_of(i * 16, 16)
        out = pl.ds(pl.multiple_of(i * 16 - 16, 16), 16)
        for source, target, (t0, t1, t2) in ((KG, CG, (g0, g1, g2)), (KV, CV, (v0, v1, v2))):
            cot = source[pl.ds(base, 32)]
            target[out] = (t0 * cot[9:25] + t1 * cot[8:24] + t2 * cot[7:23]).astype(BF16)
        return carry

    lax.fori_loop(1, TOK // 16 + 1, back_rows, 0)

    rows = [jnp.sum(part, axis=0, keepdims=True) for part in tap_sums]
    TY[y] = jnp.concatenate(rows + [jnp.zeros((2, COLS), F32)], axis=0)

    order = (0, 1, -1, 2, -2, 3, -3, 4)
    place = {dz % ZL: k for k, dz in enumerate(order)}
    COT, TERMS = {"g": CG, "v": CV}, {"g": GG, "v": GV}

    def turn(k):
        return (1, up, down) if k % 2 == 0 else (-1, down, up)

    def make_blocks(h, k):
        dz = order[k]
        z = zrow(dz)
        block = lax.dot_general(
            X[z, EDGE : EDGE + TOK, :], COT[h][...],
            (((0,), (0,)), ((), ())), preferred_element_type=F32,
        )
        TERMS[h][pl.ds(z * NY, NY)] = block.astype(BF16).reshape(NY, 64, COLS)
        way, onward, back = turn(k)
        w.send(("far", h, k), TERMS[h].at[blk(dz, 2)], FAR[h].at[k], onward)
        w.send(("dir", h, k), TERMS[h].at[blk(dz, -way)], DIR[h].at[k], back)

    def total(*parts):
        acc = parts[0].astype(F32)
        for part in parts[1:]:
            acc = acc + part.astype(F32)
        return acc

    def pass_on(h, k):
        way, onward, back = turn(k)
        w.wait(("far", h, k), FAR[h].at[k], me)
        MID[h][k] = total(FAR[h][k], TERMS[h][blk(order[k], way)]).astype(BF16)
        w.send(("mid", h, k), MID[h].at[k], END[h].at[k], onward)

    def row_done(h, k):
        w.wait(("dir", h, k), DIR[h].at[k], me)
        w.wait(("mid", h, k), END[h].at[k], me)
        RED[h][k] = total(TERMS[h][blk(order[k], 0)], DIR[h][k], END[h][k]).astype(BF16)

    chains = {
        "gr": ("g", ZRG, -1, 0, 8, right, None),
        "gl": ("g", ZLG, 1, 1, 7, left, None),
        "vr": ("v", ZRV, -1, 1, 7, right, dev(z=zg + 4)),
        "vl": ("v", ZLV, 1, 0, 8, left, dev(z=zg - 4)),
    }

    def hop(name, s):
        h, landing, way, start, length, to, end = chains[name]
        k = place[(way * (start + s)) % ZL]
        cut = length - 4 if end is not None else None
        first = s == 0 or (cut is not None and s == cut + 1)
        slot = landing.at[s]
        if first:
            w.send((name, s), RED[h].at[k], slot, to)
            return
        w.wait((name, s - 1), landing.at[s - 1], me)
        SUMS[name][s] = total(landing[s - 1], RED[h][k]).astype(BF16)
        w.send((name, s), SUMS[name].at[s], slot, end if s == cut else to)

    def finish(h, names, out):
        parts = [RED[h][place[0]]]
        for name in names:
            _, landing, _, _, length, _, end = chains[name]
            for s in (length - 1,) if end is None else (length - 1, length - 4):
                w.wait((name, s), landing.at[s], me)
                parts.append(landing[s])
        out[...] = total(*parts) * factor

    def input_terms(j):
        part = lax.dot_general(
            CG[...], WG[NY * j : NY * j + NY].reshape(FEAT, COLS),
            (((1,), (1,)), ((), ())), preferred_element_type=F32,
        ) + lax.dot_general(
            CV[...], WV[NY * j : NY * j + NY].reshape(FEAT, COLS),
            (((1,), (1,)), ((), ())), preferred_element_type=F32,
        )
        IP[NX * (j % 2) + j // 2] = part.astype(BF16)

    def input_swap():
        for i in range(NX):
            w.send(("ip", i), IP.at[NX * (1 - c) + i], IR.at[i], partner, "tile")

    def input_sums():
        for i in range(NX):
            w.wait(("ip", i), IR.at[i], me, "tile")
            IS[i] = total(IP[NX * c + i], IR[i]).astype(BF16)
        for dx in (1, 3, 2):
            w.send(("is", dx), IS.at[lax.rem(x + dx, NX)], ISR.at[dx - 1], dev(x=x + dx), "tile")

    results = []

    def put_out(source, target):
        copy = pltpu.make_async_copy(source, target, local_sems.at[6 + len(results)])
        copy.start()
        results.append(copy)

    def input_done():
        for dx in (1, 3, 2):
            w.wait(("is", dx), ISR.at[dx - 1], me, "tile")
        DIN[...] = total(IP[NX * c + x], IR[x], ISR[0], ISR[1], ISR[2]).astype(BF16)
        put_out(DIN, din_hbm)

    def taps_y():
        for dy in (1, 2, 3):
            w.send(("ty",), TY.at[y], TY.at[y], dev(y=y + dy), "taps")

    def taps_z():
        w.wait(("ty",), TY.at[pl.ds(0, 3)], me, "taps")
        TZ1[zo] = TY[0] + TY[1] + TY[2] + TY[3]
        for k in (1, 2, 3):
            w.send(("tz",), TZ1.at[zo], TZ1.at[zo], z_near(k), "taps")

    def taps_pair(stage):
        if stage == 0:
            w.wait(("tz",), TZ1.at[pl.ds(0, 3)], me, "taps")
            TB[0] = TZ1[0] + TZ1[1] + TZ1[2] + TZ1[3]
            w.send(("tb", 0), TB.at[0], TB.at[1], dev(z=zg + side), "taps")
        else:
            w.wait(("tb", 0), TB.at[1], me, "taps")
            TB[2] = TB[0] + TB[1]
            w.send(("tb", 1), TB.at[2], TB.at[3], dev(z=zg - side), "taps")

    def taps_spread():
        w.wait(("tb", 1), TB.at[3], me, "taps")
        TT[tp] = (TB[2] + TB[3]) * factor
        for k in range(1, 8):
            w.send(("tt",), TT.at[tp], TT.at[tp], tp_peer(k), "taps")

    def taps_done():
        w.wait(("tt",), TT.at[pl.ds(0, 7)], me, "taps")
        put_out(TT, tout_hbm)

    steps = [(h, k) for h in "gv" for k in range(ZL)]
    after_row = {
        ("g", 0): [("gr", 0)],
        ("g", 1): [("gl", 0)],
        ("g", 2): [("gr", 1)],
        ("g", 3): [("gl", 1)],
        ("g", 4): [("gr", 2)],
        ("g", 5): [("gl", 2)],
        ("g", 6): [("gr", 3)],
        ("g", 7): [("gl", 3), ("gr", 4)],
        ("v", 0): [("vl", 0)],
        ("v", 1): [("vl", 1), ("gl", 4), ("gr", 5)],
        ("v", 2): [("vr", 0)],
        ("v", 3): [("vl", 2), ("gl", 5), ("gr", 6)],
        ("v", 4): [("vr", 1)],
        ("v", 5): [("vl", 3), ("vr", 4)],
        ("v", 6): [("vr", 2), ("vl", 5), ("gl", 6), ("gr", 7)],
        ("v", 7): [("vl", 4), ("vr", 3)],
    }
    extra = {2: [taps_y], 6: [taps_z], 10: [lambda: taps_pair(0)], 11: [input_swap], 13: [lambda: taps_pair(1)],
             14: [input_sums], 16: [taps_spread]}
    for j in range(8):
        extra.setdefault(3 + j, []).append(functools.partial(input_terms, j))
    for i in range(len(steps) + 5):
        if i < len(steps):
            make_blocks(*steps[i])
        if 0 <= i - 3 < len(steps):
            pass_on(*steps[i - 3])
        if 0 <= i - 5 < len(steps):
            row_done(*steps[i - 5])
            for name, s in after_row[steps[i - 5]]:
                hop(name, s)
        for run in extra.get(i, ()):
            run()
    hop("vl", 6)
    hop("vr", 5)
    input_done()
    taps_done()
    finish("g", ("gr", "gl"), DG)
    put_out(DG, dg_hbm)
    hop("vl", 7)
    hop("vr", 6)
    finish("v", ("vl", "vr"), DV)
    put_out(DV, dv_hbm)
    w.drain(
        {
            "unit": lambda n: U.at[pl.ds(0, n)],
            "tile": lambda n: XB.at[pl.ds(0, n)],
            "edge": lambda n: X.at[0, pl.ds(0, n * EDGE)],
            "og": lambda n: OG.at[pl.ds(0, n * EDGE)],
            "taps": lambda n: TS.at[pl.ds(0, n)],
        },
        me,
    )
    for copy in results:
        copy.wait()
    if len(w.index) != RECEIVES:
        raise ValueError(str(len(w.index)))


RECEIVES = 165


def finisher(din_ref, dg_ref, dv_ref, tt_ref, din_out, dg_out, dv_out, tg_out, tv_out):
    din_out[...] = din_ref[...]
    dg_out[...] = dg_ref[...]
    dv_out[...] = dv_ref[...]
    taps = jnp.concatenate([tt_ref[i] for i in range(8)], axis=1)
    tg_out[...] = taps[0:3]
    tv_out[...] = taps[3:6]


def shards(inputs, gate_proj, value_proj, gate_taps, value_taps, out_grad):
    unit = gate_proj.shape
    cols = unit[1]
    factor = float(TOK * NY * NZ) ** (-0.5)
    vm = pltpu.VMEM
    scratch = [
        vm((8, EXT, FEAT), BF16),
        vm((272, *unit), BF16),
        vm((4 * NX + 3, TOK, FEAT), BF16),
        vm((20, 8, cols), F32),
        vm(gate_taps.shape, F32),
        vm(gate_taps.shape, F32),
        vm((384, TOK), BF16),
        vm((EXT, cols), BF16),
        vm((EXT + 16, cols), F32),
        vm((EXT + 16, cols), F32),
        vm((EXT + 16, cols), F32),
        vm((EXT + 16, cols), F32),
        vm((TOK, cols), BF16),
        vm((TOK, cols), BF16),
        vm((TOK, FEAT), BF16),
        vm(unit, F32),
        vm(unit, F32),
        pltpu.SemaphoreType.DMA((5,)),
        pltpu.SemaphoreType.DMA((RECEIVES,)),
        pltpu.SemaphoreType.DMA((10,)),
    ]
    anywhere = pl.BlockSpec(memory_space=pl.ANY)
    vmem = pl.BlockSpec(memory_space=pltpu.VMEM)
    tile = jax.ShapeDtypeStruct((TOK, FEAT), BF16)
    grad = jax.ShapeDtypeStruct(unit, F32)
    tap = jax.ShapeDtypeStruct(gate_taps.shape, F32)
    sums = pl.pallas_call(
        functools.partial(kernel, factor),
        out_shape=(tile, grad, grad, jax.ShapeDtypeStruct((8, 8, cols), F32)),
        in_specs=[anywhere] * 6,
        out_specs=(anywhere,) * 4,
        scratch_shapes=scratch,
        compiler_params=pltpu.CompilerParams(
            collective_id=0, has_side_effects=True, vmem_limit_bytes=65000 * 1024
        ),
    )(inputs[0], gate_proj, value_proj, gate_taps, value_taps, jnp.swapaxes(out_grad[0], 0, 1))
    din, dg, dv, tg, tv = pl.pallas_call(
        finisher,
        out_shape=(tile, grad, grad, tap, tap),
        in_specs=[vmem] * 4,
        out_specs=(vmem,) * 5,
    )(*sums)
    return din[None], dg, dv, tg, tv


def solution(mesh):
    return jax.shard_map(
        shards,
        mesh=mesh,
        in_specs=(P("rep", "fs", "tp"), P("fs", "tp"), P("fs", "tp"), P(), P(), P("rep", "fs", "tp")),
        out_specs=(P("rep", "fs", "tp"), P("fs", "tp"), P("fs", "tp"), P(), P()),
        check_vma=False,
    )
```

```python
import functools

import jax
import jax.numpy as jnp
from jax import lax
from jax.experimental import pallas as pl
from jax.experimental.pallas import tpu as pltpu
from jax.sharding import PartitionSpec as P

MESH = pl.DeviceIdType.MESH
BF16 = jnp.bfloat16
F32 = jnp.float32

NX, NC, NY, NZ = 4, 2, 4, 16
ZL = 8
TOK = 384
COLS = 352
FEAT = 256
EDGE = 16
EXT = TOK + 2 * EDGE


def right_reach(r):
    return 4 if r < 2 else 3


class Wires:
    def __init__(self, send_sems, recv_sems):
        self.send_sems, self.recv_sems = send_sems, recv_sems
        self.index = {}
        self.count = dict.fromkeys(("unit", "tile", "edge", "og", "taps"), 0)

    def at(self, key):
        return self.index.setdefault(key, len(self.index))

    def copy(self, key, src, dst, to, kind):
        return pltpu.make_async_remote_copy(
            src_ref=src,
            dst_ref=dst,
            send_sem=self.send_sems.at[list(self.count).index(kind)],
            recv_sem=self.recv_sems.at[self.at(key)],
            device_id=to,
            device_id_type=MESH,
        )

    def send(self, key, src, dst, to, kind="unit"):
        self.count[kind] += 1
        self.copy(key, src, dst, to, kind).start()

    def wait(self, key, dst, to, kind="unit"):
        self.copy(key, dst, dst, to, kind).wait_recv()

    def drain(self, spans, to):
        for kind, span in spans.items():
            whole = span(self.count[kind])
            self.copy(("drain",), whole, whole, to, kind).wait_send()


def kernel(
    factor,
    x_hbm, wg_hbm, wv_hbm, gt_hbm, vt_hbm, ogt_hbm,
    din_hbm, dg_hbm, dv_hbm, tout_hbm,
    X, U, XB, TS, GT, VT, OGT, OG, PG, PV, KG, KV, CG, CV, DIN, DG, DV,
    send_sems, recv_sems, local_sems,
):
    def parts_of(pool, sizes):
        first, parts = 0, []
        for size in sizes:
            parts.append(pool.at[pl.ds(first, size)])
            first += size
        return parts

    WG, WV, GG, GV, *rest = parts_of(U, [32] * 4 + [8] * 18)
    FAR, DIR, MID, END, RED = ({"g": rest[2 * i], "v": rest[2 * i + 1]} for i in range(5))
    ends = [(h, way) for h in "gv" for way in (1, -1)]
    LAND, SUMS = dict(zip(ends, rest[10:14])), dict(zip(ends, rest[14:18]))
    IP, IR, IS, ISR = parts_of(XB, [2 * NX, NX, NX, 3])
    TY, TZ1, TB, TT = parts_of(TS, [4, 4, 4, 8])
    rep, fs, tp = lax.axis_index("rep"), lax.axis_index("fs"), lax.axis_index("tp")
    zl, y = lax.div(fs, NY), lax.rem(fs, NY)
    x, c = lax.div(tp, NC), lax.rem(tp, NC)
    zg = rep * ZL + zl

    def dev(x=x, c=c, y=y, z=zg):
        z = lax.rem(z + NZ, NZ)
        return (
            lax.div(z, ZL),
            lax.rem(z, ZL) * NY + lax.rem(y + NY, NY),
            lax.rem(x + NX, NX) * NC + c,
        )

    def blk(dz, dy):
        return lax.rem(zl + dz + ZL, ZL) * NY + lax.rem(y + dy + NY, NY)

    def zrow(dz):
        return lax.rem(zl + dz + 2 * ZL, ZL)

    me = dev()
    right, left = dev(z=zg + 1), dev(z=zg - 1)
    up, down = dev(y=y + 1), dev(y=y - 1)
    partner = dev(c=1 - c)
    after_z = zg + lax.div(y + 1, NY)
    after = dev(y=y + 1, z=after_z)
    before_z = zg - 1 + lax.div(y + NY - 1, NY)
    before = dev(y=y - 1, z=before_z)

    def tp_peer(k):
        return (rep, fs, lax.rem(tp + k + 8, 8))

    zq, zo = lax.div(zg, 4), lax.rem(zg, 4)
    side = 4 * (1 - 2 * lax.rem(zq, 2))

    def z_near(k):
        return dev(z=zq * 4 + lax.rem(zo + k, 4))

    own = blk(0, 0)
    loads = [
        pltpu.make_async_copy(wg_hbm, WG.at[own], local_sems.at[0]),
        pltpu.make_async_copy(wv_hbm, WV.at[own], local_sems.at[1]),
        pltpu.make_async_copy(x_hbm, X.at[tp, pl.ds(EDGE, TOK)], local_sems.at[2]),
        pltpu.make_async_copy(ogt_hbm, OGT.at[pl.ds(0, COLS)], local_sems.at[3]),
        pltpu.make_async_copy(gt_hbm, GT, local_sems.at[4]),
        pltpu.make_async_copy(vt_hbm, VT, local_sems.at[5]),
    ]
    for load in loads:
        load.start()

    barrier = pltpu.get_barrier_semaphore()
    peers = [tp_peer(k) for k in range(1, 8)]
    peers += [dev(y=y + k) for k in (1, 2, 3)]
    peers += [right, left, after, before]
    peers += [z_near(k) for k in (1, 2, 3)]
    peers += [dev(z=zg + 4), dev(z=zg - 4)]
    for peer in peers:
        pl.semaphore_signal(barrier, inc=1, device_id=peer, device_id_type=MESH)
    pl.semaphore_wait(barrier, len(peers))

    w = Wires(send_sems, recv_sems)

    loads[0].wait()
    for dy in (1, 3, 2):
        w.send(("gy", dy), WG.at[own], WG.at[own], dev(y=y + dy))
    loads[1].wait()
    w.send(("vz", 1, 1), WV.at[own], WV.at[own], right)
    w.send(("vz", -1, 1), WV.at[own], WV.at[own], left)
    w.send(("gz", 0, 1, 1), WG.at[own], WG.at[own], right)
    w.send(("gz", 0, -1, 1), WG.at[own], WG.at[own], left)
    loads[2].wait()
    head, tail = X.at[tp, pl.ds(EDGE, EDGE)], X.at[tp, pl.ds(TOK, EDGE)]
    lo, hi = pl.ds(0, EDGE), pl.ds(TOK + EDGE, EDGE)
    w.send(("hx", 1), tail, X.at[tp, lo], after, "edge")
    w.send(("hx", -1), head, X.at[tp, hi], before, "edge")
    mine = X.at[tp, pl.ds(EDGE, TOK)]
    for dx in (1, 3, 2):
        w.send(("x", dx), mine, mine, dev(x=x + dx), "tile")
    w.send(("xp", 0), mine, mine, partner, "tile")
    w.send(("vy", 0, 1), WV.at[own], WV.at[own], up)
    w.send(("vy", 0, -1), WV.at[own], WV.at[own], down)

    def out_grad_rows():
        loads[3].wait()
        for i in range(3):
            for j in range(3):
                block = OGT[128 * i : 128 * i + 128, 128 * j : 128 * j + 128].astype(F32)
                cols = min(128, COLS - 128 * i)
                OG[EDGE + 128 * j : EDGE + 128 * j + 128, 128 * i : 128 * i + cols] = (
                    block.T[:, :cols].astype(BF16)
                )

    def gate_chunk(z, first=False):
        part = jnp.dot(
            X[z],
            WG[pl.ds(z * NY, NY)].reshape(FEAT, COLS),
            preferred_element_type=F32,
        )
        if first:
            PG[8 : 8 + EXT] = part
        else:
            PG[8 : 8 + EXT] += part

    def value_chunk(z, first=False):
        part = jnp.dot(
            X[z],
            WV[pl.ds(z * NY, NY)].reshape(FEAT, COLS),
            preferred_element_type=F32,
        )
        if first:
            PV[8 : 8 + EXT] = part
        else:
            PV[8 : 8 + EXT] += part

    def x_arrived(dx):
        slot = X.at[lax.rem(x - dx + NX, NX) * NC + c, pl.ds(EDGE, TOK)]
        w.wait(("x", dx), slot, me, "tile")
        w.send(("xp", dx), slot, slot, partner, "tile")

    def xp_arrived(dx):
        slot = X.at[lax.rem(x - dx + NX, NX) * NC + 1 - c, pl.ds(EDGE, TOK)]
        w.wait(("xp", dx), slot, me, "tile")

    def edges_spread():
        w.wait(("hx", 1), X.at[tp, lo], me, "edge")
        w.wait(("hx", -1), X.at[tp, hi], me, "edge")
        for k in range(1, 8):
            w.send(("hl",), X.at[tp, lo], X.at[tp, lo], tp_peer(k), "edge")
            w.send(("hl",), X.at[tp, hi], X.at[tp, hi], tp_peer(k), "edge")

    def edges_done():
        w.wait(("hl",), X.at[0, pl.ds(0, 14 * EDGE)], me, "edge")

    def gate_y(dy):
        unit = WG.at[blk(0, -dy)]
        w.wait(("gy", dy), unit, me)
        w.send(("gz", 4 - dy, 1, 1), unit, unit, right)
        w.send(("gz", 4 - dy, -1, 1), unit, unit, left)

    def gate_z(r, d):
        for way, reach, to in ((1, right_reach(r), right), (-1, 7 - right_reach(r), left)):
            if d <= reach:
                unit = WG.at[blk(-way * d, r)]
                w.wait(("gz", r, way, d), unit, me)
                if d < reach:
                    w.send(("gz", r, way, d + 1), unit, unit, to)

    def value_z(d):
        for way, reach, to in ((1, 4, right), (-1, 3, left)):
            if d <= reach:
                dz = -way * d
                unit = WV.at[blk(dz, 0)]
                w.wait(("vz", way, d), unit, me)
                if d < reach:
                    w.send(("vz", way, d + 1), unit, unit, to)
                w.send(("vy", dz, 1), unit, unit, up)
                w.send(("vy", dz, -1), unit, unit, down)

    def value_y(dz):
        from_down, from_up = WV.at[blk(dz, -1)], WV.at[blk(dz, 1)]
        w.wait(("vy", dz, 1), from_down, me)
        if dz % 2 == 0:
            w.send(("vf", dz), from_down, from_down, up)
        w.wait(("vy", dz, -1), from_up, me)
        if dz % 2 == 1:
            w.send(("vf", dz), from_up, from_up, down)

    def value_row(dz, first=False):
        w.wait(("vf", dz), WV.at[blk(dz, 2)], me)
        value_chunk(zrow(dz), first)

    value_z(1)
    gate_y(1)
    gate_y(3)
    gate_y(2)
    gate_z(0, 1)
    value_y(0)
    value_z(2)
    gate_z(3, 1)
    gate_z(1, 1)
    edges_spread()
    gate_z(2, 1)
    value_y(1)
    value_y(-1)
    out_grad_rows()
    gate_z(0, 2)
    value_z(3)
    w.send(("og", 1), OG.at[pl.ds(TOK, EDGE)], OG.at[lo], after, "og")
    w.send(("og", -1), OG.at[pl.ds(EDGE, EDGE)], OG.at[hi], before, "og")
    x_arrived(1)
    x_arrived(3)
    gate_z(3, 2)
    value_y(2)
    value_y(-2)
    gate_z(1, 2)
    gate_z(2, 2)
    gate_z(0, 3)
    value_z(4)
    x_arrived(2)
    gate_z(3, 3)
    value_y(3)
    value_y(-3)
    gate_z(1, 3)
    for dx in (0, 1, 3, 2):
        xp_arrived(dx)
    edges_done()
    gate_chunk(zrow(0), first=True)
    gate_chunk(zrow(1))
    gate_z(2, 3)
    gate_chunk(zrow(-1))
    value_row(0, first=True)
    gate_z(0, 4)
    gate_chunk(zrow(2))
    gate_chunk(zrow(-2))
    value_y(-4)
    gate_z(3, 4)
    value_row(1)
    value_row(-1)
    gate_z(1, 4)
    value_row(2)
    value_row(-2)
    gate_z(2, 4)
    gate_chunk(zrow(3))
    gate_chunk(zrow(-3))
    gate_chunk(zrow(4))
    value_row(3)
    value_row(-3)
    value_row(-4)
    w.wait(("og", 1), OG.at[lo], me, "og")
    w.wait(("og", -1), OG.at[hi], me, "og")

    not_first, not_last = fs > 0, fs < NY * ZL - 1
    for ref in (PG, PV):
        ref[8 : 8 + EDGE] = jnp.where(not_first, ref[8 : 8 + EDGE], 0.0)
        ref[8 + EDGE + TOK : 8 + EXT] = jnp.where(not_last, ref[8 + EDGE + TOK : 8 + EXT], 0.0)
    OG[:EDGE] = jnp.where(not_first, OG[:EDGE].astype(F32), 0.0).astype(BF16)
    OG[EDGE + TOK :] = jnp.where(not_last, OG[EDGE + TOK :].astype(F32), 0.0).astype(BF16)

    loads[4].wait()
    loads[5].wait()
    taps = jnp.concatenate([GT[...], VT[...], jnp.zeros((2, 8 * COLS), F32)], axis=0)
    taps = pltpu.roll(taps, lax.rem((8 - tp) * COLS, 8 * COLS), axis=1)[:, :COLS]
    g0, g1, g2, v0, v1, v2 = (taps[k : k + 1] for k in range(6))

    def rounded(value):
        return value.astype(BF16).astype(F32)

    def cot_rows(i):
        base = pl.multiple_of(i * 16, 16)
        gate = rounded(PG[pl.ds(base, 32)])
        value = rounded(PV[pl.ds(base, 32)])
        gm, gz, gp = gate[7:23], gate[8:24], gate[9:25]
        vm, vz, vp = value[7:23], value[8:24], value[9:25]
        gate_mix = g0 * gm + g1 * gz + g2 * gp
        value_mix = v0 * vm + v1 * vz + v2 * vp
        grad = OG[pl.ds(base, 16)].astype(F32)
        s = jax.nn.sigmoid(gate_mix)
        gate_cot = grad * value_mix * (s * (1.0 + gate_mix * (1.0 - s)))
        value_cot = grad * (gate_mix * s)
        KG[pl.ds(base + 8, 16)] = gate_cot
        KV[pl.ds(base + 8, 16)] = value_cot
        return [
            (p * k).reshape(2, 8, COLS).sum(axis=0)
            for p, k in (
                (gm, gate_cot), (gz, gate_cot), (gp, gate_cot),
                (vm, value_cot), (vz, value_cot), (vp, value_cot),
            )
        ]

    cot_rows(0)
    cot_rows(TOK // 16 + 1)
    zero = jnp.zeros((8, COLS), F32)
    tap_sums = lax.fori_loop(
        1, TOK // 16 + 1,
        lambda i, sums: tuple(a + b for a, b in zip(sums, cot_rows(i))),
        (zero,) * 6,
    )

    def back_rows(i, carry):
        base = pl.multiple_of(i * 16, 16)
        out = pl.ds(pl.multiple_of(i * 16 - 16, 16), 16)
        for source, target, (t0, t1, t2) in ((KG, CG, (g0, g1, g2)), (KV, CV, (v0, v1, v2))):
            cot = source[pl.ds(base, 32)]
            target[out] = (t0 * cot[9:25] + t1 * cot[8:24] + t2 * cot[7:23]).astype(BF16)
        return carry

    lax.fori_loop(1, TOK // 16 + 1, back_rows, 0)

    rows = [jnp.sum(part, axis=0, keepdims=True) for part in tap_sums]
    TY[y] = jnp.concatenate(rows + [jnp.zeros((2, COLS), F32)], axis=0)

    order = (0, 1, -1, 2, -2, 3, -3, 4)
    place = {dz % ZL: k for k, dz in enumerate(order)}
    COT, TERMS = {"g": CG, "v": CV}, {"g": GG, "v": GV}

    def turn(h, k):
        return (1, up, down) if (k % 2 == 0) == (h == "g") else (-1, down, up)

    def make_blocks(h, k):
        dz = order[k]
        z = zrow(dz)
        block = lax.dot_general(
            X[z, EDGE : EDGE + TOK, :], COT[h][...],
            (((0,), (0,)), ((), ())), preferred_element_type=F32,
        )
        TERMS[h][pl.ds(z * NY, NY)] = block.astype(BF16).reshape(NY, 64, COLS)
        way, onward, back = turn(h, k)
        w.send(("far", h, k), TERMS[h].at[blk(dz, 2)], FAR[h].at[k], onward)
        w.send(("dir", h, k), TERMS[h].at[blk(dz, -way)], DIR[h].at[k], back)

    def total(*parts):
        acc = parts[0].astype(F32)
        for part in parts[1:]:
            acc = acc + part.astype(F32)
        return acc

    def pass_on(h, k):
        way, onward, back = turn(h, k)
        w.wait(("far", h, k), FAR[h].at[k], me)
        MID[h][k] = total(FAR[h][k], TERMS[h][blk(order[k], way)]).astype(BF16)
        w.send(("mid", h, k), MID[h].at[k], END[h].at[k], onward)

    def row_done(h, k):
        w.wait(("dir", h, k), DIR[h].at[k], me)
        w.wait(("mid", h, k), END[h].at[k], me)
        RED[h][k] = total(TERMS[h][blk(order[k], 0)], DIR[h][k], END[h][k]).astype(BF16)

    def start_of(h, way):
        return 8 if (h == "g") == (way == 1) else 7

    def row_at(way, d):
        return place[(way * d) % ZL]

    def hop(h, way, d):
        landing = LAND[h, way]
        k = row_at(way, d)
        if d in (start_of(h, way), 3, 2):
            source = RED[h].at[k]
        else:
            w.wait((h, way, d), landing.at[d], me)
            SUMS[h, way][d] = total(landing[d], RED[h][k]).astype(BF16)
            source = SUMS[h, way].at[d]
        slot, to = (d - 1, 1) if d not in (3, 4) else (d - 1, d)
        w.send((h, way, slot), source, landing.at[slot], dev(z=zg + way * to))

    def finish(h, out):
        parts = [RED[h][place[0]]]
        for way in (1, -1):
            for slot in (0, 2, 3):
                w.wait((h, way, slot), LAND[h, way].at[slot], me)
                parts.append(LAND[h, way][slot])
        out[...] = total(*parts) * factor

    def input_terms(j):
        part = lax.dot_general(
            CG[...], WG[NY * j : NY * j + NY].reshape(FEAT, COLS),
            (((1,), (1,)), ((), ())), preferred_element_type=F32,
        ) + lax.dot_general(
            CV[...], WV[NY * j : NY * j + NY].reshape(FEAT, COLS),
            (((1,), (1,)), ((), ())), preferred_element_type=F32,
        )
        IP[NX * (j % 2) + j // 2] = part.astype(BF16)

    def input_swap():
        for i in range(NX):
            w.send(("ip", i), IP.at[NX * (1 - c) + i], IR.at[i], partner, "tile")

    def input_sums():
        for i in range(NX):
            w.wait(("ip", i), IR.at[i], me, "tile")
            IS[i] = total(IP[NX * c + i], IR[i]).astype(BF16)
        for dx in (1, 3, 2):
            w.send(("is", dx), IS.at[lax.rem(x + dx, NX)], ISR.at[dx - 1], dev(x=x + dx), "tile")

    results = []

    def put_out(source, target):
        copy = pltpu.make_async_copy(source, target, local_sems.at[6 + len(results)])
        copy.start()
        results.append(copy)

    def input_done():
        for dx in (1, 3, 2):
            w.wait(("is", dx), ISR.at[dx - 1], me, "tile")
        DIN[...] = total(IP[NX * c + x], IR[x], ISR[0], ISR[1], ISR[2]).astype(BF16)
        put_out(DIN, din_hbm)

    def taps_y():
        for dy in (1, 2, 3):
            w.send(("ty",), TY.at[y], TY.at[y], dev(y=y + dy), "taps")

    def taps_z():
        w.wait(("ty",), TY.at[pl.ds(0, 3)], me, "taps")
        TZ1[zo] = TY[0] + TY[1] + TY[2] + TY[3]
        for k in (1, 2, 3):
            w.send(("tz",), TZ1.at[zo], TZ1.at[zo], z_near(k), "taps")

    def taps_pair(stage):
        if stage == 0:
            w.wait(("tz",), TZ1.at[pl.ds(0, 3)], me, "taps")
            TB[0] = TZ1[0] + TZ1[1] + TZ1[2] + TZ1[3]
            w.send(("tb", 0), TB.at[0], TB.at[1], dev(z=zg + side), "taps")
        else:
            w.wait(("tb", 0), TB.at[1], me, "taps")
            TB[2] = TB[0] + TB[1]
            w.send(("tb", 1), TB.at[2], TB.at[3], dev(z=zg - side), "taps")

    def taps_spread():
        w.wait(("tb", 1), TB.at[3], me, "taps")
        TT[tp] = (TB[2] + TB[3]) * factor
        for k in range(1, 8):
            w.send(("tt",), TT.at[tp], TT.at[tp], tp_peer(k), "taps")

    def taps_done():
        w.wait(("tt",), TT.at[pl.ds(0, 7)], me, "taps")
        put_out(TT, tout_hbm)

    items = [(h, k) for k in range(5) for h in "gv"]
    items += [(h, k) for h in "gv" for k in (5, 6, 7)]
    ahead, lag, spacing = 4, 3, 3
    row_step = {item: t + lag for t, item in enumerate(items)}
    hop_step = {}
    for h, way in ends:
        for d in range(start_of(h, way), 0, -1):
            step = row_step[h, row_at(way, d)]
            if (h, way, d + 1) in hop_step and d not in (3, 2):
                step = max(step, hop_step[h, way, d + 1] + spacing)
            hop_step[h, way, d] = step
    extra = {4: [taps_z], 5: [input_swap], 8: [lambda: taps_pair(0)], 9: [input_sums], 12: [lambda: taps_pair(1)],
             16: [taps_spread]}
    for j in range(4, 8):
        extra.setdefault(j - 3, []).insert(0, functools.partial(input_terms, j))
    for item in items[:ahead]:
        make_blocks(*item)
    taps_y()
    for j in range(4):
        input_terms(j)
    for step in range(max(hop_step.values()) + 1):
        if step < len(items):
            pass_on(*items[step])
        if step + ahead < len(items):
            make_blocks(*items[step + ahead])
        if 0 <= step - lag < len(items):
            row_done(*items[step - lag])
        for key in sorted(hop_step, key=hop_step.get):
            if hop_step[key] == step:
                hop(*key)
        for run in extra.get(step, ()):
            run()
    input_done()
    taps_done()
    finish("g", DG)
    put_out(DG, dg_hbm)
    finish("v", DV)
    put_out(DV, dv_hbm)
    w.drain(
        {
            "unit": lambda n: U.at[pl.ds(0, n)],
            "tile": lambda n: XB.at[pl.ds(0, n)],
            "edge": lambda n: X.at[0, pl.ds(0, n * EDGE)],
            "og": lambda n: OG.at[pl.ds(0, n * EDGE)],
            "taps": lambda n: TS.at[pl.ds(0, n)],
        },
        me,
    )
    for copy in results:
        copy.wait()
    if len(w.index) != RECEIVES:
        raise ValueError(str(len(w.index)))


RECEIVES = 165


def finisher(din_ref, dg_ref, dv_ref, tt_ref, din_out, dg_out, dv_out, tg_out, tv_out):
    din_out[...] = din_ref[...]
    dg_out[...] = dg_ref[...]
    dv_out[...] = dv_ref[...]
    taps = jnp.concatenate([tt_ref[i] for i in range(8)], axis=1)
    tg_out[...] = taps[0:3]
    tv_out[...] = taps[3:6]


def shards(inputs, gate_proj, value_proj, gate_taps, value_taps, out_grad):
    unit = gate_proj.shape
    cols = unit[1]
    factor = float(TOK * NY * NZ) ** (-0.5)
    vm = pltpu.VMEM
    scratch = [
        vm((8, EXT, FEAT), BF16),
        vm((272, *unit), BF16),
        vm((4 * NX + 3, TOK, FEAT), BF16),
        vm((20, 8, cols), F32),
        vm(gate_taps.shape, F32),
        vm(gate_taps.shape, F32),
        vm((384, TOK), BF16),
        vm((EXT, cols), BF16),
        vm((EXT + 16, cols), F32),
        vm((EXT + 16, cols), F32),
        vm((EXT + 16, cols), F32),
        vm((EXT + 16, cols), F32),
        vm((TOK, cols), BF16),
        vm((TOK, cols), BF16),
        vm((TOK, FEAT), BF16),
        vm(unit, F32),
        vm(unit, F32),
        pltpu.SemaphoreType.DMA((5,)),
        pltpu.SemaphoreType.DMA((RECEIVES,)),
        pltpu.SemaphoreType.DMA((10,)),
    ]
    anywhere = pl.BlockSpec(memory_space=pl.ANY)
    vmem = pl.BlockSpec(memory_space=pltpu.VMEM)
    tile = jax.ShapeDtypeStruct((TOK, FEAT), BF16)
    grad = jax.ShapeDtypeStruct(unit, F32)
    tap = jax.ShapeDtypeStruct(gate_taps.shape, F32)
    sums = pl.pallas_call(
        functools.partial(kernel, factor),
        out_shape=(tile, grad, grad, jax.ShapeDtypeStruct((8, 8, cols), F32)),
        in_specs=[anywhere] * 6,
        out_specs=(anywhere,) * 4,
        scratch_shapes=scratch,
        compiler_params=pltpu.CompilerParams(
            collective_id=0, has_side_effects=True, vmem_limit_bytes=65000 * 1024
        ),
    )(inputs[0], gate_proj, value_proj, gate_taps, value_taps, jnp.swapaxes(out_grad[0], 0, 1))
    din, dg, dv, tg, tv = pl.pallas_call(
        finisher,
        out_shape=(tile, grad, grad, tap, tap),
        in_specs=[vmem] * 4,
        out_specs=(vmem,) * 5,
    )(*sums)
    return din[None], dg, dv, tg, tv


def solution(mesh):
    return jax.shard_map(
        shards,
        mesh=mesh,
        in_specs=(P("rep", "fs", "tp"), P("fs", "tp"), P("fs", "tp"), P(), P(), P("rep", "fs", "tp")),
        out_specs=(P("rep", "fs", "tp"), P("fs", "tp"), P("fs", "tp"), P(), P()),
        check_vma=False,
    )
```

```python
import functools

import jax
import jax.numpy as jnp
from jax import lax
from jax.experimental import pallas as pl
from jax.experimental.pallas import tpu as pltpu
from jax.sharding import PartitionSpec as P

MESH = pl.DeviceIdType.MESH
BF16 = jnp.bfloat16
F32 = jnp.float32

NX, NC, NY, NZ = 4, 2, 4, 16
ZL = 8
TOK = 384
COLS = 352
FEAT = 256
EDGE = 16
EXT = TOK + 2 * EDGE


def right_reach(r):
    return 4 if r < 2 else 3


class Wires:
    def __init__(self, send_sems, recv_sems):
        self.send_sems, self.recv_sems = send_sems, recv_sems
        self.index = {}
        self.count = dict.fromkeys(("unit", "tile", "edge", "og", "taps"), 0)

    def at(self, key):
        return self.index.setdefault(key, len(self.index))

    def copy(self, key, src, dst, to, kind):
        return pltpu.make_async_remote_copy(
            src_ref=src,
            dst_ref=dst,
            send_sem=self.send_sems.at[list(self.count).index(kind)],
            recv_sem=self.recv_sems.at[self.at(key)],
            device_id=to,
            device_id_type=MESH,
        )

    def send(self, key, src, dst, to, kind="unit"):
        self.count[kind] += 1
        self.copy(key, src, dst, to, kind).start()

    def wait(self, key, dst, to, kind="unit"):
        self.copy(key, dst, dst, to, kind).wait_recv()

    def drain(self, spans, to):
        for kind, span in spans.items():
            whole = span(self.count[kind])
            self.copy(("drain",), whole, whole, to, kind).wait_send()


def kernel(
    factor,
    x_hbm, wg_hbm, wv_hbm, gt_hbm, vt_hbm, ogt_hbm,
    din_hbm, dg_hbm, dv_hbm, tout_hbm,
    X, U, XB, TS, GT, VT, OGT, OG, PG, PV, KG, KV, CG, CV, DIN, DG, DV,
    send_sems, recv_sems, local_sems,
):
    def parts_of(pool, sizes):
        first, parts = 0, []
        for size in sizes:
            parts.append(pool.at[pl.ds(first, size)])
            first += size
        return parts

    WG, WV, GG, GV, *rest = parts_of(U, [32] * 4 + [8] * 18)
    FAR, DIR, MID, END, RED = ({"g": rest[2 * i], "v": rest[2 * i + 1]} for i in range(5))
    ends = [(h, way) for h in "gv" for way in (1, -1)]
    LAND, SUMS = dict(zip(ends, rest[10:14])), dict(zip(ends, rest[14:18]))
    IP, IR, IS, ISR = parts_of(XB, [2 * NX, NX, NX, 3])
    TY, TZ1, TB, TT = parts_of(TS, [4, 4, 4, 8])
    rep, fs, tp = lax.axis_index("rep"), lax.axis_index("fs"), lax.axis_index("tp")
    zl, y = lax.div(fs, NY), lax.rem(fs, NY)
    x, c = lax.div(tp, NC), lax.rem(tp, NC)
    zg = rep * ZL + zl

    def dev(x=x, c=c, y=y, z=zg):
        z = lax.rem(z + NZ, NZ)
        return (
            lax.div(z, ZL),
            lax.rem(z, ZL) * NY + lax.rem(y + NY, NY),
            lax.rem(x + NX, NX) * NC + c,
        )

    def blk(dz, dy):
        return lax.rem(zl + dz + ZL, ZL) * NY + lax.rem(y + dy + NY, NY)

    def zrow(dz):
        return lax.rem(zl + dz + 2 * ZL, ZL)

    me = dev()
    right, left = dev(z=zg + 1), dev(z=zg - 1)
    up, down = dev(y=y + 1), dev(y=y - 1)
    partner = dev(c=1 - c)
    after_z = zg + lax.div(y + 1, NY)
    after = dev(y=y + 1, z=after_z)
    before_z = zg - 1 + lax.div(y + NY - 1, NY)
    before = dev(y=y - 1, z=before_z)

    def tp_peer(k):
        return (rep, fs, lax.rem(tp + k + 8, 8))

    zq, zo = lax.div(zg, 4), lax.rem(zg, 4)
    side = 4 * (1 - 2 * lax.rem(zq, 2))

    def z_near(k):
        return dev(z=zq * 4 + lax.rem(zo + k, 4))

    own = blk(0, 0)
    loads = [
        pltpu.make_async_copy(wg_hbm, WG.at[own], local_sems.at[0]),
        pltpu.make_async_copy(wv_hbm, WV.at[own], local_sems.at[1]),
        pltpu.make_async_copy(x_hbm, X.at[tp, pl.ds(EDGE, TOK)], local_sems.at[2]),
        pltpu.make_async_copy(ogt_hbm, OGT.at[pl.ds(0, COLS)], local_sems.at[3]),
        pltpu.make_async_copy(gt_hbm, GT, local_sems.at[4]),
        pltpu.make_async_copy(vt_hbm, VT, local_sems.at[5]),
    ]
    for load in loads:
        load.start()

    barrier = pltpu.get_barrier_semaphore()
    peers = [tp_peer(k) for k in range(1, 8)]
    peers += [dev(y=y + k) for k in (1, 2, 3)]
    peers += [right, left, after, before]
    for peer in peers:
        pl.semaphore_signal(barrier, inc=1, device_id=peer, device_id_type=MESH)
    pl.semaphore_wait(barrier, len(peers))

    w = Wires(send_sems, recv_sems)

    loads[0].wait()
    for dy in (1, 3, 2):
        w.send(("gy", dy), WG.at[own], WG.at[own], dev(y=y + dy))
    loads[1].wait()
    w.send(("vz", 1, 1), WV.at[own], WV.at[own], right)
    w.send(("vz", -1, 1), WV.at[own], WV.at[own], left)
    w.send(("gz", 0, 1, 1), WG.at[own], WG.at[own], right)
    w.send(("gz", 0, -1, 1), WG.at[own], WG.at[own], left)
    loads[2].wait()
    head, tail = X.at[tp, pl.ds(EDGE, EDGE)], X.at[tp, pl.ds(TOK, EDGE)]
    lo, hi = pl.ds(0, EDGE), pl.ds(TOK + EDGE, EDGE)
    w.send(("hx", 1), tail, X.at[tp, lo], after, "edge")
    w.send(("hx", -1), head, X.at[tp, hi], before, "edge")
    mine = X.at[tp, pl.ds(EDGE, TOK)]
    for dx in (1, 3, 2):
        w.send(("x", dx), mine, mine, dev(x=x + dx), "tile")
    w.send(("xp", 0), mine, mine, partner, "tile")
    w.send(("vy", 0, 1), WV.at[own], WV.at[own], up)
    w.send(("vy", 0, -1), WV.at[own], WV.at[own], down)

    def out_grad_rows():
        loads[3].wait()
        for i in range(3):
            for j in range(3):
                block = OGT[128 * i : 128 * i + 128, 128 * j : 128 * j + 128].astype(F32)
                cols = min(128, COLS - 128 * i)
                OG[EDGE + 128 * j : EDGE + 128 * j + 128, 128 * i : 128 * i + cols] = (
                    block.T[:, :cols].astype(BF16)
                )

    def gate_chunk(z, first=False):
        part = jnp.dot(
            X[z],
            WG[pl.ds(z * NY, NY)].reshape(FEAT, COLS),
            preferred_element_type=F32,
        )
        if first:
            PG[8 : 8 + EXT] = part
        else:
            PG[8 : 8 + EXT] += part

    def value_chunk(z, first=False):
        part = jnp.dot(
            X[z],
            WV[pl.ds(z * NY, NY)].reshape(FEAT, COLS),
            preferred_element_type=F32,
        )
        if first:
            PV[8 : 8 + EXT] = part
        else:
            PV[8 : 8 + EXT] += part

    def x_arrived(dx):
        slot = X.at[lax.rem(x - dx + NX, NX) * NC + c, pl.ds(EDGE, TOK)]
        w.wait(("x", dx), slot, me, "tile")
        w.send(("xp", dx), slot, slot, partner, "tile")

    def xp_arrived(dx):
        slot = X.at[lax.rem(x - dx + NX, NX) * NC + 1 - c, pl.ds(EDGE, TOK)]
        w.wait(("xp", dx), slot, me, "tile")

    def edges_spread():
        w.wait(("hx", 1), X.at[tp, lo], me, "edge")
        w.wait(("hx", -1), X.at[tp, hi], me, "edge")
        for k in range(1, 8):
            w.send(("hl",), X.at[tp, lo], X.at[tp, lo], tp_peer(k), "edge")
            w.send(("hl",), X.at[tp, hi], X.at[tp, hi], tp_peer(k), "edge")

    def edges_done():
        w.wait(("hl",), X.at[0, pl.ds(0, 14 * EDGE)], me, "edge")

    def gate_y(dy):
        unit = WG.at[blk(0, -dy)]
        w.wait(("gy", dy), unit, me)
        w.send(("gz", 4 - dy, 1, 1), unit, unit, right)
        w.send(("gz", 4 - dy, -1, 1), unit, unit, left)

    def gate_z(r, d):
        for way, reach, to in ((1, right_reach(r), right), (-1, 7 - right_reach(r), left)):
            if d <= reach:
                unit = WG.at[blk(-way * d, r)]
                w.wait(("gz", r, way, d), unit, me)
                if d < reach:
                    w.send(("gz", r, way, d + 1), unit, unit, to)

    def value_z(d):
        for way, reach, to in ((1, 4, right), (-1, 3, left)):
            if d <= reach:
                dz = -way * d
                unit = WV.at[blk(dz, 0)]
                w.wait(("vz", way, d), unit, me)
                if d < reach:
                    w.send(("vz", way, d + 1), unit, unit, to)
                w.send(("vy", dz, 1), unit, unit, up)
                w.send(("vy", dz, -1), unit, unit, down)
                if d == 4:
                    w.send(("vf", dz), unit, unit, dev(y=y + 2))

    def value_y(dz):
        from_down, from_up = WV.at[blk(dz, -1)], WV.at[blk(dz, 1)]
        w.wait(("vy", dz, 1), from_down, me)
        if dz % 2 == 0 and dz != -4:
            w.send(("vf", dz), from_down, from_down, up)
        w.wait(("vy", dz, -1), from_up, me)
        if dz % 2 == 1:
            w.send(("vf", dz), from_up, from_up, down)

    def value_row(dz, first=False):
        w.wait(("vf", dz), WV.at[blk(dz, 2)], me)
        value_chunk(zrow(dz), first)

    value_z(1)
    gate_y(1)
    gate_y(3)
    gate_y(2)
    gate_z(0, 1)
    value_y(0)
    value_z(2)
    gate_z(3, 1)
    gate_z(1, 1)
    edges_spread()
    gate_z(2, 1)
    value_y(1)
    value_y(-1)
    out_grad_rows()
    gate_z(0, 2)
    value_z(3)
    w.send(("og", 1), OG.at[pl.ds(TOK, EDGE)], OG.at[lo], after, "og")
    w.send(("og", -1), OG.at[pl.ds(EDGE, EDGE)], OG.at[hi], before, "og")
    x_arrived(1)
    x_arrived(3)
    gate_z(3, 2)
    value_y(2)
    value_y(-2)
    gate_z(1, 2)
    gate_z(2, 2)
    gate_z(0, 3)
    value_z(4)
    x_arrived(2)
    gate_z(3, 3)
    value_y(3)
    value_y(-3)
    gate_z(1, 3)
    for dx in (0, 1, 3, 2):
        xp_arrived(dx)
    edges_done()
    gate_chunk(zrow(0), first=True)
    gate_chunk(zrow(1))
    gate_z(2, 3)
    gate_chunk(zrow(-1))
    value_row(0, first=True)
    gate_z(0, 4)
    gate_chunk(zrow(2))
    gate_chunk(zrow(-2))
    value_y(-4)
    gate_z(3, 4)
    value_row(1)
    value_row(-1)
    gate_z(1, 4)
    value_row(2)
    value_row(-2)
    gate_z(2, 4)
    gate_chunk(zrow(3))
    gate_chunk(zrow(-3))
    gate_chunk(zrow(4))
    value_row(3)
    value_row(-3)
    value_row(-4)
    w.wait(("og", 1), OG.at[lo], me, "og")
    w.wait(("og", -1), OG.at[hi], me, "og")

    not_first, not_last = fs > 0, fs < NY * ZL - 1
    for ref in (PG, PV):
        ref[8 : 8 + EDGE] = jnp.where(not_first, ref[8 : 8 + EDGE], 0.0)
        ref[8 + EDGE + TOK : 8 + EXT] = jnp.where(not_last, ref[8 + EDGE + TOK : 8 + EXT], 0.0)
    OG[:EDGE] = jnp.where(not_first, OG[:EDGE].astype(F32), 0.0).astype(BF16)
    OG[EDGE + TOK :] = jnp.where(not_last, OG[EDGE + TOK :].astype(F32), 0.0).astype(BF16)

    loads[4].wait()
    loads[5].wait()
    taps = jnp.concatenate([GT[...], VT[...], jnp.zeros((2, 8 * COLS), F32)], axis=0)
    taps = pltpu.roll(taps, lax.rem((8 - tp) * COLS, 8 * COLS), axis=1)[:, :COLS]
    g0, g1, g2, v0, v1, v2 = (taps[k : k + 1] for k in range(6))

    def rounded(value):
        return value.astype(BF16).astype(F32)

    def cot_rows(i):
        base = pl.multiple_of(i * 16, 16)
        gate = rounded(PG[pl.ds(base, 32)])
        value = rounded(PV[pl.ds(base, 32)])
        gm, gz, gp = gate[7:23], gate[8:24], gate[9:25]
        vm, vz, vp = value[7:23], value[8:24], value[9:25]
        gate_mix = g0 * gm + g1 * gz + g2 * gp
        value_mix = v0 * vm + v1 * vz + v2 * vp
        grad = OG[pl.ds(base, 16)].astype(F32)
        s = jax.nn.sigmoid(gate_mix)
        gate_cot = grad * value_mix * (s * (1.0 + gate_mix * (1.0 - s)))
        value_cot = grad * (gate_mix * s)
        KG[pl.ds(base + 8, 16)] = gate_cot
        KV[pl.ds(base + 8, 16)] = value_cot
        return [
            (p * k).reshape(2, 8, COLS).sum(axis=0)
            for p, k in (
                (gm, gate_cot), (gz, gate_cot), (gp, gate_cot),
                (vm, value_cot), (vz, value_cot), (vp, value_cot),
            )
        ]

    cot_rows(0)
    cot_rows(TOK // 16 + 1)
    zero = jnp.zeros((8, COLS), F32)
    tap_sums = lax.fori_loop(
        1, TOK // 16 + 1,
        lambda i, sums: tuple(a + b for a, b in zip(sums, cot_rows(i))),
        (zero,) * 6,
    )

    def back_rows(i, carry):
        base = pl.multiple_of(i * 16, 16)
        out = pl.ds(pl.multiple_of(i * 16 - 16, 16), 16)
        for source, target, (t0, t1, t2) in ((KG, CG, (g0, g1, g2)), (KV, CV, (v0, v1, v2))):
            cot = source[pl.ds(base, 32)]
            target[out] = (t0 * cot[9:25] + t1 * cot[8:24] + t2 * cot[7:23]).astype(BF16)
        return carry

    lax.fori_loop(1, TOK // 16 + 1, back_rows, 0)

    rows = [jnp.sum(part, axis=0, keepdims=True) for part in tap_sums]
    TY[y] = jnp.concatenate(rows + [jnp.zeros((2, COLS), F32)], axis=0)

    order = (0, 1, -1, 2, -2, 3, -3, 4)
    place = {dz % ZL: k for k, dz in enumerate(order)}
    COT, TERMS = {"g": CG, "v": CV}, {"g": GG, "v": GV}

    def turn(h, k):
        return (1, up, down) if (k % 2 == 0) == (h == "g") else (-1, down, up)

    def make_blocks(h, k):
        dz = order[k]
        z = zrow(dz)
        block = lax.dot_general(
            X[z, EDGE : EDGE + TOK, :], COT[h][...],
            (((0,), (0,)), ((), ())), preferred_element_type=F32,
        )
        TERMS[h][pl.ds(z * NY, NY)] = block.astype(BF16).reshape(NY, 64, COLS)
        way, onward, back = turn(h, k)
        w.send(("far", h, k), TERMS[h].at[blk(dz, 2)], FAR[h].at[k], onward)
        w.send(("dir", h, k), TERMS[h].at[blk(dz, -way)], DIR[h].at[k], back)

    def total(*parts):
        acc = parts[0].astype(F32)
        for part in parts[1:]:
            acc = acc + part.astype(F32)
        return acc

    def pass_on(h, k):
        way, onward, back = turn(h, k)
        w.wait(("far", h, k), FAR[h].at[k], me)
        MID[h][k] = total(FAR[h][k], TERMS[h][blk(order[k], way)]).astype(BF16)
        w.send(("mid", h, k), MID[h].at[k], END[h].at[k], onward)

    def row_done(h, k):
        w.wait(("dir", h, k), DIR[h].at[k], me)
        w.wait(("mid", h, k), END[h].at[k], me)
        RED[h][k] = total(TERMS[h][blk(order[k], 0)], DIR[h][k], END[h][k]).astype(BF16)

    def start_of(h, way):
        return 8 if (h == "g") == (way == 1) else 7

    direct = {"g": {4: (3, 4)}, "v": {5: (4, 5), 4: (3, 4)}}
    starts = {
        (h, way): (start_of(h, way), 3) if h == "g" else (start_of(h, way), 4, 3) for h, way in ends
    }

    def row_at(way, d):
        return place[(way * d) % ZL]

    def hop(h, way, d):
        landing = LAND[h, way]
        k = row_at(way, d)
        if d in starts[h, way]:
            source = RED[h].at[k]
        else:
            w.wait((h, way, d), landing.at[d], me)
            SUMS[h, way][d] = total(landing[d], RED[h][k]).astype(BF16)
            source = SUMS[h, way].at[d]
        slot, to = direct[h].get(d, (d - 1, 1))
        w.send((h, way, slot), source, landing.at[slot], dev(z=zg + way * to))

    def finish(h, out):
        parts = [RED[h][place[0]]]
        for way in (1, -1):
            for slot in [0] + [slot for slot, _ in direct[h].values()]:
                w.wait((h, way, slot), LAND[h, way].at[slot], me)
                parts.append(LAND[h, way][slot])
        out[...] = total(*parts) * factor

    def input_terms(j):
        part = lax.dot_general(
            CG[...], WG[NY * j : NY * j + NY].reshape(FEAT, COLS),
            (((1,), (1,)), ((), ())), preferred_element_type=F32,
        ) + lax.dot_general(
            CV[...], WV[NY * j : NY * j + NY].reshape(FEAT, COLS),
            (((1,), (1,)), ((), ())), preferred_element_type=F32,
        )
        IP[NX * (j % 2) + j // 2] = part.astype(BF16)

    def input_swap():
        for i in range(NX):
            w.send(("ip", i), IP.at[NX * (1 - c) + i], IR.at[i], partner, "tile")

    def input_sums():
        for i in range(NX):
            w.wait(("ip", i), IR.at[i], me, "tile")
            IS[i] = total(IP[NX * c + i], IR[i]).astype(BF16)
        for dx in (1, 3, 2):
            w.send(("is", dx), IS.at[lax.rem(x + dx, NX)], ISR.at[dx - 1], dev(x=x + dx), "tile")

    results = []

    def put_out(source, target):
        copy = pltpu.make_async_copy(source, target, local_sems.at[6 + len(results)])
        copy.start()
        results.append(copy)

    def input_done():
        for dx in (1, 3, 2):
            w.wait(("is", dx), ISR.at[dx - 1], me, "tile")
        DIN[...] = total(IP[NX * c + x], IR[x], ISR[0], ISR[1], ISR[2]).astype(BF16)
        put_out(DIN, din_hbm)

    def taps_y():
        for dy in (1, 2, 3):
            w.send(("ty",), TY.at[y], TY.at[y], dev(y=y + dy), "taps")

    def taps_z():
        w.wait(("ty",), TY.at[pl.ds(0, 3)], me, "taps")
        TZ1[zo] = TY[0] + TY[1] + TY[2] + TY[3]
        for k in (1, 2, 3):
            w.send(("tz",), TZ1.at[zo], TZ1.at[zo], z_near(k), "taps")

    def taps_pair(stage):
        if stage == 0:
            w.wait(("tz",), TZ1.at[pl.ds(0, 3)], me, "taps")
            TB[0] = TZ1[0] + TZ1[1] + TZ1[2] + TZ1[3]
            w.send(("tb", 0), TB.at[0], TB.at[1], dev(z=zg + side), "taps")
        else:
            w.wait(("tb", 0), TB.at[1], me, "taps")
            TB[2] = TB[0] + TB[1]
            w.send(("tb", 1), TB.at[2], TB.at[3], dev(z=zg - side), "taps")

    def taps_spread():
        w.wait(("tb", 1), TB.at[3], me, "taps")
        TT[tp] = (TB[2] + TB[3]) * factor
        for k in range(1, 8):
            w.send(("tt",), TT.at[tp], TT.at[tp], tp_peer(k), "taps")

    def taps_done():
        w.wait(("tt",), TT.at[pl.ds(0, 7)], me, "taps")
        put_out(TT, tout_hbm)

    items = [("v", k) for k in range(3)] + [("g", k) for k in range(ZL)] + [("v", k) for k in range(3, ZL)]
    ahead, lag, spacing = 4, 3, 3
    row_step = {item: t + lag for t, item in enumerate(items)}
    hop_step = {}
    for h, way in ends:
        for d in range(start_of(h, way), 0, -1):
            step = row_step[h, row_at(way, d)]
            if d not in starts[h, way]:
                step = max(step, hop_step[h, way, d + 1] + spacing)
            hop_step[h, way, d] = step
    extra = {4: [taps_z], 5: [input_swap], 8: [lambda: taps_pair(0)], 9: [input_sums], 13: [lambda: taps_pair(1)],
             19: [taps_spread]}
    for j in range(4, 8):
        extra.setdefault(j - 3, []).insert(0, functools.partial(input_terms, j))
    for item in items[:ahead]:
        make_blocks(*item)
    taps_y()
    for j in range(4):
        input_terms(j)
    for step in range(max(hop_step.values()) + 1):
        if step < len(items):
            pass_on(*items[step])
        if step + ahead < len(items):
            make_blocks(*items[step + ahead])
        if 0 <= step - lag < len(items):
            row_done(*items[step - lag])
        for key in sorted(hop_step, key=hop_step.get):
            if hop_step[key] == step:
                hop(*key)
        for run in extra.get(step, ()):
            run()
    input_done()
    taps_done()
    finish("g", DG)
    put_out(DG, dg_hbm)
    finish("v", DV)
    put_out(DV, dv_hbm)
    w.drain(
        {
            "unit": lambda n: U.at[pl.ds(0, n)],
            "tile": lambda n: XB.at[pl.ds(0, n)],
            "edge": lambda n: X.at[0, pl.ds(0, n * EDGE)],
            "og": lambda n: OG.at[pl.ds(0, n * EDGE)],
            "taps": lambda n: TS.at[pl.ds(0, n)],
        },
        me,
    )
    for copy in results:
        copy.wait()
    if len(w.index) != RECEIVES:
        raise ValueError(str(len(w.index)))


RECEIVES = 165


def finisher(din_ref, dg_ref, dv_ref, tt_ref, din_out, dg_out, dv_out, tg_out, tv_out):
    din_out[...] = din_ref[...]
    dg_out[...] = dg_ref[...]
    dv_out[...] = dv_ref[...]
    taps = jnp.concatenate([tt_ref[i] for i in range(8)], axis=1)
    tg_out[...] = taps[0:3]
    tv_out[...] = taps[3:6]


def shards(inputs, gate_proj, value_proj, gate_taps, value_taps, out_grad):
    unit = gate_proj.shape
    cols = unit[1]
    factor = float(TOK * NY * NZ) ** (-0.5)
    vm = pltpu.VMEM
    scratch = [
        vm((8, EXT, FEAT), BF16),
        vm((272, *unit), BF16),
        vm((4 * NX + 3, TOK, FEAT), BF16),
        vm((20, 8, cols), F32),
        vm(gate_taps.shape, F32),
        vm(gate_taps.shape, F32),
        vm((384, TOK), BF16),
        vm((EXT, cols), BF16),
        vm((EXT + 16, cols), F32),
        vm((EXT + 16, cols), F32),
        vm((EXT + 16, cols), F32),
        vm((EXT + 16, cols), F32),
        vm((TOK, cols), BF16),
        vm((TOK, cols), BF16),
        vm((TOK, FEAT), BF16),
        vm(unit, F32),
        vm(unit, F32),
        pltpu.SemaphoreType.DMA((5,)),
        pltpu.SemaphoreType.DMA((RECEIVES,)),
        pltpu.SemaphoreType.DMA((10,)),
    ]
    anywhere = pl.BlockSpec(memory_space=pl.ANY)
    vmem = pl.BlockSpec(memory_space=pltpu.VMEM)
    tile = jax.ShapeDtypeStruct((TOK, FEAT), BF16)
    grad = jax.ShapeDtypeStruct(unit, F32)
    tap = jax.ShapeDtypeStruct(gate_taps.shape, F32)
    sums = pl.pallas_call(
        functools.partial(kernel, factor),
        out_shape=(tile, grad, grad, jax.ShapeDtypeStruct((8, 8, cols), F32)),
        in_specs=[anywhere] * 6,
        out_specs=(anywhere,) * 4,
        scratch_shapes=scratch,
        compiler_params=pltpu.CompilerParams(
            collective_id=0, has_side_effects=True, vmem_limit_bytes=65000 * 1024
        ),
    )(inputs[0], gate_proj, value_proj, gate_taps, value_taps, jnp.swapaxes(out_grad[0], 0, 1))
    din, dg, dv, tg, tv = pl.pallas_call(
        finisher,
        out_shape=(tile, grad, grad, tap, tap),
        in_specs=[vmem] * 4,
        out_specs=(vmem,) * 5,
    )(*sums)
    return din[None], dg, dv, tg, tv


def solution(mesh):
    return jax.shard_map(
        shards,
        mesh=mesh,
        in_specs=(P("rep", "fs", "tp"), P("fs", "tp"), P("fs", "tp"), P(), P(), P("rep", "fs", "tp")),
        out_specs=(P("rep", "fs", "tp"), P("fs", "tp"), P("fs", "tp"), P(), P()),
        check_vma=False,
    )
```

```python
import functools

import jax
import jax.numpy as jnp
from jax import lax
from jax.experimental import pallas as pl
from jax.experimental.pallas import tpu as pltpu
from jax.sharding import PartitionSpec as P

MESH = pl.DeviceIdType.MESH
BF16 = jnp.bfloat16
F32 = jnp.float32

NX, NC, NY, NZ = 4, 2, 4, 16
ZL = 8
TOK = 384
COLS = 352
FEAT = 256
EDGE = 16
EXT = TOK + 2 * EDGE


def right_reach(r):
    return 4 if r < 2 else 3


class Wires:
    def __init__(self, send_sems, recv_sems):
        self.send_sems, self.recv_sems = send_sems, recv_sems
        self.index = {}
        self.count = dict.fromkeys(("unit", "tile", "edge", "og", "taps"), 0)

    def at(self, key):
        return self.index.setdefault(key, len(self.index))

    def copy(self, key, src, dst, to, kind):
        return pltpu.make_async_remote_copy(
            src_ref=src,
            dst_ref=dst,
            send_sem=self.send_sems.at[list(self.count).index(kind)],
            recv_sem=self.recv_sems.at[self.at(key)],
            device_id=to,
            device_id_type=MESH,
        )

    def send(self, key, src, dst, to, kind="unit", amount=1):
        self.count[kind] += amount
        self.copy(key, src, dst, to, kind).start()

    def wait(self, key, dst, to, kind="unit"):
        self.copy(key, dst, dst, to, kind).wait_recv()

    def drain(self, spans, to):
        for kind, span in spans.items():
            whole = span(int(self.count[kind]))
            self.copy(("drain",), whole, whole, to, kind).wait_send()


def kernel(
    factor,
    x_hbm, wg_hbm, wv_hbm, gt_hbm, vt_hbm, ogt_hbm,
    din_hbm, dg_hbm, dv_hbm, tout_hbm,
    X, U, XB, TS, GT, VT, OGT, OG, PG, PV, KG, KV, CG, CV, DIN, DG, DV,
    send_sems, recv_sems, local_sems,
):
    def parts_of(pool, sizes):
        first, parts = 0, []
        for size in sizes:
            parts.append(pool.at[pl.ds(first, size)])
            first += size
        return parts

    WG, WV, GG, GV, *rest = parts_of(U, [32] * 4 + [8] * 18)
    FAR, DIR, MID, END, RED = ({"g": rest[2 * i], "v": rest[2 * i + 1]} for i in range(5))
    ends = [(h, way) for h in "gv" for way in (1, -1)]
    LAND, SUMS = dict(zip(ends, rest[10:14])), dict(zip(ends, rest[14:18]))
    IP, IR, IS, ISR = parts_of(XB, [2 * NX, NX, NX, 3])
    TY, TZ1, TB, TT = parts_of(TS, [4, 4, 4, 8])
    rep, fs, tp = lax.axis_index("rep"), lax.axis_index("fs"), lax.axis_index("tp")
    zl, y = lax.div(fs, NY), lax.rem(fs, NY)
    x, c = lax.div(tp, NC), lax.rem(tp, NC)
    zg = rep * ZL + zl

    def dev(x=x, c=c, y=y, z=zg):
        z = lax.rem(z + NZ, NZ)
        return (
            lax.div(z, ZL),
            lax.rem(z, ZL) * NY + lax.rem(y + NY, NY),
            lax.rem(x + NX, NX) * NC + c,
        )

    def blk(dz, dy):
        return lax.rem(zl + dz + ZL, ZL) * NY + lax.rem(y + dy + NY, NY)

    def zrow(dz):
        return lax.rem(zl + dz + 2 * ZL, ZL)

    me = dev()
    right, left = dev(z=zg + 1), dev(z=zg - 1)
    up, down = dev(y=y + 1), dev(y=y - 1)
    partner = dev(c=1 - c)
    after_z = zg + lax.div(y + 1, NY)
    after = dev(y=y + 1, z=after_z)
    before_z = zg - 1 + lax.div(y + NY - 1, NY)
    before = dev(y=y - 1, z=before_z)

    def tp_peer(k):
        return (rep, fs, lax.rem(tp + k + 8, 8))

    zq, zo = lax.div(zg, 4), lax.rem(zg, 4)
    side = 4 * (1 - 2 * lax.rem(zq, 2))

    def z_near(k):
        return dev(z=zq * 4 + lax.rem(zo + k, 4))

    own = blk(0, 0)
    loads = [
        pltpu.make_async_copy(wg_hbm, WG.at[own], local_sems.at[0]),
        pltpu.make_async_copy(wv_hbm, WV.at[own], local_sems.at[1]),
        pltpu.make_async_copy(x_hbm, X.at[tp, pl.ds(EDGE, TOK)], local_sems.at[2]),
        pltpu.make_async_copy(ogt_hbm, OGT.at[pl.ds(0, COLS)], local_sems.at[3]),
        pltpu.make_async_copy(gt_hbm, GT, local_sems.at[4]),
        pltpu.make_async_copy(vt_hbm, VT, local_sems.at[5]),
    ]
    for load in loads:
        load.start()

    barrier = pltpu.get_barrier_semaphore()
    peers = [tp_peer(k) for k in range(1, 8)]
    peers += [dev(y=y + k) for k in (1, 2, 3)]
    peers += [right, left, after, before]
    for peer in peers:
        pl.semaphore_signal(barrier, inc=1, device_id=peer, device_id_type=MESH)
    pl.semaphore_wait(barrier, len(peers))

    w = Wires(send_sems, recv_sems)

    loads[0].wait()
    for dy in (1, 3, 2):
        w.send(("gy", dy), WG.at[own], WG.at[own], dev(y=y + dy))
    loads[1].wait()
    w.send(("vz", 1, 1), WV.at[own], WV.at[own], right)
    w.send(("vz", -1, 1), WV.at[own], WV.at[own], left)
    w.send(("gz", 0, 1, 1), WG.at[own], WG.at[own], right)
    w.send(("gz", 0, -1, 1), WG.at[own], WG.at[own], left)
    loads[2].wait()
    head, tail = X.at[tp, pl.ds(EDGE, EDGE)], X.at[tp, pl.ds(TOK, EDGE)]
    lo, hi = pl.ds(0, EDGE), pl.ds(TOK + EDGE, EDGE)
    w.send(("hx", 1), tail, X.at[tp, lo], after, "edge")
    w.send(("hx", -1), head, X.at[tp, hi], before, "edge")
    mine = X.at[tp, pl.ds(EDGE, TOK)]
    HALF = TOK // 2

    def half_of(dx, i):
        return X.at[lax.rem(x - dx + NX, NX) * NC + c, pl.ds(EDGE + HALF * i, HALF)]

    for i in (0, 1):
        for way, part in ((1, half_of(0, i)), (-1, half_of(0, 1 - i))):
            w.send(("x", way, i), part, part, dev(x=x + way), "tile", 0.5)
    w.send(("xp", 0), mine, mine, partner, "tile")
    w.send(("vy", 0, 1), WV.at[own], WV.at[own], up)
    w.send(("vy", 0, -1), WV.at[own], WV.at[own], down)

    def out_grad_rows():
        loads[3].wait()
        for i in range(3):
            for j in range(3):
                block = OGT[128 * i : 128 * i + 128, 128 * j : 128 * j + 128].astype(F32)
                cols = min(128, COLS - 128 * i)
                OG[EDGE + 128 * j : EDGE + 128 * j + 128, 128 * i : 128 * i + cols] = (
                    block.T[:, :cols].astype(BF16)
                )

    def rounded(value):
        return value.astype(BF16).astype(F32)

    def gate_chunk(z, first=False, last=False):
        part = jnp.dot(
            X[z],
            WG[pl.ds(z * NY, NY)].reshape(FEAT, COLS),
            preferred_element_type=F32,
        )
        if first:
            PG[8 : 8 + EXT] = part
        elif last:
            PG[8 : 8 + EXT] = rounded(PG[8 : 8 + EXT] + part)
        else:
            PG[8 : 8 + EXT] += part

    def value_chunk(z, first=False, last=False):
        part = jnp.dot(
            X[z],
            WV[pl.ds(z * NY, NY)].reshape(FEAT, COLS),
            preferred_element_type=F32,
        )
        if first:
            PV[8 : 8 + EXT] = part
        elif last:
            PV[8 : 8 + EXT] = rounded(PV[8 : 8 + EXT] + part)
        else:
            PV[8 : 8 + EXT] += part

    def x_first():
        for way in (1, -1):
            part = half_of(way, (1 - way) // 2)
            w.wait(("x", way, 0), part, me, "tile")
            w.send(("x2", way), part, part, dev(x=x + way), "tile", 0.5)

    def x_whole(dx):
        slot = X.at[lax.rem(x - dx + NX, NX) * NC + c, pl.ds(EDGE, TOK)]
        w.send(("xp", dx), slot, slot, partner, "tile")

    def x_near():
        for way in (1, -1):
            w.wait(("x", way, 1), half_of(way, (1 + way) // 2), me, "tile")
            x_whole(way)

    def x_far():
        for way in (1, -1):
            w.wait(("x2", way), half_of(2, (1 - way) // 2), me, "tile")
        x_whole(2)

    def xp_arrived(dx):
        slot = X.at[lax.rem(x - dx + NX, NX) * NC + 1 - c, pl.ds(EDGE, TOK)]
        w.wait(("xp", dx), slot, me, "tile")

    def edges_spread():
        w.wait(("hx", 1), X.at[tp, lo], me, "edge")
        w.wait(("hx", -1), X.at[tp, hi], me, "edge")
        for k in range(1, 8):
            w.send(("hl",), X.at[tp, lo], X.at[tp, lo], tp_peer(k), "edge")
            w.send(("hl",), X.at[tp, hi], X.at[tp, hi], tp_peer(k), "edge")

    def edges_done():
        w.wait(("hl",), X.at[0, pl.ds(0, 14 * EDGE)], me, "edge")

    def gate_y(dy):
        unit = WG.at[blk(0, -dy)]
        w.wait(("gy", dy), unit, me)
        w.send(("gz", 4 - dy, 1, 1), unit, unit, right)
        w.send(("gz", 4 - dy, -1, 1), unit, unit, left)

    def gate_z(r, d):
        for way, reach, to in ((1, right_reach(r), right), (-1, 7 - right_reach(r), left)):
            if d <= reach:
                unit = WG.at[blk(-way * d, r)]
                w.wait(("gz", r, way, d), unit, me)
                if d < reach:
                    w.send(("gz", r, way, d + 1), unit, unit, to)

    def value_z(d):
        for way, reach, to in ((1, 4, right), (-1, 3, left)):
            if d <= reach:
                dz = -way * d
                unit = WV.at[blk(dz, 0)]
                w.wait(("vz", way, d), unit, me)
                if d < reach:
                    w.send(("vz", way, d + 1), unit, unit, to)
                w.send(("vy", dz, 1), unit, unit, up)
                w.send(("vy", dz, -1), unit, unit, down)
                if d == 4:
                    w.send(("vf", dz), unit, unit, dev(y=y + 2))

    def value_y(dz):
        from_down, from_up = WV.at[blk(dz, -1)], WV.at[blk(dz, 1)]
        w.wait(("vy", dz, 1), from_down, me)
        if dz % 2 == 0 and dz != -4:
            w.send(("vf", dz), from_down, from_down, up)
        w.wait(("vy", dz, -1), from_up, me)
        if dz % 2 == 1:
            w.send(("vf", dz), from_up, from_up, down)

    def value_row(dz, first=False, last=False):
        w.wait(("vf", dz), WV.at[blk(dz, 2)], me)
        value_chunk(zrow(dz), first, last)

    value_z(1)
    gate_y(1)
    gate_y(3)
    gate_y(2)
    gate_z(0, 1)
    value_y(0)
    value_z(2)
    gate_z(3, 1)
    x_first()
    gate_z(1, 1)
    edges_spread()
    gate_z(2, 1)
    value_y(1)
    value_y(-1)
    x_near()
    out_grad_rows()
    gate_z(0, 2)
    value_z(3)
    w.send(("og", 1), OG.at[pl.ds(TOK, EDGE)], OG.at[lo], after, "og")
    w.send(("og", -1), OG.at[pl.ds(EDGE, EDGE)], OG.at[hi], before, "og")
    gate_z(3, 2)
    value_y(2)
    value_y(-2)
    gate_z(1, 2)
    x_far()
    gate_z(2, 2)
    gate_z(0, 3)
    value_z(4)
    for dx in (0, 1, -1, 2):
        xp_arrived(dx)
    edges_done()
    gate_chunk(zrow(0), first=True)
    gate_chunk(zrow(1))
    gate_z(3, 3)
    gate_chunk(zrow(-1))
    value_y(3)
    value_y(-3)
    gate_z(1, 3)
    value_row(0, first=True)
    gate_chunk(zrow(2))
    gate_z(2, 3)
    gate_chunk(zrow(-2))
    value_row(1)
    gate_z(0, 4)
    value_row(-1)
    value_row(2)
    gate_chunk(zrow(3))
    gate_z(3, 4)
    value_row(-2)
    gate_chunk(zrow(-3))
    value_y(-4)
    value_row(3)
    gate_z(1, 4)
    value_row(-3)
    value_row(-4, last=True)
    gate_z(2, 4)
    gate_chunk(zrow(4), last=True)
    w.wait(("og", 1), OG.at[lo], me, "og")
    w.wait(("og", -1), OG.at[hi], me, "og")

    not_first, not_last = fs > 0, fs < NY * ZL - 1
    for ref in (PG, PV):
        ref[8 : 8 + EDGE] = jnp.where(not_first, ref[8 : 8 + EDGE], 0.0)
        ref[8 + EDGE + TOK : 8 + EXT] = jnp.where(not_last, ref[8 + EDGE + TOK : 8 + EXT], 0.0)
    OG[:EDGE] = jnp.where(not_first, OG[:EDGE].astype(F32), 0.0).astype(BF16)
    OG[EDGE + TOK :] = jnp.where(not_last, OG[EDGE + TOK :].astype(F32), 0.0).astype(BF16)

    loads[4].wait()
    loads[5].wait()
    taps = jnp.concatenate([GT[...], VT[...], jnp.zeros((2, 8 * COLS), F32)], axis=0)
    taps = pltpu.roll(taps, lax.rem((8 - tp) * COLS, 8 * COLS), axis=1)[:, :COLS]
    g0, g1, g2, v0, v1, v2 = (taps[k : k + 1] for k in range(6))

    def cot_rows(i):
        base = pl.multiple_of(i * 16, 16)
        gate = PG[pl.ds(base, 32)]
        value = PV[pl.ds(base, 32)]
        gm, gz, gp = gate[7:23], gate[8:24], gate[9:25]
        vm, vz, vp = value[7:23], value[8:24], value[9:25]
        gate_mix = g0 * gm + g1 * gz + g2 * gp
        value_mix = v0 * vm + v1 * vz + v2 * vp
        grad = OG[pl.ds(base, 16)].astype(F32)
        s = jax.nn.sigmoid(gate_mix)
        gate_cot = grad * value_mix * (s * (1.0 + gate_mix * (1.0 - s)))
        value_cot = grad * (gate_mix * s)
        KG[pl.ds(base + 8, 16)] = gate_cot
        KV[pl.ds(base + 8, 16)] = value_cot
        return [
            (p * k).reshape(2, 8, COLS).sum(axis=0)
            for p, k in (
                (gm, gate_cot), (gz, gate_cot), (gp, gate_cot),
                (vm, value_cot), (vz, value_cot), (vp, value_cot),
            )
        ]

    cot_rows(0)
    cot_rows(TOK // 16 + 1)
    zero = jnp.zeros((8, COLS), F32)
    tap_sums = lax.fori_loop(
        1, TOK // 16 + 1,
        lambda i, sums: tuple(a + b for a, b in zip(sums, cot_rows(i))),
        (zero,) * 6,
    )

    def back_rows(i, carry):
        base = pl.multiple_of(i * 16, 16)
        out = pl.ds(pl.multiple_of(i * 16 - 16, 16), 16)
        for source, target, (t0, t1, t2) in ((KG, CG, (g0, g1, g2)), (KV, CV, (v0, v1, v2))):
            cot = source[pl.ds(base, 32)]
            target[out] = (t0 * cot[9:25] + t1 * cot[8:24] + t2 * cot[7:23]).astype(BF16)
        return carry

    lax.fori_loop(1, TOK // 16 + 1, back_rows, 0)

    rows = [jnp.sum(part, axis=0, keepdims=True) for part in tap_sums]
    TY[y] = jnp.concatenate(rows + [jnp.zeros((2, COLS), F32)], axis=0)

    order = (0, 1, -1, 2, -2, 3, -3, 4)
    place = {dz % ZL: k for k, dz in enumerate(order)}
    COT, TERMS = {"g": CG, "v": CV}, {"g": GG, "v": GV}

    def turn(h, k):
        return (1, up, down) if (k % 2 == 0) == (h == "g") else (-1, down, up)

    def make_blocks(h, k):
        dz = order[k]
        z = zrow(dz)
        block = lax.dot_general(
            X[z, EDGE : EDGE + TOK, :], COT[h][...],
            (((0,), (0,)), ((), ())), preferred_element_type=F32,
        )
        TERMS[h][pl.ds(z * NY, NY)] = block.astype(BF16).reshape(NY, 64, COLS)
        way, onward, back = turn(h, k)
        w.send(("far", h, k), TERMS[h].at[blk(dz, 2)], FAR[h].at[k], onward)
        w.send(("dir", h, k), TERMS[h].at[blk(dz, -way)], DIR[h].at[k], back)

    def total(*parts):
        acc = parts[0].astype(F32)
        for part in parts[1:]:
            acc = acc + part.astype(F32)
        return acc

    def pass_on(h, k):
        way, onward, back = turn(h, k)
        w.wait(("far", h, k), FAR[h].at[k], me)
        MID[h][k] = total(FAR[h][k], TERMS[h][blk(order[k], way)]).astype(BF16)
        w.send(("mid", h, k), MID[h].at[k], END[h].at[k], onward)

    def row_done(h, k):
        w.wait(("dir", h, k), DIR[h].at[k], me)
        w.wait(("mid", h, k), END[h].at[k], me)
        RED[h][k] = total(TERMS[h][blk(order[k], 0)], DIR[h][k], END[h][k]).astype(BF16)

    def start_of(h, way):
        return 8 if (h == "g") == (way == 1) else 7

    direct = {4: (3, 4)}
    starts = {(h, way): (start_of(h, way), 3) for h, way in ends}

    def row_at(way, d):
        return place[(way * d) % ZL]

    def hop(h, way, d):
        landing = LAND[h, way]
        k = row_at(way, d)
        if d in starts[h, way]:
            source = RED[h].at[k]
        else:
            w.wait((h, way, d), landing.at[d], me)
            SUMS[h, way][d] = total(landing[d], RED[h][k]).astype(BF16)
            source = SUMS[h, way].at[d]
        slot, to = direct.get(d, (d - 1, 1))
        w.send((h, way, slot), source, landing.at[slot], dev(z=zg + way * to))

    def finish(h, out):
        parts = [RED[h][place[0]]]
        for way in (1, -1):
            for slot in [0] + [slot for slot, _ in direct.values()]:
                w.wait((h, way, slot), LAND[h, way].at[slot], me)
                parts.append(LAND[h, way][slot])
        out[...] = total(*parts) * factor

    def input_terms(j):
        part = lax.dot_general(
            CG[...], WG[NY * j : NY * j + NY].reshape(FEAT, COLS),
            (((1,), (1,)), ((), ())), preferred_element_type=F32,
        ) + lax.dot_general(
            CV[...], WV[NY * j : NY * j + NY].reshape(FEAT, COLS),
            (((1,), (1,)), ((), ())), preferred_element_type=F32,
        )
        IP[NX * (j % 2) + j // 2] = part.astype(BF16)

    def input_swap():
        for i in range(NX):
            w.send(("ip", i), IP.at[NX * (1 - c) + i], IR.at[i], partner, "tile")

    def input_sums():
        for i in range(NX):
            w.wait(("ip", i), IR.at[i], me, "tile")
            IS[i] = total(IP[NX * c + i], IR[i]).astype(BF16)
        for dx in (1, 3, 2):
            w.send(("is", dx), IS.at[lax.rem(x + dx, NX)], ISR.at[dx - 1], dev(x=x + dx), "tile")

    results = []

    def put_out(source, target):
        copy = pltpu.make_async_copy(source, target, local_sems.at[6 + len(results)])
        copy.start()
        results.append(copy)

    def input_done():
        for dx in (1, 3, 2):
            w.wait(("is", dx), ISR.at[dx - 1], me, "tile")
        DIN[...] = total(IP[NX * c + x], IR[x], ISR[0], ISR[1], ISR[2]).astype(BF16)
        put_out(DIN, din_hbm)

    def taps_y():
        for dy in (1, 2, 3):
            w.send(("ty",), TY.at[y], TY.at[y], dev(y=y + dy), "taps")

    def taps_z():
        w.wait(("ty",), TY.at[pl.ds(0, 3)], me, "taps")
        TZ1[zo] = TY[0] + TY[1] + TY[2] + TY[3]
        for k in (1, 2, 3):
            w.send(("tz",), TZ1.at[zo], TZ1.at[zo], z_near(k), "taps")

    def taps_pair(stage):
        if stage == 0:
            w.wait(("tz",), TZ1.at[pl.ds(0, 3)], me, "taps")
            TB[0] = TZ1[0] + TZ1[1] + TZ1[2] + TZ1[3]
            w.send(("tb", 0), TB.at[0], TB.at[1], dev(z=zg + side), "taps")
        else:
            w.wait(("tb", 0), TB.at[1], me, "taps")
            TB[2] = TB[0] + TB[1]
            w.send(("tb", 1), TB.at[2], TB.at[3], dev(z=zg - side), "taps")

    def taps_spread():
        w.wait(("tb", 1), TB.at[3], me, "taps")
        TT[tp] = (TB[2] + TB[3]) * factor
        for k in range(1, 8):
            w.send(("tt",), TT.at[tp], TT.at[tp], tp_peer(k), "taps")

    def taps_done():
        w.wait(("tt",), TT.at[pl.ds(0, 7)], me, "taps")
        put_out(TT, tout_hbm)

    items = [(h, k) for k in range(5) for h in "gv"]
    items += [(h, k) for h in "gv" for k in (5, 6, 7)]
    ahead, lag, spacing = 4, 3, 3
    row_step = {item: t + lag for t, item in enumerate(items)}
    hop_step = {}
    for h, way in ends:
        for d in range(start_of(h, way), 0, -1):
            step = row_step[h, row_at(way, d)]
            if d not in starts[h, way]:
                step = max(step, hop_step[h, way, d + 1] + spacing)
            hop_step[h, way, d] = step
    extra = {4: [taps_z], 5: [input_swap], 8: [lambda: taps_pair(0)], 9: [input_sums], 13: [lambda: taps_pair(1)],
             19: [taps_spread]}
    for j in range(4, 8):
        extra.setdefault(j - 3, []).insert(0, functools.partial(input_terms, j))
    for item in items[:ahead]:
        make_blocks(*item)
    taps_y()
    for j in range(4):
        input_terms(j)
    for step in range(max(hop_step.values()) + 1):
        if step < len(items):
            pass_on(*items[step])
        if step + ahead < len(items):
            make_blocks(*items[step + ahead])
        if 0 <= step - lag < len(items):
            row_done(*items[step - lag])
        for key in sorted(hop_step, key=hop_step.get):
            if hop_step[key] == step:
                hop(*key)
        for run in extra.get(step, ()):
            run()
    input_done()
    taps_done()
    finish("g", DG)
    put_out(DG, dg_hbm)
    finish("v", DV)
    put_out(DV, dv_hbm)
    w.drain(
        {
            "unit": lambda n: U.at[pl.ds(0, n)],
            "tile": lambda n: XB.at[pl.ds(0, n)],
            "edge": lambda n: X.at[0, pl.ds(0, n * EDGE)],
            "og": lambda n: OG.at[pl.ds(0, n * EDGE)],
            "taps": lambda n: TS.at[pl.ds(0, n)],
        },
        me,
    )
    for copy in results:
        copy.wait()
    if len(w.index) != RECEIVES:
        raise ValueError(str(len(w.index)))


RECEIVES = 168


def finisher(din_ref, dg_ref, dv_ref, tt_ref, din_out, dg_out, dv_out, tg_out, tv_out):
    din_out[...] = din_ref[...]
    dg_out[...] = dg_ref[...]
    dv_out[...] = dv_ref[...]
    taps = jnp.concatenate([tt_ref[i] for i in range(8)], axis=1)
    tg_out[...] = taps[0:3]
    tv_out[...] = taps[3:6]


def shards(inputs, gate_proj, value_proj, gate_taps, value_taps, out_grad):
    unit = gate_proj.shape
    cols = unit[1]
    factor = float(TOK * NY * NZ) ** (-0.5)
    vm = pltpu.VMEM
    scratch = [
        vm((8, EXT, FEAT), BF16),
        vm((272, *unit), BF16),
        vm((4 * NX + 3, TOK, FEAT), BF16),
        vm((20, 8, cols), F32),
        vm(gate_taps.shape, F32),
        vm(gate_taps.shape, F32),
        vm((384, TOK), BF16),
        vm((EXT, cols), BF16),
        vm((EXT + 16, cols), F32),
        vm((EXT + 16, cols), F32),
        vm((EXT + 16, cols), F32),
        vm((EXT + 16, cols), F32),
        vm((TOK, cols), BF16),
        vm((TOK, cols), BF16),
        vm((TOK, FEAT), BF16),
        vm(unit, F32),
        vm(unit, F32),
        pltpu.SemaphoreType.DMA((5,)),
        pltpu.SemaphoreType.DMA((RECEIVES,)),
        pltpu.SemaphoreType.DMA((10,)),
    ]
    anywhere = pl.BlockSpec(memory_space=pl.ANY)
    vmem = pl.BlockSpec(memory_space=pltpu.VMEM)
    tile = jax.ShapeDtypeStruct((TOK, FEAT), BF16)
    grad = jax.ShapeDtypeStruct(unit, F32)
    tap = jax.ShapeDtypeStruct(gate_taps.shape, F32)
    sums = pl.pallas_call(
        functools.partial(kernel, factor),
        out_shape=(tile, grad, grad, jax.ShapeDtypeStruct((8, 8, cols), F32)),
        in_specs=[anywhere] * 6,
        out_specs=(anywhere,) * 4,
        scratch_shapes=scratch,
        compiler_params=pltpu.CompilerParams(
            collective_id=0, has_side_effects=True, vmem_limit_bytes=65000 * 1024
        ),
    )(inputs[0], gate_proj, value_proj, gate_taps, value_taps, jnp.swapaxes(out_grad[0], 0, 1))
    din, dg, dv, tg, tv = pl.pallas_call(
        finisher,
        out_shape=(tile, grad, grad, tap, tap),
        in_specs=[vmem] * 4,
        out_specs=(vmem,) * 5,
    )(*sums)
    return din[None], dg, dv, tg, tv


def solution(mesh):
    return jax.shard_map(
        shards,
        mesh=mesh,
        in_specs=(P("rep", "fs", "tp"), P("fs", "tp"), P("fs", "tp"), P(), P(), P("rep", "fs", "tp")),
        out_specs=(P("rep", "fs", "tp"), P("fs", "tp"), P("fs", "tp"), P(), P()),
        check_vma=False,
    )
```

```python
import functools

import jax
import jax.numpy as jnp
from jax import lax
from jax.experimental import pallas as pl
from jax.experimental.pallas import tpu as pltpu
from jax.sharding import PartitionSpec as P

MESH = pl.DeviceIdType.MESH
BF16 = jnp.bfloat16
F32 = jnp.float32

NX, NC, NY, NZ = 4, 2, 4, 16
ZL = 8
TOK = 384
COLS = 352
FEAT = 256
EDGE = 16
EXT = TOK + 2 * EDGE


def right_reach(r):
    return 4 if r < 2 else 3


class Wires:
    def __init__(self, send_sems, recv_sems):
        self.send_sems, self.recv_sems = send_sems, recv_sems
        self.index = {}
        self.count = dict.fromkeys(("unit", "tile", "edge", "og", "taps"), 0)

    def at(self, key):
        return self.index.setdefault(key, len(self.index))

    def copy(self, key, src, dst, to, kind):
        return pltpu.make_async_remote_copy(
            src_ref=src,
            dst_ref=dst,
            send_sem=self.send_sems.at[list(self.count).index(kind)],
            recv_sem=self.recv_sems.at[self.at(key)],
            device_id=to,
            device_id_type=MESH,
        )

    def send(self, key, src, dst, to, kind="unit", amount=1):
        self.count[kind] += amount
        self.copy(key, src, dst, to, kind).start()

    def wait(self, key, dst, to, kind="unit"):
        self.copy(key, dst, dst, to, kind).wait_recv()

    def drain(self, spans, to):
        for kind, span in spans.items():
            whole = span(int(self.count[kind]))
            self.copy(("drain",), whole, whole, to, kind).wait_send()


def kernel(
    factor,
    x_hbm, wg_hbm, wv_hbm, gt_hbm, vt_hbm, ogt_hbm,
    din_hbm, dg_hbm, dv_hbm, tout_hbm,
    X, U, XB, TS, GT, VT, OGT, OG, PG, PV, KG, KV, CG, CV, DIN, DG, DV,
    send_sems, recv_sems, local_sems,
):
    def parts_of(pool, sizes):
        first, parts = 0, []
        for size in sizes:
            parts.append(pool.at[pl.ds(first, size)])
            first += size
        return parts

    WG, WV, GG, GV, *rest = parts_of(U, [32] * 4 + [8] * 18)
    FAR, DIR, MID, END, RED = ({"g": rest[2 * i], "v": rest[2 * i + 1]} for i in range(5))
    ends = [(h, way) for h in "gv" for way in (1, -1)]
    LAND, SUMS = dict(zip(ends, rest[10:14])), dict(zip(ends, rest[14:18]))
    IP, IR, IS, ISR = parts_of(XB, [2 * NX, NX, NX, 3])
    TY, TZ1, TB, TT = parts_of(TS, [4, 4, 4, 8])
    rep, fs, tp = lax.axis_index("rep"), lax.axis_index("fs"), lax.axis_index("tp")
    zl, y = lax.div(fs, NY), lax.rem(fs, NY)
    x, c = lax.div(tp, NC), lax.rem(tp, NC)
    zg = rep * ZL + zl

    def dev(x=x, c=c, y=y, z=zg):
        z = lax.rem(z + NZ, NZ)
        return (
            lax.div(z, ZL),
            lax.rem(z, ZL) * NY + lax.rem(y + NY, NY),
            lax.rem(x + NX, NX) * NC + c,
        )

    def blk(dz, dy):
        return lax.rem(zl + dz + ZL, ZL) * NY + lax.rem(y + dy + NY, NY)

    def zrow(dz):
        return lax.rem(zl + dz + 2 * ZL, ZL)

    me = dev()
    right, left = dev(z=zg + 1), dev(z=zg - 1)
    up, down = dev(y=y + 1), dev(y=y - 1)
    partner = dev(c=1 - c)
    after_z = zg + lax.div(y + 1, NY)
    after = dev(y=y + 1, z=after_z)
    before_z = zg - 1 + lax.div(y + NY - 1, NY)
    before = dev(y=y - 1, z=before_z)

    def tp_peer(k):
        return (rep, fs, lax.rem(tp + k + 8, 8))

    zq, zo = lax.div(zg, 4), lax.rem(zg, 4)
    side = 4 * (1 - 2 * lax.rem(zq, 2))

    def z_near(k):
        return dev(z=zq * 4 + lax.rem(zo + k, 4))

    own = blk(0, 0)
    loads = [
        pltpu.make_async_copy(wg_hbm, WG.at[own], local_sems.at[0]),
        pltpu.make_async_copy(wv_hbm, WV.at[own], local_sems.at[1]),
        pltpu.make_async_copy(x_hbm, X.at[tp, pl.ds(EDGE, TOK)], local_sems.at[2]),
        pltpu.make_async_copy(ogt_hbm, OGT.at[pl.ds(0, COLS)], local_sems.at[3]),
        pltpu.make_async_copy(gt_hbm, GT, local_sems.at[4]),
        pltpu.make_async_copy(vt_hbm, VT, local_sems.at[5]),
    ]
    for load in loads:
        load.start()

    barrier = pltpu.get_barrier_semaphore()
    peers = [tp_peer(k) for k in range(1, 8)]
    peers += [dev(y=y + k) for k in (1, 2, 3)]
    peers += [right, left, after, before]
    for peer in peers:
        pl.semaphore_signal(barrier, inc=1, device_id=peer, device_id_type=MESH)
    pl.semaphore_wait(barrier, len(peers))

    w = Wires(send_sems, recv_sems)

    loads[0].wait()
    for dy in (1, 3, 2):
        w.send(("gy", dy), WG.at[own], WG.at[own], dev(y=y + dy))
    loads[1].wait()
    w.send(("vz", 1, 1), WV.at[own], WV.at[own], right)
    w.send(("vz", -1, 1), WV.at[own], WV.at[own], left)
    w.send(("gz", 0, 1, 1), WG.at[own], WG.at[own], right)
    w.send(("gz", 0, -1, 1), WG.at[own], WG.at[own], left)
    loads[2].wait()
    head, tail = X.at[tp, pl.ds(EDGE, EDGE)], X.at[tp, pl.ds(TOK, EDGE)]
    lo, hi = pl.ds(0, EDGE), pl.ds(TOK + EDGE, EDGE)
    w.send(("hx", 1), tail, X.at[tp, lo], after, "edge")
    w.send(("hx", -1), head, X.at[tp, hi], before, "edge")
    mine = X.at[tp, pl.ds(EDGE, TOK)]
    HALF = TOK // 2

    def half_of(dx, i):
        return X.at[lax.rem(x - dx + NX, NX) * NC + c, pl.ds(EDGE + HALF * i, HALF)]

    for i in (0, 1):
        for way, part in ((1, half_of(0, i)), (-1, half_of(0, 1 - i))):
            w.send(("x", way, i), part, part, dev(x=x + way), "tile", 0.5)
    w.send(("xp", 0), mine, mine, partner, "tile")
    w.send(("vy", 0, 1), WV.at[own], WV.at[own], up)
    w.send(("vy", 0, -1), WV.at[own], WV.at[own], down)

    def out_grad_rows():
        loads[3].wait()
        for i in range(3):
            for j in range(3):
                block = OGT[128 * i : 128 * i + 128, 128 * j : 128 * j + 128].astype(F32)
                cols = min(128, COLS - 128 * i)
                OG[EDGE + 128 * j : EDGE + 128 * j + 128, 128 * i : 128 * i + cols] = (
                    block.T[:, :cols].astype(BF16)
                )

    def rounded(value):
        return value.astype(BF16).astype(F32)

    def gate_chunk(z, first=False, last=False):
        part = jnp.dot(
            X[z],
            WG[pl.ds(z * NY, NY)].reshape(FEAT, COLS),
            preferred_element_type=F32,
        )
        if first:
            PG[8 : 8 + EXT] = part
        elif last:
            PG[8 : 8 + EXT] = rounded(PG[8 : 8 + EXT] + part)
        else:
            PG[8 : 8 + EXT] += part

    def value_chunk(z, first=False, last=False):
        part = jnp.dot(
            X[z],
            WV[pl.ds(z * NY, NY)].reshape(FEAT, COLS),
            preferred_element_type=F32,
        )
        if first:
            PV[8 : 8 + EXT] = part
        elif last:
            PV[8 : 8 + EXT] = rounded(PV[8 : 8 + EXT] + part)
        else:
            PV[8 : 8 + EXT] += part

    def x_first():
        for way in (1, -1):
            part = half_of(way, (1 - way) // 2)
            w.wait(("x", way, 0), part, me, "tile")
            w.send(("x2", way), part, part, dev(x=x + way), "tile", 0.5)

    def x_whole(dx):
        slot = X.at[lax.rem(x - dx + NX, NX) * NC + c, pl.ds(EDGE, TOK)]
        w.send(("xp", dx), slot, slot, partner, "tile")

    def x_near():
        for way in (1, -1):
            w.wait(("x", way, 1), half_of(way, (1 + way) // 2), me, "tile")
            x_whole(way)

    def x_far():
        for way in (1, -1):
            w.wait(("x2", way), half_of(2, (1 - way) // 2), me, "tile")
        x_whole(2)

    def xp_arrived(dx):
        slot = X.at[lax.rem(x - dx + NX, NX) * NC + 1 - c, pl.ds(EDGE, TOK)]
        w.wait(("xp", dx), slot, me, "tile")

    def edges_spread():
        w.wait(("hx", 1), X.at[tp, lo], me, "edge")
        w.wait(("hx", -1), X.at[tp, hi], me, "edge")
        for k in range(1, 8):
            w.send(("hl",), X.at[tp, lo], X.at[tp, lo], tp_peer(k), "edge")
            w.send(("hl",), X.at[tp, hi], X.at[tp, hi], tp_peer(k), "edge")

    def edges_done():
        w.wait(("hl",), X.at[0, pl.ds(0, 14 * EDGE)], me, "edge")

    def gate_y(dy):
        unit = WG.at[blk(0, -dy)]
        w.wait(("gy", dy), unit, me)
        w.send(("gz", 4 - dy, 1, 1), unit, unit, right)
        w.send(("gz", 4 - dy, -1, 1), unit, unit, left)

    def gate_z(r, d):
        for way, reach, to in ((1, right_reach(r), right), (-1, 7 - right_reach(r), left)):
            if d <= reach:
                unit = WG.at[blk(-way * d, r)]
                w.wait(("gz", r, way, d), unit, me)
                if d < reach:
                    w.send(("gz", r, way, d + 1), unit, unit, to)

    def value_z(d):
        for way, reach, to in ((1, 4, right), (-1, 3, left)):
            if d <= reach:
                dz = -way * d
                unit = WV.at[blk(dz, 0)]
                w.wait(("vz", way, d), unit, me)
                if d < reach:
                    w.send(("vz", way, d + 1), unit, unit, to)
                w.send(("vy", dz, 1), unit, unit, up)
                w.send(("vy", dz, -1), unit, unit, down)
                if d == 4:
                    w.send(("vf", dz), unit, unit, dev(y=y + 2))

    def value_y(dz):
        from_down, from_up = WV.at[blk(dz, -1)], WV.at[blk(dz, 1)]
        w.wait(("vy", dz, 1), from_down, me)
        if dz % 2 == 0 and dz != -4:
            w.send(("vf", dz), from_down, from_down, up)
        w.wait(("vy", dz, -1), from_up, me)
        if dz % 2 == 1:
            w.send(("vf", dz), from_up, from_up, down)

    def value_row(dz, first=False, last=False):
        w.wait(("vf", dz), WV.at[blk(dz, 2)], me)
        value_chunk(zrow(dz), first, last)

    value_z(1)
    gate_y(1)
    gate_y(3)
    gate_y(2)
    gate_z(0, 1)
    value_y(0)
    value_z(2)
    gate_z(3, 1)
    x_first()
    gate_z(1, 1)
    edges_spread()
    gate_z(2, 1)
    value_y(1)
    value_y(-1)
    x_near()
    out_grad_rows()
    gate_z(0, 2)
    value_z(3)
    x_far()
    w.send(("og", 1), OG.at[pl.ds(TOK, EDGE)], OG.at[lo], after, "og")
    w.send(("og", -1), OG.at[pl.ds(EDGE, EDGE)], OG.at[hi], before, "og")
    gate_z(3, 2)
    value_y(2)
    value_y(-2)
    gate_z(1, 2)
    gate_z(2, 2)
    gate_z(0, 3)
    value_z(4)
    for dx in (0, 1, -1, 2):
        xp_arrived(dx)
    edges_done()
    gate_chunk(zrow(0), first=True)
    gate_chunk(zrow(1))
    gate_z(3, 3)
    gate_chunk(zrow(-1))
    value_y(3)
    value_y(-3)
    gate_z(1, 3)
    value_row(0, first=True)
    gate_chunk(zrow(2))
    gate_z(2, 3)
    gate_chunk(zrow(-2))
    value_row(1)
    gate_z(0, 4)
    value_row(-1)
    value_row(2)
    gate_chunk(zrow(3))
    gate_z(3, 4)
    value_row(-2)
    gate_chunk(zrow(-3))
    value_y(-4)
    value_row(3)
    gate_z(1, 4)
    value_row(-3)
    value_row(-4, last=True)
    gate_z(2, 4)
    gate_chunk(zrow(4), last=True)
    w.wait(("og", 1), OG.at[lo], me, "og")
    w.wait(("og", -1), OG.at[hi], me, "og")

    not_first, not_last = fs > 0, fs < NY * ZL - 1
    for ref in (PG, PV):
        ref[8 : 8 + EDGE] = jnp.where(not_first, ref[8 : 8 + EDGE], 0.0)
        ref[8 + EDGE + TOK : 8 + EXT] = jnp.where(not_last, ref[8 + EDGE + TOK : 8 + EXT], 0.0)
    OG[:EDGE] = jnp.where(not_first, OG[:EDGE].astype(F32), 0.0).astype(BF16)
    OG[EDGE + TOK :] = jnp.where(not_last, OG[EDGE + TOK :].astype(F32), 0.0).astype(BF16)

    loads[4].wait()
    loads[5].wait()
    taps = jnp.concatenate([GT[...], VT[...], jnp.zeros((2, 8 * COLS), F32)], axis=0)
    taps = pltpu.roll(taps, lax.rem((8 - tp) * COLS, 8 * COLS), axis=1)[:, :COLS]
    g0, g1, g2, v0, v1, v2 = (taps[k : k + 1] for k in range(6))

    def cot_rows(i):
        base = pl.multiple_of(i * 16, 16)
        gate = PG[pl.ds(base, 32)]
        value = PV[pl.ds(base, 32)]
        gm, gz, gp = gate[7:23], gate[8:24], gate[9:25]
        vm, vz, vp = value[7:23], value[8:24], value[9:25]
        gate_mix = g0 * gm + g1 * gz + g2 * gp
        value_mix = v0 * vm + v1 * vz + v2 * vp
        grad = OG[pl.ds(base, 16)].astype(F32)
        s = jax.nn.sigmoid(gate_mix)
        gate_cot = grad * value_mix * (s * (1.0 + gate_mix * (1.0 - s)))
        value_cot = grad * (gate_mix * s)
        KG[pl.ds(base + 8, 16)] = gate_cot
        KV[pl.ds(base + 8, 16)] = value_cot
        return [
            (p * k).reshape(2, 8, COLS).sum(axis=0)
            for p, k in (
                (gm, gate_cot), (gz, gate_cot), (gp, gate_cot),
                (vm, value_cot), (vz, value_cot), (vp, value_cot),
            )
        ]

    cot_rows(0)
    cot_rows(TOK // 16 + 1)
    zero = jnp.zeros((8, COLS), F32)
    tap_sums = lax.fori_loop(
        1, TOK // 16 + 1,
        lambda i, sums: tuple(a + b for a, b in zip(sums, cot_rows(i))),
        (zero,) * 6,
    )

    def back_rows(i, carry):
        base = pl.multiple_of(i * 16, 16)
        out = pl.ds(pl.multiple_of(i * 16 - 16, 16), 16)
        for source, target, (t0, t1, t2) in ((KG, CG, (g0, g1, g2)), (KV, CV, (v0, v1, v2))):
            cot = source[pl.ds(base, 32)]
            target[out] = (t0 * cot[9:25] + t1 * cot[8:24] + t2 * cot[7:23]).astype(BF16)
        return carry

    lax.fori_loop(1, TOK // 16 + 1, back_rows, 0)

    rows = [jnp.sum(part, axis=0, keepdims=True) for part in tap_sums]
    TY[y] = jnp.concatenate(rows + [jnp.zeros((2, COLS), F32)], axis=0)

    order = (0, 1, -1, 2, -2, 3, -3, 4)
    place = {dz % ZL: k for k, dz in enumerate(order)}
    COT, TERMS = {"g": CG, "v": CV}, {"g": GG, "v": GV}

    def turn(h, k):
        return (1, up, down) if (k % 2 == 0) == (h == "g") else (-1, down, up)

    def make_blocks(h, k):
        dz = order[k]
        z = zrow(dz)
        block = lax.dot_general(
            X[z, EDGE : EDGE + TOK, :], COT[h][...],
            (((0,), (0,)), ((), ())), preferred_element_type=F32,
        )
        TERMS[h][pl.ds(z * NY, NY)] = block.astype(BF16).reshape(NY, 64, COLS)
        way, onward, back = turn(h, k)
        w.send(("far", h, k), TERMS[h].at[blk(dz, 2)], FAR[h].at[k], onward)
        w.send(("dir", h, k), TERMS[h].at[blk(dz, -way)], DIR[h].at[k], back)

    def total(*parts):
        acc = parts[0].astype(F32)
        for part in parts[1:]:
            acc = acc + part.astype(F32)
        return acc

    def pass_on(h, k):
        way, onward, back = turn(h, k)
        w.wait(("far", h, k), FAR[h].at[k], me)
        MID[h][k] = total(FAR[h][k], TERMS[h][blk(order[k], way)]).astype(BF16)
        w.send(("mid", h, k), MID[h].at[k], END[h].at[k], onward)

    def row_done(h, k):
        w.wait(("dir", h, k), DIR[h].at[k], me)
        w.wait(("mid", h, k), END[h].at[k], me)
        RED[h][k] = total(TERMS[h][blk(order[k], 0)], DIR[h][k], END[h][k]).astype(BF16)

    def start_of(h, way):
        return 8 if (h == "g") == (way == 1) else 7

    direct = {4: (3, 4)}
    starts = {(h, way): (start_of(h, way), 3) for h, way in ends}

    def row_at(way, d):
        return place[(way * d) % ZL]

    def hop(h, way, d):
        landing = LAND[h, way]
        k = row_at(way, d)
        if d in starts[h, way]:
            source = RED[h].at[k]
        else:
            w.wait((h, way, d), landing.at[d], me)
            SUMS[h, way][d] = total(landing[d], RED[h][k]).astype(BF16)
            source = SUMS[h, way].at[d]
        slot, to = direct.get(d, (d - 1, 1))
        w.send((h, way, slot), source, landing.at[slot], dev(z=zg + way * to))

    def finish(h, out):
        parts = [RED[h][place[0]]]
        for way in (1, -1):
            for slot in [0] + [slot for slot, _ in direct.values()]:
                w.wait((h, way, slot), LAND[h, way].at[slot], me)
                parts.append(LAND[h, way][slot])
        out[...] = total(*parts) * factor

    def input_terms(j):
        part = lax.dot_general(
            CG[...], WG[NY * j : NY * j + NY].reshape(FEAT, COLS),
            (((1,), (1,)), ((), ())), preferred_element_type=F32,
        ) + lax.dot_general(
            CV[...], WV[NY * j : NY * j + NY].reshape(FEAT, COLS),
            (((1,), (1,)), ((), ())), preferred_element_type=F32,
        )
        IP[NX * (j % 2) + j // 2] = part.astype(BF16)

    def input_swap():
        for i in range(NX):
            w.send(("ip", i), IP.at[NX * (1 - c) + i], IR.at[i], partner, "tile")

    def input_sums():
        for i in range(NX):
            w.wait(("ip", i), IR.at[i], me, "tile")
            IS[i] = total(IP[NX * c + i], IR[i]).astype(BF16)
        for dx in (1, 3, 2):
            w.send(("is", dx), IS.at[lax.rem(x + dx, NX)], ISR.at[dx - 1], dev(x=x + dx), "tile")

    results = []

    def put_out(source, target):
        copy = pltpu.make_async_copy(source, target, local_sems.at[6 + len(results)])
        copy.start()
        results.append(copy)

    def input_done():
        for dx in (1, 3, 2):
            w.wait(("is", dx), ISR.at[dx - 1], me, "tile")
        DIN[...] = total(IP[NX * c + x], IR[x], ISR[0], ISR[1], ISR[2]).astype(BF16)
        put_out(DIN, din_hbm)

    def taps_y():
        for dy in (1, 2, 3):
            w.send(("ty",), TY.at[y], TY.at[y], dev(y=y + dy), "taps")

    def taps_z():
        w.wait(("ty",), TY.at[pl.ds(0, 3)], me, "taps")
        TZ1[zo] = TY[0] + TY[1] + TY[2] + TY[3]
        for k in (1, 2, 3):
            w.send(("tz",), TZ1.at[zo], TZ1.at[zo], z_near(k), "taps")

    def taps_pair(stage):
        if stage == 0:
            w.wait(("tz",), TZ1.at[pl.ds(0, 3)], me, "taps")
            TB[0] = TZ1[0] + TZ1[1] + TZ1[2] + TZ1[3]
            w.send(("tb", 0), TB.at[0], TB.at[1], dev(z=zg + side), "taps")
        else:
            w.wait(("tb", 0), TB.at[1], me, "taps")
            TB[2] = TB[0] + TB[1]
            w.send(("tb", 1), TB.at[2], TB.at[3], dev(z=zg - side), "taps")

    def taps_spread():
        w.wait(("tb", 1), TB.at[3], me, "taps")
        TT[tp] = (TB[2] + TB[3]) * factor
        for k in range(1, 8):
            w.send(("tt",), TT.at[tp], TT.at[tp], tp_peer(k), "taps")

    def taps_done():
        w.wait(("tt",), TT.at[pl.ds(0, 7)], me, "taps")
        put_out(TT, tout_hbm)

    items = [(h, k) for k in range(5) for h in "gv"]
    items += [(h, k) for h in "gv" for k in (5, 6, 7)]
    ahead, lag, spacing = 6, 3, 3
    row_step = {item: t + lag for t, item in enumerate(items)}
    hop_step = {}
    for h, way in ends:
        for d in range(start_of(h, way), 0, -1):
            step = row_step[h, row_at(way, d)]
            if d not in starts[h, way]:
                step = max(step, hop_step[h, way, d + 1] + spacing)
            hop_step[h, way, d] = step
    late = {
        16: [("v", 1, 3), ("v", -1, 5), ("g", -1, 4)],
        17: [("v", -1, 3), ("v", 1, 5), ("g", 1, 4)],
        18: [("g", 1, 2), ("g", -1, 2), ("v", -1, 4), ("v", 1, 4)],
        19: [("g", 1, 1), ("v", 1, 2), ("g", -1, 1), ("v", -1, 2)],
        20: [("v", 1, 1), ("v", -1, 1)],
    }
    for step, keys in late.items():
        for key in keys:
            del hop_step[key]
            hop_step[key] = step
    extra = {4: [taps_z], 5: [input_swap], 8: [lambda: taps_pair(0)], 9: [input_sums], 13: [lambda: taps_pair(1)],
             19: [taps_spread]}
    for j in range(4, 8):
        extra.setdefault(j - 3, []).insert(0, functools.partial(input_terms, j))
    for item in items[:ahead]:
        make_blocks(*item)
    taps_y()
    for j in range(4):
        input_terms(j)
    for step in range(max(hop_step.values()) + 1):
        if step < len(items):
            pass_on(*items[step])
        if step + ahead < len(items):
            make_blocks(*items[step + ahead])
        if 0 <= step - lag < len(items):
            row_done(*items[step - lag])
        for key in sorted(hop_step, key=hop_step.get):
            if hop_step[key] == step:
                hop(*key)
        for run in extra.get(step, ()):
            run()
    input_done()
    taps_done()
    finish("g", DG)
    put_out(DG, dg_hbm)
    finish("v", DV)
    put_out(DV, dv_hbm)
    w.drain(
        {
            "unit": lambda n: U.at[pl.ds(0, n)],
            "tile": lambda n: XB.at[pl.ds(0, n)],
            "edge": lambda n: X.at[0, pl.ds(0, n * EDGE)],
            "og": lambda n: OG.at[pl.ds(0, n * EDGE)],
            "taps": lambda n: TS.at[pl.ds(0, n)],
        },
        me,
    )
    for copy in results:
        copy.wait()
    if len(w.index) != RECEIVES:
        raise ValueError(str(len(w.index)))


RECEIVES = 168


def finisher(din_ref, dg_ref, dv_ref, tt_ref, din_out, dg_out, dv_out, tg_out, tv_out):
    din_out[...] = din_ref[...]
    dg_out[...] = dg_ref[...]
    dv_out[...] = dv_ref[...]
    taps = jnp.concatenate([tt_ref[i] for i in range(8)], axis=1)
    tg_out[...] = taps[0:3]
    tv_out[...] = taps[3:6]


def shards(inputs, gate_proj, value_proj, gate_taps, value_taps, out_grad):
    unit = gate_proj.shape
    cols = unit[1]
    factor = float(TOK * NY * NZ) ** (-0.5)
    vm = pltpu.VMEM
    scratch = [
        vm((8, EXT, FEAT), BF16),
        vm((272, *unit), BF16),
        vm((4 * NX + 3, TOK, FEAT), BF16),
        vm((20, 8, cols), F32),
        vm(gate_taps.shape, F32),
        vm(gate_taps.shape, F32),
        vm((384, TOK), BF16),
        vm((EXT, cols), BF16),
        vm((EXT + 16, cols), F32),
        vm((EXT + 16, cols), F32),
        vm((EXT + 16, cols), F32),
        vm((EXT + 16, cols), F32),
        vm((TOK, cols), BF16),
        vm((TOK, cols), BF16),
        vm((TOK, FEAT), BF16),
        vm(unit, F32),
        vm(unit, F32),
        pltpu.SemaphoreType.DMA((5,)),
        pltpu.SemaphoreType.DMA((RECEIVES,)),
        pltpu.SemaphoreType.DMA((10,)),
    ]
    anywhere = pl.BlockSpec(memory_space=pl.ANY)
    vmem = pl.BlockSpec(memory_space=pltpu.VMEM)
    tile = jax.ShapeDtypeStruct((TOK, FEAT), BF16)
    grad = jax.ShapeDtypeStruct(unit, F32)
    tap = jax.ShapeDtypeStruct(gate_taps.shape, F32)
    sums = pl.pallas_call(
        functools.partial(kernel, factor),
        out_shape=(tile, grad, grad, jax.ShapeDtypeStruct((8, 8, cols), F32)),
        in_specs=[anywhere] * 6,
        out_specs=(anywhere,) * 4,
        scratch_shapes=scratch,
        compiler_params=pltpu.CompilerParams(
            collective_id=0, has_side_effects=True, vmem_limit_bytes=65000 * 1024
        ),
    )(inputs[0], gate_proj, value_proj, gate_taps, value_taps, jnp.swapaxes(out_grad[0], 0, 1))
    din, dg, dv, tg, tv = pl.pallas_call(
        finisher,
        out_shape=(tile, grad, grad, tap, tap),
        in_specs=[vmem] * 4,
        out_specs=(vmem,) * 5,
    )(*sums)
    return din[None], dg, dv, tg, tv


def solution(mesh):
    return jax.shard_map(
        shards,
        mesh=mesh,
        in_specs=(P("rep", "fs", "tp"), P("fs", "tp"), P("fs", "tp"), P(), P(), P("rep", "fs", "tp")),
        out_specs=(P("rep", "fs", "tp"), P("fs", "tp"), P("fs", "tp"), P(), P()),
        check_vma=False,
    )
```

```python
import functools

import jax
import jax.numpy as jnp
from jax import lax
from jax.experimental import pallas as pl
from jax.experimental.pallas import tpu as pltpu
from jax.sharding import PartitionSpec as P

MESH = pl.DeviceIdType.MESH
BF16 = jnp.bfloat16
F32 = jnp.float32

NX, NC, NY, NZ = 4, 2, 4, 16
ZL = 8
TOK = 384
COLS = 352
FEAT = 256
EDGE = 16
EXT = TOK + 2 * EDGE


def right_reach(r):
    return 4 if r < 2 else 3


TREES = {
    "g": {8: 7, 7: 6, 6: 5, 5: 4, 4: 3, 3: 2, 2: 1, 1: 0},
    "v": {8: 7, 7: 6, 6: 5, 5: 4, 4: 0, 3: 2, 2: 1, 1: 0},
}
ITEMS = [(h, k) for h in "gv" for k in range(ZL)]
AHEAD, SPACING = 4, 3


class Wires:
    def __init__(self, send_sems, recv_sems):
        self.send_sems, self.recv_sems = send_sems, recv_sems
        self.index = {}
        self.count = dict.fromkeys(("unit", "tile", "edge", "og", "taps"), 0)

    def at(self, key):
        return self.index.setdefault(key, len(self.index))

    def copy(self, key, src, dst, to, kind):
        return pltpu.make_async_remote_copy(
            src_ref=src,
            dst_ref=dst,
            send_sem=self.send_sems.at[list(self.count).index(kind)],
            recv_sem=self.recv_sems.at[self.at(key)],
            device_id=to,
            device_id_type=MESH,
        )

    def send(self, key, src, dst, to, kind="unit", amount=1):
        self.count[kind] += amount
        self.copy(key, src, dst, to, kind).start()

    def wait(self, key, dst, to, kind="unit"):
        self.copy(key, dst, dst, to, kind).wait_recv()

    def drain(self, spans, to):
        for kind, span in spans.items():
            whole = span(int(self.count[kind]))
            self.copy(("drain",), whole, whole, to, kind).wait_send()


def kernel(
    factor,
    x_hbm, wg_hbm, wv_hbm, gt_hbm, vt_hbm, ogt_hbm,
    din_hbm, dg_hbm, dv_hbm, tout_hbm,
    X, U, XB, TS, GT, VT, OGT, OG, PG, PV, KG, KV, CG, CV, DIN, DG, DV,
    send_sems, recv_sems, local_sems,
):
    def parts_of(pool, sizes):
        first, parts = 0, []
        for size in sizes:
            parts.append(pool.at[pl.ds(first, size)])
            first += size
        return parts

    WG, WV, GG, GV, *rest = parts_of(U, [32] * 4 + [8] * 10 + [9] * 8)
    FAR, DIR, MID, END, RED = ({"g": rest[2 * i], "v": rest[2 * i + 1]} for i in range(5))
    ends = [(h, way) for h in "gv" for way in (1, -1)]
    LAND, SUMS = dict(zip(ends, rest[10:14])), dict(zip(ends, rest[14:18]))
    IP, IR, IS, ISR = parts_of(XB, [2 * NX, NX, NX, 3])
    TY, TZ1, TB, TT = parts_of(TS, [4, 4, 4, 8])
    rep, fs, tp = lax.axis_index("rep"), lax.axis_index("fs"), lax.axis_index("tp")
    zl, y = lax.div(fs, NY), lax.rem(fs, NY)
    x, c = lax.div(tp, NC), lax.rem(tp, NC)
    zg = rep * ZL + zl

    def dev(x=x, c=c, y=y, z=zg):
        z = lax.rem(z + NZ, NZ)
        return (
            lax.div(z, ZL),
            lax.rem(z, ZL) * NY + lax.rem(y + NY, NY),
            lax.rem(x + NX, NX) * NC + c,
        )

    def blk(dz, dy):
        return lax.rem(zl + dz + ZL, ZL) * NY + lax.rem(y + dy + NY, NY)

    def zrow(dz):
        return lax.rem(zl + dz + 2 * ZL, ZL)

    me = dev()
    right, left = dev(z=zg + 1), dev(z=zg - 1)
    up, down = dev(y=y + 1), dev(y=y - 1)
    partner = dev(c=1 - c)
    after_z = zg + lax.div(y + 1, NY)
    after = dev(y=y + 1, z=after_z)
    before_z = zg - 1 + lax.div(y + NY - 1, NY)
    before = dev(y=y - 1, z=before_z)

    def tp_peer(k):
        return (rep, fs, lax.rem(tp + k + 8, 8))

    zq, zo = lax.div(zg, 4), lax.rem(zg, 4)
    side = 4 * (1 - 2 * lax.rem(zq, 2))

    def z_near(k):
        return dev(z=zq * 4 + lax.rem(zo + k, 4))

    own = blk(0, 0)
    loads = [
        pltpu.make_async_copy(wg_hbm, WG.at[own], local_sems.at[0]),
        pltpu.make_async_copy(wv_hbm, WV.at[own], local_sems.at[1]),
        pltpu.make_async_copy(x_hbm, X.at[tp, pl.ds(EDGE, TOK)], local_sems.at[2]),
        pltpu.make_async_copy(ogt_hbm, OGT.at[pl.ds(0, COLS)], local_sems.at[3]),
        pltpu.make_async_copy(gt_hbm, GT, local_sems.at[4]),
        pltpu.make_async_copy(vt_hbm, VT, local_sems.at[5]),
    ]
    for load in loads:
        load.start()

    barrier = pltpu.get_barrier_semaphore()
    peers = [tp_peer(k) for k in range(1, 8)]
    peers += [dev(y=y + k) for k in (1, 2, 3)]
    peers += [right, left, after, before]
    for peer in peers:
        pl.semaphore_signal(barrier, inc=1, device_id=peer, device_id_type=MESH)
    pl.semaphore_wait(barrier, len(peers))

    w = Wires(send_sems, recv_sems)

    loads[0].wait()
    for dy in (1, 3, 2):
        w.send(("gy", dy), WG.at[own], WG.at[own], dev(y=y + dy))
    loads[1].wait()
    w.send(("vz", 1, 1), WV.at[own], WV.at[own], right)
    w.send(("vz", -1, 1), WV.at[own], WV.at[own], left)
    w.send(("gz", 0, 1, 1), WG.at[own], WG.at[own], right)
    w.send(("gz", 0, -1, 1), WG.at[own], WG.at[own], left)
    loads[2].wait()
    head, tail = X.at[tp, pl.ds(EDGE, EDGE)], X.at[tp, pl.ds(TOK, EDGE)]
    lo, hi = pl.ds(0, EDGE), pl.ds(TOK + EDGE, EDGE)
    w.send(("hx", 1), tail, X.at[tp, lo], after, "edge")
    w.send(("hx", -1), head, X.at[tp, hi], before, "edge")
    mine = X.at[tp, pl.ds(EDGE, TOK)]
    HALF = TOK // 2

    def half_of(dx, i):
        return X.at[lax.rem(x - dx + NX, NX) * NC + c, pl.ds(EDGE + HALF * i, HALF)]

    for i in (0, 1):
        for way, part in ((1, half_of(0, i)), (-1, half_of(0, 1 - i))):
            w.send(("x", way, i), part, part, dev(x=x + way), "tile", 0.5)
    w.send(("xp", 0), mine, mine, partner, "tile")
    w.send(("vy", 0, 1), WV.at[own], WV.at[own], up)
    w.send(("vy", 0, -1), WV.at[own], WV.at[own], down)

    def out_grad_rows():
        loads[3].wait()
        for i in range(3):
            for j in range(3):
                block = OGT[128 * i : 128 * i + 128, 128 * j : 128 * j + 128].astype(F32)
                cols = min(128, COLS - 128 * i)
                OG[EDGE + 128 * j : EDGE + 128 * j + 128, 128 * i : 128 * i + cols] = (
                    block.T[:, :cols].astype(BF16)
                )

    def rounded(value):
        return value.astype(BF16).astype(F32)

    def gate_chunk(z, first=False, last=False):
        part = jnp.dot(
            X[z],
            WG[pl.ds(z * NY, NY)].reshape(FEAT, COLS),
            preferred_element_type=F32,
        )
        if first:
            PG[8 : 8 + EXT] = part
        elif last:
            PG[8 : 8 + EXT] = rounded(PG[8 : 8 + EXT] + part)
        else:
            PG[8 : 8 + EXT] += part

    def value_chunk(z, first=False, last=False):
        part = jnp.dot(
            X[z],
            WV[pl.ds(z * NY, NY)].reshape(FEAT, COLS),
            preferred_element_type=F32,
        )
        if first:
            PV[8 : 8 + EXT] = part
        elif last:
            PV[8 : 8 + EXT] = rounded(PV[8 : 8 + EXT] + part)
        else:
            PV[8 : 8 + EXT] += part

    def x_first():
        for way in (1, -1):
            part = half_of(way, (1 - way) // 2)
            w.wait(("x", way, 0), part, me, "tile")
            w.send(("x2", way), part, part, dev(x=x + way), "tile", 0.5)

    def x_whole(dx):
        slot = X.at[lax.rem(x - dx + NX, NX) * NC + c, pl.ds(EDGE, TOK)]
        w.send(("xp", dx), slot, slot, partner, "tile")

    def x_near():
        for way in (1, -1):
            w.wait(("x", way, 1), half_of(way, (1 + way) // 2), me, "tile")
            x_whole(way)

    def x_far():
        for way in (1, -1):
            w.wait(("x2", way), half_of(2, (1 - way) // 2), me, "tile")
        x_whole(2)

    def xp_arrived(dx):
        slot = X.at[lax.rem(x - dx + NX, NX) * NC + 1 - c, pl.ds(EDGE, TOK)]
        w.wait(("xp", dx), slot, me, "tile")

    def edges_spread():
        w.wait(("hx", 1), X.at[tp, lo], me, "edge")
        w.wait(("hx", -1), X.at[tp, hi], me, "edge")
        for k in range(1, 8):
            w.send(("hl",), X.at[tp, lo], X.at[tp, lo], tp_peer(k), "edge")
            w.send(("hl",), X.at[tp, hi], X.at[tp, hi], tp_peer(k), "edge")

    def edges_done():
        w.wait(("hl",), X.at[0, pl.ds(0, 14 * EDGE)], me, "edge")

    def gate_y(dy):
        unit = WG.at[blk(0, -dy)]
        w.wait(("gy", dy), unit, me)
        w.send(("gz", 4 - dy, 1, 1), unit, unit, right)
        w.send(("gz", 4 - dy, -1, 1), unit, unit, left)

    def gate_z(r, d):
        for way, reach, to in ((1, right_reach(r), right), (-1, 7 - right_reach(r), left)):
            if d <= reach:
                unit = WG.at[blk(-way * d, r)]
                w.wait(("gz", r, way, d), unit, me)
                if d < reach:
                    w.send(("gz", r, way, d + 1), unit, unit, to)

    def value_z(d):
        for way, reach, to in ((1, 4, right), (-1, 3, left)):
            if d <= reach:
                dz = -way * d
                unit = WV.at[blk(dz, 0)]
                w.wait(("vz", way, d), unit, me)
                if d < reach:
                    w.send(("vz", way, d + 1), unit, unit, to)
                w.send(("vy", dz, 1), unit, unit, up)
                w.send(("vy", dz, -1), unit, unit, down)
                if d == 4:
                    w.send(("vf", dz), unit, unit, dev(y=y + 2))

    def value_y(dz):
        from_down, from_up = WV.at[blk(dz, -1)], WV.at[blk(dz, 1)]
        w.wait(("vy", dz, 1), from_down, me)
        if dz % 2 == 0 and dz != -4:
            w.send(("vf", dz), from_down, from_down, up)
        w.wait(("vy", dz, -1), from_up, me)
        if dz % 2 == 1:
            w.send(("vf", dz), from_up, from_up, down)

    def value_row(dz, first=False, last=False):
        w.wait(("vf", dz), WV.at[blk(dz, 2)], me)
        value_chunk(zrow(dz), first, last)

    value_z(1)
    gate_y(1)
    gate_y(3)
    gate_y(2)
    gate_z(0, 1)
    value_y(0)
    value_z(2)
    gate_z(3, 1)
    x_first()
    gate_z(1, 1)
    edges_spread()
    gate_z(2, 1)
    value_y(1)
    value_y(-1)
    x_near()
    out_grad_rows()
    gate_z(0, 2)
    value_z(3)
    x_far()
    w.send(("og", 1), OG.at[pl.ds(TOK, EDGE)], OG.at[lo], after, "og")
    w.send(("og", -1), OG.at[pl.ds(EDGE, EDGE)], OG.at[hi], before, "og")
    gate_z(3, 2)
    value_y(2)
    value_y(-2)
    gate_z(1, 2)
    gate_z(2, 2)
    gate_z(0, 3)
    value_z(4)
    for dx in (0, 1, -1, 2):
        xp_arrived(dx)
    edges_done()
    gate_chunk(zrow(0), first=True)
    gate_chunk(zrow(1))
    gate_z(3, 3)
    gate_chunk(zrow(-1))
    value_y(3)
    value_y(-3)
    gate_z(1, 3)
    value_row(0, first=True)
    gate_chunk(zrow(2))
    gate_z(2, 3)
    gate_chunk(zrow(-2))
    value_row(1)
    gate_z(0, 4)
    value_row(-1)
    value_row(2)
    gate_chunk(zrow(3))
    gate_z(3, 4)
    value_row(-2)
    gate_chunk(zrow(-3))
    value_y(-4)
    value_row(3)
    gate_z(1, 4)
    value_row(-3)
    value_row(-4, last=True)
    gate_z(2, 4)
    gate_chunk(zrow(4), last=True)
    w.wait(("og", 1), OG.at[lo], me, "og")
    w.wait(("og", -1), OG.at[hi], me, "og")

    not_first, not_last = fs > 0, fs < NY * ZL - 1
    for ref in (PG, PV):
        ref[8 : 8 + EDGE] = jnp.where(not_first, ref[8 : 8 + EDGE], 0.0)
        ref[8 + EDGE + TOK : 8 + EXT] = jnp.where(not_last, ref[8 + EDGE + TOK : 8 + EXT], 0.0)
    OG[:EDGE] = jnp.where(not_first, OG[:EDGE].astype(F32), 0.0).astype(BF16)
    OG[EDGE + TOK :] = jnp.where(not_last, OG[EDGE + TOK :].astype(F32), 0.0).astype(BF16)

    loads[4].wait()
    loads[5].wait()
    taps = jnp.concatenate([GT[...], VT[...], jnp.zeros((2, 8 * COLS), F32)], axis=0)
    taps = pltpu.roll(taps, lax.rem((8 - tp) * COLS, 8 * COLS), axis=1)[:, :COLS]
    g0, g1, g2, v0, v1, v2 = (taps[k : k + 1] for k in range(6))

    def cot_rows(i):
        base = pl.multiple_of(i * 16, 16)
        gate = PG[pl.ds(base, 32)]
        value = PV[pl.ds(base, 32)]
        gm, gz, gp = gate[7:23], gate[8:24], gate[9:25]
        vm, vz, vp = value[7:23], value[8:24], value[9:25]
        gate_mix = g0 * gm + g1 * gz + g2 * gp
        value_mix = v0 * vm + v1 * vz + v2 * vp
        grad = OG[pl.ds(base, 16)].astype(F32)
        s = jax.nn.sigmoid(gate_mix)
        gate_cot = grad * value_mix * (s * (1.0 + gate_mix * (1.0 - s)))
        value_cot = grad * (gate_mix * s)
        KG[pl.ds(base + 8, 16)] = gate_cot
        KV[pl.ds(base + 8, 16)] = value_cot
        return [
            (p * k).reshape(2, 8, COLS).sum(axis=0)
            for p, k in (
                (gm, gate_cot), (gz, gate_cot), (gp, gate_cot),
                (vm, value_cot), (vz, value_cot), (vp, value_cot),
            )
        ]

    cot_rows(0)
    cot_rows(TOK // 16 + 1)
    zero = jnp.zeros((8, COLS), F32)
    tap_sums = lax.fori_loop(
        1, TOK // 16 + 1,
        lambda i, sums: tuple(a + b for a, b in zip(sums, cot_rows(i))),
        (zero,) * 6,
    )

    def back_rows(i, carry):
        base = pl.multiple_of(i * 16, 16)
        out = pl.ds(pl.multiple_of(i * 16 - 16, 16), 16)
        for source, target, (t0, t1, t2) in ((KG, CG, (g0, g1, g2)), (KV, CV, (v0, v1, v2))):
            cot = source[pl.ds(base, 32)]
            target[out] = (t0 * cot[9:25] + t1 * cot[8:24] + t2 * cot[7:23]).astype(BF16)
        return carry

    lax.fori_loop(1, TOK // 16 + 1, back_rows, 0)

    rows = [jnp.sum(part, axis=0, keepdims=True) for part in tap_sums]
    TY[y] = jnp.concatenate(rows + [jnp.zeros((2, COLS), F32)], axis=0)

    order = (0, 1, -1, 2, -2, 3, -3, 4)
    place = {dz % ZL: k for k, dz in enumerate(order)}
    COT, TERMS = {"g": CG, "v": CV}, {"g": GG, "v": GV}

    def turn(h, k):
        return (1, up, down) if (k % 2 == 0) == (h == "g") else (-1, down, up)

    def make_blocks(h, k):
        dz = order[k]
        z = zrow(dz)
        block = lax.dot_general(
            X[z, EDGE : EDGE + TOK, :], COT[h][...],
            (((0,), (0,)), ((), ())), preferred_element_type=F32,
        )
        TERMS[h][pl.ds(z * NY, NY)] = block.astype(BF16).reshape(NY, 64, COLS)
        way, onward, back = turn(h, k)
        w.send(("far", h, k), TERMS[h].at[blk(dz, 2)], FAR[h].at[k], onward)
        w.send(("dir", h, k), TERMS[h].at[blk(dz, -way)], DIR[h].at[k], back)

    def total(*parts):
        acc = parts[0].astype(F32)
        for part in parts[1:]:
            acc = acc + part.astype(F32)
        return acc

    def pass_on(h, k):
        way, onward, back = turn(h, k)
        w.wait(("far", h, k), FAR[h].at[k], me)
        MID[h][k] = total(FAR[h][k], TERMS[h][blk(order[k], way)]).astype(BF16)
        w.send(("mid", h, k), MID[h].at[k], END[h].at[k], onward)

    def row_done(h, k):
        w.wait(("dir", h, k), DIR[h].at[k], me)
        w.wait(("mid", h, k), END[h].at[k], me)
        RED[h][k] = total(TERMS[h][blk(order[k], 0)], DIR[h][k], END[h][k]).astype(BF16)

    def start_of(h, way):
        return 8 if (h == "g") == (way == 1) else 7

    def row_at(way, d):
        return place[(way * d) % ZL]

    def sources(h, way, d):
        return [e for e in range(start_of(h, way), d, -1) if TREES[h][e] == d]

    def arrived(h, way, d):
        landing = LAND[h, way]
        for e in sources(h, way, d):
            w.wait((h, way, e), landing.at[e], me)
        return [landing[e] for e in sources(h, way, d)]

    def hop(h, way, d):
        k = row_at(way, d)
        source = RED[h].at[k]
        if sources(h, way, d):
            SUMS[h, way][d] = total(*arrived(h, way, d), RED[h][k]).astype(BF16)
            source = SUMS[h, way].at[d]
        w.send((h, way, d), source, LAND[h, way].at[d], dev(z=zg + way * (d - TREES[h][d])))

    def finish(h, out):
        parts = arrived(h, 1, 0) + arrived(h, -1, 0)
        out[...] = total(RED[h][place[0]], *parts) * factor

    def input_terms(j):
        part = lax.dot_general(
            CG[...], WG[NY * j : NY * j + NY].reshape(FEAT, COLS),
            (((1,), (1,)), ((), ())), preferred_element_type=F32,
        ) + lax.dot_general(
            CV[...], WV[NY * j : NY * j + NY].reshape(FEAT, COLS),
            (((1,), (1,)), ((), ())), preferred_element_type=F32,
        )
        IP[NX * (j % 2) + j // 2] = part.astype(BF16)

    def input_swap():
        for i in range(NX):
            w.send(("ip", i), IP.at[NX * (1 - c) + i], IR.at[i], partner, "tile")

    def input_sums():
        for i in range(NX):
            w.wait(("ip", i), IR.at[i], me, "tile")
            IS[i] = total(IP[NX * c + i], IR[i]).astype(BF16)
        for dx in (1, 3, 2):
            w.send(("is", dx), IS.at[lax.rem(x + dx, NX)], ISR.at[dx - 1], dev(x=x + dx), "tile")

    results = []

    def put_out(source, target):
        copy = pltpu.make_async_copy(source, target, local_sems.at[6 + len(results)])
        copy.start()
        results.append(copy)

    def input_done():
        for dx in (1, 3, 2):
            w.wait(("is", dx), ISR.at[dx - 1], me, "tile")
        DIN[...] = total(IP[NX * c + x], IR[x], ISR[0], ISR[1], ISR[2]).astype(BF16)
        put_out(DIN, din_hbm)

    def taps_y():
        for dy in (1, 2, 3):
            w.send(("ty",), TY.at[y], TY.at[y], dev(y=y + dy), "taps")

    def taps_z():
        w.wait(("ty",), TY.at[pl.ds(0, 3)], me, "taps")
        TZ1[zo] = TY[0] + TY[1] + TY[2] + TY[3]
        for k in (1, 2, 3):
            w.send(("tz",), TZ1.at[zo], TZ1.at[zo], z_near(k), "taps")

    def taps_pair(stage):
        if stage == 0:
            w.wait(("tz",), TZ1.at[pl.ds(0, 3)], me, "taps")
            TB[0] = TZ1[0] + TZ1[1] + TZ1[2] + TZ1[3]
            w.send(("tb", 0), TB.at[0], TB.at[1], dev(z=zg + side), "taps")
        else:
            w.wait(("tb", 0), TB.at[1], me, "taps")
            TB[2] = TB[0] + TB[1]
            w.send(("tb", 1), TB.at[2], TB.at[3], dev(z=zg - side), "taps")

    def taps_spread():
        w.wait(("tb", 1), TB.at[3], me, "taps")
        TT[tp] = (TB[2] + TB[3]) * factor
        for k in range(1, 8):
            w.send(("tt",), TT.at[tp], TT.at[tp], tp_peer(k), "taps")

    def taps_done():
        w.wait(("tt",), TT.at[pl.ds(0, 7)], me, "taps")
        put_out(TT, tout_hbm)

    ahead, lag, spacing = AHEAD, 3, SPACING
    row_step = {item: t + lag for t, item in enumerate(ITEMS)}
    hop_step = {}
    for h, way in ends:
        for d in range(start_of(h, way), 0, -1):
            steps = [hop_step[h, way, e] + spacing + e - d - 1 for e in sources(h, way, d)]
            hop_step[h, way, d] = max([row_step[h, row_at(way, d)], *steps])
    items = ITEMS
    extra = {4: [taps_z], 5: [input_swap], 8: [lambda: taps_pair(0)], 9: [input_sums], 13: [lambda: taps_pair(1)],
             19: [taps_spread]}
    for j in range(4, 8):
        extra.setdefault(j - 3, []).insert(0, functools.partial(input_terms, j))
    for item in items[:ahead]:
        make_blocks(*item)
    taps_y()
    for j in range(4):
        input_terms(j)
    for step in range(max(hop_step.values()) + 1):
        if step < len(items):
            pass_on(*items[step])
        if step + ahead < len(items):
            make_blocks(*items[step + ahead])
        if 0 <= step - lag < len(items):
            row_done(*items[step - lag])
        for key in sorted(hop_step, key=hop_step.get):
            if hop_step[key] == step:
                hop(*key)
        for run in extra.get(step, ()):
            run()
    input_done()
    taps_done()
    finish("g", DG)
    put_out(DG, dg_hbm)
    finish("v", DV)
    put_out(DV, dv_hbm)
    w.drain(
        {
            "unit": lambda n: U.at[pl.ds(0, n)],
            "tile": lambda n: XB.at[pl.ds(0, n)],
            "edge": lambda n: X.at[0, pl.ds(0, n * EDGE)],
            "og": lambda n: OG.at[pl.ds(0, n * EDGE)],
            "taps": lambda n: TS.at[pl.ds(0, n)],
        },
        me,
    )
    for copy in results:
        copy.wait()
    if len(w.index) > RECEIVES:
        raise ValueError(str(len(w.index)))


RECEIVES = 168


def finisher(din_ref, dg_ref, dv_ref, tt_ref, din_out, dg_out, dv_out, tg_out, tv_out):
    din_out[...] = din_ref[...]
    dg_out[...] = dg_ref[...]
    dv_out[...] = dv_ref[...]
    taps = jnp.concatenate([tt_ref[i] for i in range(8)], axis=1)
    tg_out[...] = taps[0:3]
    tv_out[...] = taps[3:6]


def shards(inputs, gate_proj, value_proj, gate_taps, value_taps, out_grad):
    unit = gate_proj.shape
    cols = unit[1]
    factor = float(TOK * NY * NZ) ** (-0.5)
    vm = pltpu.VMEM
    scratch = [
        vm((8, EXT, FEAT), BF16),
        vm((280, *unit), BF16),
        vm((4 * NX + 3, TOK, FEAT), BF16),
        vm((20, 8, cols), F32),
        vm(gate_taps.shape, F32),
        vm(gate_taps.shape, F32),
        vm((384, TOK), BF16),
        vm((EXT, cols), BF16),
        vm((EXT + 16, cols), F32),
        vm((EXT + 16, cols), F32),
        vm((EXT + 16, cols), F32),
        vm((EXT + 16, cols), F32),
        vm((TOK, cols), BF16),
        vm((TOK, cols), BF16),
        vm((TOK, FEAT), BF16),
        vm(unit, F32),
        vm(unit, F32),
        pltpu.SemaphoreType.DMA((5,)),
        pltpu.SemaphoreType.DMA((RECEIVES,)),
        pltpu.SemaphoreType.DMA((10,)),
    ]
    anywhere = pl.BlockSpec(memory_space=pl.ANY)
    vmem = pl.BlockSpec(memory_space=pltpu.VMEM)
    tile = jax.ShapeDtypeStruct((TOK, FEAT), BF16)
    grad = jax.ShapeDtypeStruct(unit, F32)
    tap = jax.ShapeDtypeStruct(gate_taps.shape, F32)
    sums = pl.pallas_call(
        functools.partial(kernel, factor),
        out_shape=(tile, grad, grad, jax.ShapeDtypeStruct((8, 8, cols), F32)),
        in_specs=[anywhere] * 6,
        out_specs=(anywhere,) * 4,
        scratch_shapes=scratch,
        compiler_params=pltpu.CompilerParams(
            collective_id=0, has_side_effects=True, vmem_limit_bytes=65000 * 1024
        ),
    )(inputs[0], gate_proj, value_proj, gate_taps, value_taps, jnp.swapaxes(out_grad[0], 0, 1))
    din, dg, dv, tg, tv = pl.pallas_call(
        finisher,
        out_shape=(tile, grad, grad, tap, tap),
        in_specs=[vmem] * 4,
        out_specs=(vmem,) * 5,
    )(*sums)
    return din[None], dg, dv, tg, tv


def solution(mesh):
    return jax.shard_map(
        shards,
        mesh=mesh,
        in_specs=(P("rep", "fs", "tp"), P("fs", "tp"), P("fs", "tp"), P(), P(), P("rep", "fs", "tp")),
        out_specs=(P("rep", "fs", "tp"), P("fs", "tp"), P("fs", "tp"), P(), P()),
        check_vma=False,
    )
```

```python
import functools

import jax
import jax.numpy as jnp
from jax import lax
from jax.experimental import pallas as pl
from jax.experimental.pallas import tpu as pltpu
from jax.sharding import PartitionSpec as P

MESH = pl.DeviceIdType.MESH
BF16 = jnp.bfloat16
F32 = jnp.float32

NX, NC, NY, NZ = 4, 2, 4, 16
ZL = 8
TOK = 384
COLS = 352
FEAT = 256
EDGE = 16
EXT = TOK + 2 * EDGE
PACK = 176


def right_reach(r):
    return 4 if r < 2 else 3


TREES = {
    "g": {8: 7, 7: 6, 6: 5, 5: 4, 4: 3, 3: 2, 2: 1, 1: 0},
    "v": {8: 7, 7: 6, 6: 5, 5: 4, 4: 0, 3: 2, 2: 1, 1: 0},
}
ITEMS = [(h, k) for h in "gv" for k in range(ZL)]
AHEAD, SPACING = 4, 3


class Wires:
    def __init__(self, send_sems, recv_sems):
        self.send_sems, self.recv_sems = send_sems, recv_sems
        self.index = {}
        self.count = dict.fromkeys(("unit", "pack", "tile", "edge", "og", "taps"), 0)

    def at(self, key):
        return self.index.setdefault(key, len(self.index))

    def copy(self, key, src, dst, to, kind):
        return pltpu.make_async_remote_copy(
            src_ref=src,
            dst_ref=dst,
            send_sem=self.send_sems.at[list(self.count).index(kind)],
            recv_sem=self.recv_sems.at[self.at(key)],
            device_id=to,
            device_id_type=MESH,
        )

    def send(self, key, src, dst, to, kind="unit", amount=1):
        self.count[kind] += amount
        self.copy(key, src, dst, to, kind).start()

    def wait(self, key, dst, to, kind="unit"):
        self.copy(key, dst, dst, to, kind).wait_recv()

    def drain(self, spans, to):
        for kind, span in spans.items():
            whole = span(int(self.count[kind]))
            self.copy(("drain",), whole, whole, to, kind).wait_send()


def kernel(
    factor,
    x_hbm, wg_hbm, wv_hbm, gt_hbm, vt_hbm, ogt_hbm,
    din_hbm, dg_hbm, dv_hbm, tout_hbm,
    X, U, Q, XB, TS, GT, VT, OGT, OG, PG, PV, KG, KV, CG, CV, DIN, DG, DV,
    send_sems, recv_sems, local_sems,
):
    def parts_of(pool, sizes):
        first, parts = 0, []
        for size in sizes:
            parts.append(pool.at[pl.ds(first, size)])
            first += size
        return parts

    WG, WV = parts_of(U, [32] * 2)
    GG, GV, *rest = parts_of(Q, [32] * 2 + [8] * 10 + [9] * 8)
    FAR, DIR, MID, END, RED = ({"g": rest[2 * i], "v": rest[2 * i + 1]} for i in range(5))
    ends = [(h, way) for h in "gv" for way in (1, -1)]
    LAND, SUMS = dict(zip(ends, rest[10:14])), dict(zip(ends, rest[14:18]))
    IP, IR, IS, ISR = parts_of(XB, [2 * NX, NX, NX, 3])
    TY, TZ1, TB, TT = parts_of(TS, [4, 4, 4, 8])
    rep, fs, tp = lax.axis_index("rep"), lax.axis_index("fs"), lax.axis_index("tp")
    zl, y = lax.div(fs, NY), lax.rem(fs, NY)
    x, c = lax.div(tp, NC), lax.rem(tp, NC)
    zg = rep * ZL + zl

    def dev(x=x, c=c, y=y, z=zg):
        z = lax.rem(z + NZ, NZ)
        return (
            lax.div(z, ZL),
            lax.rem(z, ZL) * NY + lax.rem(y + NY, NY),
            lax.rem(x + NX, NX) * NC + c,
        )

    def blk(dz, dy):
        return lax.rem(zl + dz + ZL, ZL) * NY + lax.rem(y + dy + NY, NY)

    def zrow(dz):
        return lax.rem(zl + dz + 2 * ZL, ZL)

    me = dev()
    right, left = dev(z=zg + 1), dev(z=zg - 1)
    up, down = dev(y=y + 1), dev(y=y - 1)
    partner = dev(c=1 - c)
    after_z = zg + lax.div(y + 1, NY)
    after = dev(y=y + 1, z=after_z)
    before_z = zg - 1 + lax.div(y + NY - 1, NY)
    before = dev(y=y - 1, z=before_z)

    def tp_peer(k):
        return (rep, fs, lax.rem(tp + k + 8, 8))

    zq, zo = lax.div(zg, 4), lax.rem(zg, 4)
    side = 4 * (1 - 2 * lax.rem(zq, 2))

    def z_near(k):
        return dev(z=zq * 4 + lax.rem(zo + k, 4))

    own = blk(0, 0)
    loads = [
        pltpu.make_async_copy(wg_hbm, WG.at[own], local_sems.at[0]),
        pltpu.make_async_copy(wv_hbm, WV.at[own], local_sems.at[1]),
        pltpu.make_async_copy(x_hbm, X.at[tp, pl.ds(EDGE, TOK)], local_sems.at[2]),
        pltpu.make_async_copy(ogt_hbm, OGT.at[pl.ds(0, COLS)], local_sems.at[3]),
        pltpu.make_async_copy(gt_hbm, GT, local_sems.at[4]),
        pltpu.make_async_copy(vt_hbm, VT, local_sems.at[5]),
    ]
    for load in loads:
        load.start()

    barrier = pltpu.get_barrier_semaphore()
    peers = [tp_peer(k) for k in range(1, 8)]
    peers += [dev(y=y + k) for k in (1, 2, 3)]
    peers += [right, left, after, before]
    for peer in peers:
        pl.semaphore_signal(barrier, inc=1, device_id=peer, device_id_type=MESH)
    pl.semaphore_wait(barrier, len(peers))

    w = Wires(send_sems, recv_sems)

    loads[0].wait()
    for dy in (1, 3, 2):
        w.send(("gy", dy), WG.at[own], WG.at[own], dev(y=y + dy))
    loads[1].wait()
    w.send(("vz", 1, 1), WV.at[own], WV.at[own], right)
    w.send(("vz", -1, 1), WV.at[own], WV.at[own], left)
    w.send(("gz", 0, 1, 1), WG.at[own], WG.at[own], right)
    w.send(("gz", 0, -1, 1), WG.at[own], WG.at[own], left)
    loads[2].wait()
    head, tail = X.at[tp, pl.ds(EDGE, EDGE)], X.at[tp, pl.ds(TOK, EDGE)]
    lo, hi = pl.ds(0, EDGE), pl.ds(TOK + EDGE, EDGE)
    w.send(("hx", 1), tail, X.at[tp, lo], after, "edge")
    w.send(("hx", -1), head, X.at[tp, hi], before, "edge")
    mine = X.at[tp, pl.ds(EDGE, TOK)]
    HALF = TOK // 2

    def half_of(dx, i):
        return X.at[lax.rem(x - dx + NX, NX) * NC + c, pl.ds(EDGE + HALF * i, HALF)]

    for i in (0, 1):
        for way, part in ((1, half_of(0, i)), (-1, half_of(0, 1 - i))):
            w.send(("x", way, i), part, part, dev(x=x + way), "tile", 0.5)
    w.send(("xp", 0), mine, mine, partner, "tile")
    w.send(("vy", 0, 1), WV.at[own], WV.at[own], up)
    w.send(("vy", 0, -1), WV.at[own], WV.at[own], down)

    def out_grad_rows():
        loads[3].wait()
        for i in range(3):
            for j in range(3):
                block = OGT[128 * i : 128 * i + 128, 128 * j : 128 * j + 128].astype(F32)
                cols = min(128, COLS - 128 * i)
                OG[EDGE + 128 * j : EDGE + 128 * j + 128, 128 * i : 128 * i + cols] = (
                    block.T[:, :cols].astype(BF16)
                )

    def rounded(value):
        return value.astype(BF16).astype(F32)

    def gate_chunk(z, first=False, last=False):
        part = jnp.dot(
            X[z],
            WG[pl.ds(z * NY, NY)].reshape(FEAT, COLS),
            preferred_element_type=F32,
        )
        if first:
            PG[8 : 8 + EXT] = part
        elif last:
            PG[8 : 8 + EXT] = rounded(PG[8 : 8 + EXT] + part)
        else:
            PG[8 : 8 + EXT] += part

    def value_chunk(z, first=False, last=False):
        part = jnp.dot(
            X[z],
            WV[pl.ds(z * NY, NY)].reshape(FEAT, COLS),
            preferred_element_type=F32,
        )
        if first:
            PV[8 : 8 + EXT] = part
        elif last:
            PV[8 : 8 + EXT] = rounded(PV[8 : 8 + EXT] + part)
        else:
            PV[8 : 8 + EXT] += part

    def x_first():
        for way in (1, -1):
            part = half_of(way, (1 - way) // 2)
            w.wait(("x", way, 0), part, me, "tile")
            w.send(("x2", way), part, part, dev(x=x + way), "tile", 0.5)

    def x_whole(dx):
        slot = X.at[lax.rem(x - dx + NX, NX) * NC + c, pl.ds(EDGE, TOK)]
        w.send(("xp", dx), slot, slot, partner, "tile")

    def x_near():
        for way in (1, -1):
            w.wait(("x", way, 1), half_of(way, (1 + way) // 2), me, "tile")
            x_whole(way)

    def x_far():
        for way in (1, -1):
            w.wait(("x2", way), half_of(2, (1 - way) // 2), me, "tile")
        x_whole(2)

    def xp_arrived(dx):
        slot = X.at[lax.rem(x - dx + NX, NX) * NC + 1 - c, pl.ds(EDGE, TOK)]
        w.wait(("xp", dx), slot, me, "tile")

    def edges_spread():
        w.wait(("hx", 1), X.at[tp, lo], me, "edge")
        w.wait(("hx", -1), X.at[tp, hi], me, "edge")
        for k in range(1, 8):
            w.send(("hl",), X.at[tp, lo], X.at[tp, lo], tp_peer(k), "edge")
            w.send(("hl",), X.at[tp, hi], X.at[tp, hi], tp_peer(k), "edge")

    def edges_done():
        w.wait(("hl",), X.at[0, pl.ds(0, 14 * EDGE)], me, "edge")

    def gate_y(dy):
        unit = WG.at[blk(0, -dy)]
        w.wait(("gy", dy), unit, me)
        w.send(("gz", 4 - dy, 1, 1), unit, unit, right)
        w.send(("gz", 4 - dy, -1, 1), unit, unit, left)

    def gate_z(r, d):
        for way, reach, to in ((1, right_reach(r), right), (-1, 7 - right_reach(r), left)):
            if d <= reach:
                unit = WG.at[blk(-way * d, r)]
                w.wait(("gz", r, way, d), unit, me)
                if d < reach:
                    w.send(("gz", r, way, d + 1), unit, unit, to)

    def value_z(d):
        for way, reach, to in ((1, 4, right), (-1, 3, left)):
            if d <= reach:
                dz = -way * d
                unit = WV.at[blk(dz, 0)]
                w.wait(("vz", way, d), unit, me)
                if d < reach:
                    w.send(("vz", way, d + 1), unit, unit, to)
                w.send(("vy", dz, 1), unit, unit, up)
                w.send(("vy", dz, -1), unit, unit, down)
                if d == 4:
                    w.send(("vf", dz), unit, unit, dev(y=y + 2))

    def value_y(dz):
        from_down, from_up = WV.at[blk(dz, -1)], WV.at[blk(dz, 1)]
        w.wait(("vy", dz, 1), from_down, me)
        if dz % 2 == 0 and dz != -4:
            w.send(("vf", dz), from_down, from_down, up)
        w.wait(("vy", dz, -1), from_up, me)
        if dz % 2 == 1:
            w.send(("vf", dz), from_up, from_up, down)

    def value_row(dz, first=False, last=False):
        w.wait(("vf", dz), WV.at[blk(dz, 2)], me)
        value_chunk(zrow(dz), first, last)

    value_z(1)
    gate_y(1)
    gate_y(3)
    gate_y(2)
    gate_z(0, 1)
    value_y(0)
    value_z(2)
    gate_z(3, 1)
    x_first()
    gate_z(1, 1)
    edges_spread()
    gate_z(2, 1)
    value_y(1)
    value_y(-1)
    x_near()
    out_grad_rows()
    gate_z(0, 2)
    value_z(3)
    x_far()
    w.send(("og", 1), OG.at[pl.ds(TOK, EDGE)], OG.at[lo], after, "og")
    w.send(("og", -1), OG.at[pl.ds(EDGE, EDGE)], OG.at[hi], before, "og")
    gate_z(3, 2)
    value_y(2)
    value_y(-2)
    gate_z(1, 2)
    gate_z(2, 2)
    gate_z(0, 3)
    value_z(4)
    for dx in (0, 1, -1, 2):
        xp_arrived(dx)
    edges_done()
    gate_chunk(zrow(0), first=True)
    gate_chunk(zrow(1))
    gate_z(3, 3)
    gate_chunk(zrow(-1))
    value_y(3)
    value_y(-3)
    gate_z(1, 3)
    value_row(0, first=True)
    gate_chunk(zrow(2))
    gate_z(2, 3)
    gate_chunk(zrow(-2))
    value_row(1)
    gate_z(0, 4)
    value_row(-1)
    value_row(2)
    gate_chunk(zrow(3))
    gate_z(3, 4)
    value_row(-2)
    gate_chunk(zrow(-3))
    value_y(-4)
    value_row(3)
    gate_z(1, 4)
    value_row(-3)
    value_row(-4, last=True)
    gate_z(2, 4)
    gate_chunk(zrow(4), last=True)
    w.wait(("og", 1), OG.at[lo], me, "og")
    w.wait(("og", -1), OG.at[hi], me, "og")

    not_first, not_last = fs > 0, fs < NY * ZL - 1
    for ref in (PG, PV):
        ref[8 : 8 + EDGE] = jnp.where(not_first, ref[8 : 8 + EDGE], 0.0)
        ref[8 + EDGE + TOK : 8 + EXT] = jnp.where(not_last, ref[8 + EDGE + TOK : 8 + EXT], 0.0)
    OG[:EDGE] = jnp.where(not_first, OG[:EDGE].astype(F32), 0.0).astype(BF16)
    OG[EDGE + TOK :] = jnp.where(not_last, OG[EDGE + TOK :].astype(F32), 0.0).astype(BF16)

    loads[4].wait()
    loads[5].wait()
    taps = jnp.concatenate([GT[...], VT[...], jnp.zeros((2, 8 * COLS), F32)], axis=0)
    taps = pltpu.roll(taps, lax.rem((8 - tp) * COLS, 8 * COLS), axis=1)[:, :COLS]
    g0, g1, g2, v0, v1, v2 = (taps[k : k + 1] for k in range(6))

    def cot_rows(i):
        base = pl.multiple_of(i * 16, 16)
        gate = PG[pl.ds(base, 32)]
        value = PV[pl.ds(base, 32)]
        gm, gz, gp = gate[7:23], gate[8:24], gate[9:25]
        vm, vz, vp = value[7:23], value[8:24], value[9:25]
        gate_mix = g0 * gm + g1 * gz + g2 * gp
        value_mix = v0 * vm + v1 * vz + v2 * vp
        grad = OG[pl.ds(base, 16)].astype(F32)
        s = jax.nn.sigmoid(gate_mix)
        gate_cot = grad * value_mix * (s * (1.0 + gate_mix * (1.0 - s)))
        value_cot = grad * (gate_mix * s)
        KG[pl.ds(base + 8, 16)] = gate_cot
        KV[pl.ds(base + 8, 16)] = value_cot
        return [
            (p * k).reshape(2, 8, COLS).sum(axis=0)
            for p, k in (
                (gm, gate_cot), (gz, gate_cot), (gp, gate_cot),
                (vm, value_cot), (vz, value_cot), (vp, value_cot),
            )
        ]

    cot_rows(0)
    cot_rows(TOK // 16 + 1)
    zero = jnp.zeros((8, COLS), F32)
    tap_sums = lax.fori_loop(
        1, TOK // 16 + 1,
        lambda i, sums: tuple(a + b for a, b in zip(sums, cot_rows(i))),
        (zero,) * 6,
    )

    def back_all(source, target, t0, t1, t2):
        def back_rows(i, carry):
            cot = source[pl.ds(pl.multiple_of(i * 16, 16), 32)]
            out = pl.ds(pl.multiple_of(i * 16 - 16, 16), 16)
            target[out] = (t0 * cot[9:25] + t1 * cot[8:24] + t2 * cot[7:23]).astype(BF16)
            return carry

        lax.fori_loop(1, TOK // 16 + 1, back_rows, 0)

    back_all(KG, CG, g0, g1, g2)

    rows = [jnp.sum(part, axis=0, keepdims=True) for part in tap_sums]
    TY[y] = jnp.concatenate(rows + [jnp.zeros((2, COLS), F32)], axis=0)

    order = (0, 1, -1, 2, -2, 3, -3, 4)
    place = {dz % ZL: k for k, dz in enumerate(order)}
    COT, TERMS = {"g": CG, "v": CV}, {"g": GG, "v": GV}

    def turn(h, k):
        return (1, up, down) if (k % 2 == 0) == (h == "g") else (-1, down, up)

    def packed(block, out):
        out[0:64] = block[:, :128].astype(BF16)
        out[64:128] = block[:, 128:256].astype(BF16)
        rest = block[:, 256:]
        for j in range(3):
            row = jnp.concatenate([rest[16 * j : 16 * j + 16], rest[48:64, 32 * j : 32 * j + 32]], axis=1)
            out[128 + 16 * j : 144 + 16 * j] = row.astype(BF16)

    def unpacked(block, out):
        out[:, :128] = block[0:64]
        out[:, 128:256] = block[64:128]
        last = jnp.concatenate([block[128 + 16 * j : 144 + 16 * j, 96:] for j in range(3)], axis=1)
        out[:, 256:] = jnp.concatenate([block[128:, :96], last], axis=0)

    def make_blocks(h, k):
        dz = order[k]
        z = zrow(dz)
        block = lax.dot_general(
            X[z, EDGE : EDGE + TOK, :], COT[h][...],
            (((0,), (0,)), ((), ())), preferred_element_type=F32,
        )
        for i in range(NY):
            packed(block[64 * i : 64 * i + 64], TERMS[h].at[z * NY + i])
        way, onward, back = turn(h, k)
        w.send(("far", h, k), TERMS[h].at[blk(dz, 2)], FAR[h].at[k], onward, "pack")
        w.send(("dir", h, k), TERMS[h].at[blk(dz, -way)], DIR[h].at[k], back, "pack")

    def total(*parts):
        acc = parts[0].astype(F32)
        for part in parts[1:]:
            acc = acc + part.astype(F32)
        return acc

    def pass_on(h, k):
        way, onward, back = turn(h, k)
        w.wait(("far", h, k), FAR[h].at[k], me, "pack")
        MID[h][k] = total(FAR[h][k], TERMS[h][blk(order[k], way)]).astype(BF16)
        w.send(("mid", h, k), MID[h].at[k], END[h].at[k], onward, "pack")

    def row_done(h, k):
        w.wait(("dir", h, k), DIR[h].at[k], me, "pack")
        w.wait(("mid", h, k), END[h].at[k], me, "pack")
        RED[h][k] = total(TERMS[h][blk(order[k], 0)], DIR[h][k], END[h][k]).astype(BF16)

    def start_of(h, way):
        return 8 if (h == "g") == (way == 1) else 7

    def row_at(way, d):
        return place[(way * d) % ZL]

    def sources(h, way, d):
        return [e for e in range(start_of(h, way), d, -1) if TREES[h][e] == d]

    def arrived(h, way, d):
        landing = LAND[h, way]
        for e in sources(h, way, d):
            w.wait((h, way, e), landing.at[e], me, "pack")
        return [landing[e] for e in sources(h, way, d)]

    def hop(h, way, d):
        k = row_at(way, d)
        source = RED[h].at[k]
        if sources(h, way, d):
            SUMS[h, way][d] = total(*arrived(h, way, d), RED[h][k]).astype(BF16)
            source = SUMS[h, way].at[d]
        w.send((h, way, d), source, LAND[h, way].at[d], dev(z=zg + way * (d - TREES[h][d])), "pack")

    def finish(h, out):
        parts = arrived(h, 1, 0) + arrived(h, -1, 0)
        unpacked(total(RED[h][place[0]], *parts) * factor, out)

    def input_terms(j):
        part = lax.dot_general(
            CG[...], WG[NY * j : NY * j + NY].reshape(FEAT, COLS),
            (((1,), (1,)), ((), ())), preferred_element_type=F32,
        ) + lax.dot_general(
            CV[...], WV[NY * j : NY * j + NY].reshape(FEAT, COLS),
            (((1,), (1,)), ((), ())), preferred_element_type=F32,
        )
        IP[NX * (j % 2) + j // 2] = part.astype(BF16)

    def input_swap():
        for i in range(NX):
            w.send(("ip", i), IP.at[NX * (1 - c) + i], IR.at[i], partner, "tile")

    def input_sums():
        for i in range(NX):
            w.wait(("ip", i), IR.at[i], me, "tile")
            IS[i] = total(IP[NX * c + i], IR[i]).astype(BF16)
        for dx in (1, 3, 2):
            w.send(("is", dx), IS.at[lax.rem(x + dx, NX)], ISR.at[dx - 1], dev(x=x + dx), "tile")

    results = []

    def put_out(source, target):
        copy = pltpu.make_async_copy(source, target, local_sems.at[6 + len(results)])
        copy.start()
        results.append(copy)

    def input_done():
        for dx in (1, 3, 2):
            w.wait(("is", dx), ISR.at[dx - 1], me, "tile")
        DIN[...] = total(IP[NX * c + x], IR[x], ISR[0], ISR[1], ISR[2]).astype(BF16)
        put_out(DIN, din_hbm)

    def taps_y():
        for dy in (1, 2, 3):
            w.send(("ty",), TY.at[y], TY.at[y], dev(y=y + dy), "taps")

    def taps_z():
        w.wait(("ty",), TY.at[pl.ds(0, 3)], me, "taps")
        TZ1[zo] = TY[0] + TY[1] + TY[2] + TY[3]
        for k in (1, 2, 3):
            w.send(("tz",), TZ1.at[zo], TZ1.at[zo], z_near(k), "taps")

    def taps_pair(stage):
        if stage == 0:
            w.wait(("tz",), TZ1.at[pl.ds(0, 3)], me, "taps")
            TB[0] = TZ1[0] + TZ1[1] + TZ1[2] + TZ1[3]
            w.send(("tb", 0), TB.at[0], TB.at[1], dev(z=zg + side), "taps")
        else:
            w.wait(("tb", 0), TB.at[1], me, "taps")
            TB[2] = TB[0] + TB[1]
            w.send(("tb", 1), TB.at[2], TB.at[3], dev(z=zg - side), "taps")

    def taps_spread():
        w.wait(("tb", 1), TB.at[3], me, "taps")
        TT[tp] = (TB[2] + TB[3]) * factor
        for k in range(1, 8):
            w.send(("tt",), TT.at[tp], TT.at[tp], tp_peer(k), "taps")

    def taps_done():
        w.wait(("tt",), TT.at[pl.ds(0, 7)], me, "taps")
        put_out(TT, tout_hbm)

    ahead, lag, spacing = AHEAD, 3, SPACING
    row_step = {item: t + lag for t, item in enumerate(ITEMS)}
    hop_step = {}
    for h, way in ends:
        for d in range(start_of(h, way), 0, -1):
            steps = [hop_step[h, way, e] + spacing + e - d - 1 for e in sources(h, way, d)]
            hop_step[h, way, d] = max([row_step[h, row_at(way, d)], *steps])
    items = ITEMS
    extra = {4: [taps_z], 5: [input_swap], 8: [lambda: taps_pair(0)], 9: [input_sums], 13: [lambda: taps_pair(1)],
             19: [taps_spread]}
    for j in range(4, 8):
        extra.setdefault(j - 3, []).insert(0, functools.partial(input_terms, j))
    for item in items[:ahead]:
        make_blocks(*item)
    taps_y()
    back_all(KV, CV, v0, v1, v2)
    for j in range(4):
        input_terms(j)
    for step in range(max(hop_step.values()) + 1):
        if step < len(items):
            pass_on(*items[step])
        if step + ahead < len(items):
            make_blocks(*items[step + ahead])
        if 0 <= step - lag < len(items):
            row_done(*items[step - lag])
        for key in sorted(hop_step, key=hop_step.get):
            if hop_step[key] == step:
                hop(*key)
        for run in extra.get(step, ()):
            run()
    input_done()
    taps_done()
    finish("g", DG)
    put_out(DG, dg_hbm)
    finish("v", DV)
    put_out(DV, dv_hbm)
    w.drain(
        {
            "unit": lambda n: U.at[pl.ds(0, n)],
            "pack": lambda n: Q.at[pl.ds(0, n)],
            "tile": lambda n: XB.at[pl.ds(0, n)],
            "edge": lambda n: X.at[0, pl.ds(0, n * EDGE)],
            "og": lambda n: OG.at[pl.ds(0, n * EDGE)],
            "taps": lambda n: TS.at[pl.ds(0, n)],
        },
        me,
    )
    for copy in results:
        copy.wait()
    if len(w.index) > RECEIVES:
        raise ValueError(str(len(w.index)))


RECEIVES = 168


def finisher(din_ref, dg_ref, dv_ref, tt_ref, din_out, dg_out, dv_out, tg_out, tv_out):
    din_out[...] = din_ref[...]
    dg_out[...] = dg_ref[...]
    dv_out[...] = dv_ref[...]
    taps = jnp.concatenate([tt_ref[i] for i in range(8)], axis=1)
    tg_out[...] = taps[0:3]
    tv_out[...] = taps[3:6]


def shards(inputs, gate_proj, value_proj, gate_taps, value_taps, out_grad):
    unit = gate_proj.shape
    cols = unit[1]
    factor = float(TOK * NY * NZ) ** (-0.5)
    vm = pltpu.VMEM
    scratch = [
        vm((8, EXT, FEAT), BF16),
        vm((64, *unit), BF16),
        vm((216, PACK, 128), BF16),
        vm((4 * NX + 3, TOK, FEAT), BF16),
        vm((20, 8, cols), F32),
        vm(gate_taps.shape, F32),
        vm(gate_taps.shape, F32),
        vm((384, TOK), BF16),
        vm((EXT, cols), BF16),
        vm((EXT + 16, cols), F32),
        vm((EXT + 16, cols), F32),
        vm((EXT + 16, cols), F32),
        vm((EXT + 16, cols), F32),
        vm((TOK, cols), BF16),
        vm((TOK, cols), BF16),
        vm((TOK, FEAT), BF16),
        vm(unit, F32),
        vm(unit, F32),
        pltpu.SemaphoreType.DMA((6,)),
        pltpu.SemaphoreType.DMA((RECEIVES,)),
        pltpu.SemaphoreType.DMA((10,)),
    ]
    anywhere = pl.BlockSpec(memory_space=pl.ANY)
    vmem = pl.BlockSpec(memory_space=pltpu.VMEM)
    tile = jax.ShapeDtypeStruct((TOK, FEAT), BF16)
    grad = jax.ShapeDtypeStruct(unit, F32)
    tap = jax.ShapeDtypeStruct(gate_taps.shape, F32)
    sums = pl.pallas_call(
        functools.partial(kernel, factor),
        out_shape=(tile, grad, grad, jax.ShapeDtypeStruct((8, 8, cols), F32)),
        in_specs=[anywhere] * 6,
        out_specs=(anywhere,) * 4,
        scratch_shapes=scratch,
        compiler_params=pltpu.CompilerParams(
            collective_id=0, has_side_effects=True, vmem_limit_bytes=65000 * 1024
        ),
    )(inputs[0], gate_proj, value_proj, gate_taps, value_taps, jnp.swapaxes(out_grad[0], 0, 1))
    din, dg, dv, tg, tv = pl.pallas_call(
        finisher,
        out_shape=(tile, grad, grad, tap, tap),
        in_specs=[vmem] * 4,
        out_specs=(vmem,) * 5,
    )(*sums)
    return din[None], dg, dv, tg, tv


def solution(mesh):
    return jax.shard_map(
        shards,
        mesh=mesh,
        in_specs=(P("rep", "fs", "tp"), P("fs", "tp"), P("fs", "tp"), P(), P(), P("rep", "fs", "tp")),
        out_specs=(P("rep", "fs", "tp"), P("fs", "tp"), P("fs", "tp"), P(), P()),
        check_vma=False,
    )
```

```python
import functools

import jax
import jax.numpy as jnp
from jax import lax
from jax.experimental import pallas as pl
from jax.experimental.pallas import tpu as pltpu
from jax.sharding import PartitionSpec as P

MESH = pl.DeviceIdType.MESH
BF16 = jnp.bfloat16
F32 = jnp.float32

NX, NC, NY, NZ = 4, 2, 4, 16
ZL = 8
TOK = 384
COLS = 352
FEAT = 256
EDGE = 16
EXT = TOK + 2 * EDGE
PACK = 176


def right_reach(r):
    return 4 if r < 2 else 3


TREES = {
    "g": {8: 7, 7: 6, 6: 5, 5: 4, 4: 3, 3: 2, 2: 1, 1: 0},
    "v": {8: 7, 7: 6, 6: 5, 5: 4, 4: 0, 3: 2, 2: 1, 1: 0},
}
ITEMS = [(h, k) for h in "gv" for k in range(ZL)]
AHEAD, SPACING = 4, 3


class Wires:
    def __init__(self, send_sems, recv_sems):
        self.send_sems, self.recv_sems = send_sems, recv_sems
        self.index = {}
        self.count = dict.fromkeys(("unit", "pack", "tile", "edge", "og", "taps"), 0)

    def at(self, key):
        return self.index.setdefault(key, len(self.index))

    def copy(self, key, src, dst, to, kind):
        return pltpu.make_async_remote_copy(
            src_ref=src,
            dst_ref=dst,
            send_sem=self.send_sems.at[list(self.count).index(kind)],
            recv_sem=self.recv_sems.at[self.at(key)],
            device_id=to,
            device_id_type=MESH,
        )

    def send(self, key, src, dst, to, kind="unit", amount=1):
        self.count[kind] += amount
        self.copy(key, src, dst, to, kind).start()

    def wait(self, key, dst, to, kind="unit"):
        self.copy(key, dst, dst, to, kind).wait_recv()

    def drain(self, spans, to):
        for kind, span in spans.items():
            whole = span(int(self.count[kind]))
            self.copy(("drain",), whole, whole, to, kind).wait_send()


def kernel(
    factor,
    x_hbm, wg_hbm, wv_hbm, gt_hbm, vt_hbm, ogt_hbm,
    din_hbm, dg_hbm, dv_hbm, tout_hbm,
    X, U, Q, XB, TS, GT, VT, OGT, OG, PG, PV, KG, KV, CG, CV, DIN, DG, DV,
    send_sems, recv_sems, local_sems,
):
    def parts_of(pool, sizes):
        first, parts = 0, []
        for size in sizes:
            parts.append(pool.at[pl.ds(first, size)])
            first += size
        return parts

    WG, WV = parts_of(U, [32] * 2)
    GG, GV, *rest = parts_of(Q, [32] * 2 + [8] * 10 + [9] * 8)
    FAR, DIR, MID, END, RED = ({"g": rest[2 * i], "v": rest[2 * i + 1]} for i in range(5))
    ends = [(h, way) for h in "gv" for way in (1, -1)]
    LAND, SUMS = dict(zip(ends, rest[10:14])), dict(zip(ends, rest[14:18]))
    IP, IR, IS, ISR = parts_of(XB, [2 * NX, NX, NX, 3])
    TY, TZ1, TB, TT = parts_of(TS, [4, 4, 4, 8])
    rep, fs, tp = lax.axis_index("rep"), lax.axis_index("fs"), lax.axis_index("tp")
    zl, y = lax.div(fs, NY), lax.rem(fs, NY)
    x, c = lax.div(tp, NC), lax.rem(tp, NC)
    zg = rep * ZL + zl

    def dev(x=x, c=c, y=y, z=zg):
        z = lax.rem(z + NZ, NZ)
        return (
            lax.div(z, ZL),
            lax.rem(z, ZL) * NY + lax.rem(y + NY, NY),
            lax.rem(x + NX, NX) * NC + c,
        )

    def blk(dz, dy):
        return lax.rem(zl + dz + ZL, ZL) * NY + lax.rem(y + dy + NY, NY)

    def zrow(dz):
        return lax.rem(zl + dz + 2 * ZL, ZL)

    me = dev()
    right, left = dev(z=zg + 1), dev(z=zg - 1)
    up, down = dev(y=y + 1), dev(y=y - 1)
    partner = dev(c=1 - c)
    after_z = zg + lax.div(y + 1, NY)
    after = dev(y=y + 1, z=after_z)
    before_z = zg - 1 + lax.div(y + NY - 1, NY)
    before = dev(y=y - 1, z=before_z)

    def tp_peer(k):
        return (rep, fs, lax.rem(tp + k + 8, 8))

    zq, zo = lax.div(zg, 4), lax.rem(zg, 4)
    side = 4 * (1 - 2 * lax.rem(zq, 2))

    def z_near(k):
        return dev(z=zq * 4 + lax.rem(zo + k, 4))

    own = blk(0, 0)
    loads = [
        pltpu.make_async_copy(wg_hbm, WG.at[own], local_sems.at[0]),
        pltpu.make_async_copy(wv_hbm, WV.at[own], local_sems.at[1]),
        pltpu.make_async_copy(x_hbm, X.at[tp, pl.ds(EDGE, TOK)], local_sems.at[2]),
        pltpu.make_async_copy(ogt_hbm, OGT.at[pl.ds(0, COLS)], local_sems.at[3]),
        pltpu.make_async_copy(gt_hbm, GT, local_sems.at[4]),
        pltpu.make_async_copy(vt_hbm, VT, local_sems.at[5]),
    ]
    for load in loads:
        load.start()

    barrier = pltpu.get_barrier_semaphore()
    peers = [tp_peer(k) for k in range(1, 8)]
    peers += [dev(y=y + k) for k in (1, 2, 3)]
    peers += [right, left, after, before]
    for peer in peers:
        pl.semaphore_signal(barrier, inc=1, device_id=peer, device_id_type=MESH)
    pl.semaphore_wait(barrier, len(peers))

    w = Wires(send_sems, recv_sems)

    loads[0].wait()
    for dy in (1, 3, 2):
        w.send(("gy", dy), WG.at[own], WG.at[own], dev(y=y + dy))
    loads[1].wait()
    w.send(("vz", 1, 1), WV.at[own], WV.at[own], right)
    w.send(("vz", -1, 1), WV.at[own], WV.at[own], left)
    w.send(("gz", 0, 1, 1), WG.at[own], WG.at[own], right)
    w.send(("gz", 0, -1, 1), WG.at[own], WG.at[own], left)
    loads[2].wait()
    head, tail = X.at[tp, pl.ds(EDGE, EDGE)], X.at[tp, pl.ds(TOK, EDGE)]
    lo, hi = pl.ds(0, EDGE), pl.ds(TOK + EDGE, EDGE)
    w.send(("hx", 1), tail, X.at[tp, lo], after, "edge")
    w.send(("hx", -1), head, X.at[tp, hi], before, "edge")
    mine = X.at[tp, pl.ds(EDGE, TOK)]
    HALF = TOK // 2

    def half_of(dx, i):
        return X.at[lax.rem(x - dx + NX, NX) * NC + c, pl.ds(EDGE + HALF * i, HALF)]

    for i in (0, 1):
        for way, part in ((1, half_of(0, i)), (-1, half_of(0, 1 - i))):
            w.send(("x", way, i), part, part, dev(x=x + way), "tile", 0.5)
    w.send(("xp", 0), mine, mine, partner, "tile")
    w.send(("vy", 0, 1), WV.at[own], WV.at[own], up)
    w.send(("vy", 0, -1), WV.at[own], WV.at[own], down)

    def out_grad_rows():
        loads[3].wait()
        for i in range(3):
            for j in range(3):
                block = OGT[128 * i : 128 * i + 128, 128 * j : 128 * j + 128].astype(F32)
                cols = min(128, COLS - 128 * i)
                OG[EDGE + 128 * j : EDGE + 128 * j + 128, 128 * i : 128 * i + cols] = (
                    block.T[:, :cols].astype(BF16)
                )

    def rounded(value):
        return value.astype(BF16).astype(F32)

    def gate_chunk(z, first=False, last=False):
        part = jnp.dot(
            X[z],
            WG[pl.ds(z * NY, NY)].reshape(FEAT, COLS),
            preferred_element_type=F32,
        )
        if first:
            PG[8 : 8 + EXT] = part
        elif last:
            PG[8 : 8 + EXT] = rounded(PG[8 : 8 + EXT] + part)
        else:
            PG[8 : 8 + EXT] += part

    def value_chunk(z, first=False, last=False):
        part = jnp.dot(
            X[z],
            WV[pl.ds(z * NY, NY)].reshape(FEAT, COLS),
            preferred_element_type=F32,
        )
        if first:
            PV[8 : 8 + EXT] = part
        elif last:
            PV[8 : 8 + EXT] = rounded(PV[8 : 8 + EXT] + part)
        else:
            PV[8 : 8 + EXT] += part

    def x_first():
        for way in (1, -1):
            part = half_of(way, (1 - way) // 2)
            w.wait(("x", way, 0), part, me, "tile")
            w.send(("x2", way), part, part, dev(x=x + way), "tile", 0.5)

    def x_whole(dx):
        slot = X.at[lax.rem(x - dx + NX, NX) * NC + c, pl.ds(EDGE, TOK)]
        w.send(("xp", dx), slot, slot, partner, "tile")

    def x_near():
        for way in (1, -1):
            w.wait(("x", way, 1), half_of(way, (1 + way) // 2), me, "tile")
            x_whole(way)

    def x_far():
        for way in (1, -1):
            w.wait(("x2", way), half_of(2, (1 - way) // 2), me, "tile")
        x_whole(2)

    def xp_arrived(dx):
        slot = X.at[lax.rem(x - dx + NX, NX) * NC + 1 - c, pl.ds(EDGE, TOK)]
        w.wait(("xp", dx), slot, me, "tile")

    def edges_spread():
        w.wait(("hx", 1), X.at[tp, lo], me, "edge")
        w.wait(("hx", -1), X.at[tp, hi], me, "edge")
        for k in range(1, 8):
            w.send(("hl",), X.at[tp, lo], X.at[tp, lo], tp_peer(k), "edge")
            w.send(("hl",), X.at[tp, hi], X.at[tp, hi], tp_peer(k), "edge")

    def edges_done():
        w.wait(("hl",), X.at[0, pl.ds(0, 14 * EDGE)], me, "edge")

    def gate_y(dy):
        unit = WG.at[blk(0, -dy)]
        w.wait(("gy", dy), unit, me)
        w.send(("gz", 4 - dy, 1, 1), unit, unit, right)
        w.send(("gz", 4 - dy, -1, 1), unit, unit, left)

    def gate_z(r, d):
        for way, reach, to in ((1, right_reach(r), right), (-1, 7 - right_reach(r), left)):
            if d <= reach:
                unit = WG.at[blk(-way * d, r)]
                w.wait(("gz", r, way, d), unit, me)
                if d < reach:
                    w.send(("gz", r, way, d + 1), unit, unit, to)

    def value_z(d):
        for way, reach, to in ((1, 4, right), (-1, 3, left)):
            if d <= reach:
                dz = -way * d
                unit = WV.at[blk(dz, 0)]
                w.wait(("vz", way, d), unit, me)
                if d < reach:
                    w.send(("vz", way, d + 1), unit, unit, to)
                w.send(("vy", dz, 1), unit, unit, up)
                w.send(("vy", dz, -1), unit, unit, down)
                if d == 4:
                    w.send(("vf", dz), unit, unit, dev(y=y + 2))

    def value_y(dz):
        from_down, from_up = WV.at[blk(dz, -1)], WV.at[blk(dz, 1)]
        w.wait(("vy", dz, 1), from_down, me)
        if dz % 2 == 0 and dz != -4:
            w.send(("vf", dz), from_down, from_down, up)
        w.wait(("vy", dz, -1), from_up, me)
        if dz % 2 == 1:
            w.send(("vf", dz), from_up, from_up, down)

    def value_row(dz, first=False, last=False):
        w.wait(("vf", dz), WV.at[blk(dz, 2)], me)
        value_chunk(zrow(dz), first, last)

    value_z(1)
    gate_y(1)
    gate_y(3)
    gate_y(2)
    gate_z(0, 1)
    value_y(0)
    value_z(2)
    gate_z(3, 1)
    x_first()
    gate_z(1, 1)
    edges_spread()
    gate_z(2, 1)
    value_y(1)
    value_y(-1)
    x_near()
    out_grad_rows()
    gate_z(0, 2)
    value_z(3)
    x_far()
    w.send(("og", 1), OG.at[pl.ds(TOK, EDGE)], OG.at[lo], after, "og")
    w.send(("og", -1), OG.at[pl.ds(EDGE, EDGE)], OG.at[hi], before, "og")
    gate_z(3, 2)
    value_y(2)
    value_y(-2)
    gate_z(1, 2)
    gate_z(2, 2)
    gate_z(0, 3)
    value_z(4)
    for dx in (0, 1, -1, 2):
        xp_arrived(dx)
    edges_done()
    gate_chunk(zrow(0), first=True)
    gate_chunk(zrow(1))
    gate_z(3, 3)
    gate_chunk(zrow(-1))
    value_y(3)
    value_y(-3)
    gate_z(1, 3)
    value_row(0, first=True)
    gate_chunk(zrow(2))
    gate_z(2, 3)
    gate_chunk(zrow(-2))
    value_row(1)
    gate_z(0, 4)
    value_row(-1)
    value_row(2)
    gate_chunk(zrow(3))
    gate_z(3, 4)
    value_row(-2)
    gate_chunk(zrow(-3))
    value_y(-4)
    value_row(3)
    gate_z(1, 4)
    value_row(-3)
    value_row(-4, last=True)
    gate_z(2, 4)
    gate_chunk(zrow(4), last=True)
    w.wait(("og", 1), OG.at[lo], me, "og")
    w.wait(("og", -1), OG.at[hi], me, "og")

    not_first, not_last = fs > 0, fs < NY * ZL - 1
    for ref in (PG, PV):
        ref[8 : 8 + EDGE] = jnp.where(not_first, ref[8 : 8 + EDGE], 0.0)
        ref[8 + EDGE + TOK : 8 + EXT] = jnp.where(not_last, ref[8 + EDGE + TOK : 8 + EXT], 0.0)
    OG[:EDGE] = jnp.where(not_first, OG[:EDGE].astype(F32), 0.0).astype(BF16)
    OG[EDGE + TOK :] = jnp.where(not_last, OG[EDGE + TOK :].astype(F32), 0.0).astype(BF16)

    loads[4].wait()
    loads[5].wait()
    taps = jnp.concatenate([GT[...], VT[...], jnp.zeros((2, 8 * COLS), F32)], axis=0)
    taps = pltpu.roll(taps, lax.rem((8 - tp) * COLS, 8 * COLS), axis=1)[:, :COLS]
    g0, g1, g2, v0, v1, v2 = (taps[k : k + 1] for k in range(6))

    def cot_rows(i):
        base = pl.multiple_of(i * 16, 16)
        gate = PG[pl.ds(base, 32)]
        value = PV[pl.ds(base, 32)]
        gm, gz, gp = gate[7:23], gate[8:24], gate[9:25]
        vm, vz, vp = value[7:23], value[8:24], value[9:25]
        gate_mix = g0 * gm + g1 * gz + g2 * gp
        value_mix = v0 * vm + v1 * vz + v2 * vp
        grad = OG[pl.ds(base, 16)].astype(F32)
        s = jax.nn.sigmoid(gate_mix)
        gate_cot = grad * value_mix * (s * (1.0 + gate_mix * (1.0 - s)))
        value_cot = grad * (gate_mix * s)
        KG[pl.ds(base + 8, 16)] = gate_cot
        KV[pl.ds(base + 8, 16)] = value_cot

    def all_cots(i, carry):
        cot_rows(i)
        return carry

    lax.fori_loop(0, TOK // 16 + 2, all_cots, 0)

    def tap_rows(i, sums):
        base = pl.multiple_of(i * 16, 16)
        terms = []
        for pre, cot in ((PG, KG), (PV, KV)):
            rows, cots = pre[pl.ds(base, 32)], cot[pl.ds(base + 8, 16)]
            terms += [(rows[7 + k : 23 + k] * cots).reshape(2, 8, COLS).sum(axis=0) for k in range(3)]
        return tuple(a + b for a, b in zip(sums, terms))

    def taps_own():
        sums = lax.fori_loop(1, TOK // 16 + 1, tap_rows, (jnp.zeros((8, COLS), F32),) * 6)
        rows = [jnp.sum(part, axis=0, keepdims=True) for part in sums]
        TY[y] = jnp.concatenate(rows + [jnp.zeros((2, COLS), F32)], axis=0)

    def back_all(source, target, t0, t1, t2):
        def back_rows(i, carry):
            cot = source[pl.ds(pl.multiple_of(i * 16, 16), 32)]
            out = pl.ds(pl.multiple_of(i * 16 - 16, 16), 16)
            target[out] = (t0 * cot[9:25] + t1 * cot[8:24] + t2 * cot[7:23]).astype(BF16)
            return carry

        lax.fori_loop(1, TOK // 16 + 1, back_rows, 0)

    back_all(KG, CG, g0, g1, g2)

    order = (0, 1, -1, 2, -2, 3, -3, 4)
    place = {dz % ZL: k for k, dz in enumerate(order)}
    COT, TERMS = {"g": CG, "v": CV}, {"g": GG, "v": GV}

    def turn(h, k):
        return (1, up, down) if (k % 2 == 0) == (h == "g") else (-1, down, up)

    def packed(block, out):
        out[0:64] = block[:, :128].astype(BF16)
        out[64:128] = block[:, 128:256].astype(BF16)
        rest = block[:, 256:]
        for j in range(3):
            row = jnp.concatenate([rest[16 * j : 16 * j + 16], rest[48:64, 32 * j : 32 * j + 32]], axis=1)
            out[128 + 16 * j : 144 + 16 * j] = row.astype(BF16)

    def unpacked(block, out):
        out[:, :128] = block[0:64]
        out[:, 128:256] = block[64:128]
        last = jnp.concatenate([block[128 + 16 * j : 144 + 16 * j, 96:] for j in range(3)], axis=1)
        out[:, 256:] = jnp.concatenate([block[128:, :96], last], axis=0)

    def make_blocks(h, k):
        dz = order[k]
        z = zrow(dz)
        block = lax.dot_general(
            X[z, EDGE : EDGE + TOK, :], COT[h][...],
            (((0,), (0,)), ((), ())), preferred_element_type=F32,
        )
        for i in range(NY):
            packed(block[64 * i : 64 * i + 64], TERMS[h].at[z * NY + i])
        way, onward, back = turn(h, k)
        w.send(("far", h, k), TERMS[h].at[blk(dz, 2)], FAR[h].at[k], onward, "pack")
        w.send(("dir", h, k), TERMS[h].at[blk(dz, -way)], DIR[h].at[k], back, "pack")

    def total(*parts):
        acc = parts[0].astype(F32)
        for part in parts[1:]:
            acc = acc + part.astype(F32)
        return acc

    def pass_on(h, k):
        way, onward, back = turn(h, k)
        w.wait(("far", h, k), FAR[h].at[k], me, "pack")
        MID[h][k] = total(FAR[h][k], TERMS[h][blk(order[k], way)]).astype(BF16)
        w.send(("mid", h, k), MID[h].at[k], END[h].at[k], onward, "pack")

    def row_done(h, k):
        w.wait(("dir", h, k), DIR[h].at[k], me, "pack")
        w.wait(("mid", h, k), END[h].at[k], me, "pack")
        RED[h][k] = total(TERMS[h][blk(order[k], 0)], DIR[h][k], END[h][k]).astype(BF16)

    def start_of(h, way):
        return 8 if (h == "g") == (way == 1) else 7

    def row_at(way, d):
        return place[(way * d) % ZL]

    def sources(h, way, d):
        return [e for e in range(start_of(h, way), d, -1) if TREES[h][e] == d]

    def arrived(h, way, d):
        landing = LAND[h, way]
        for e in sources(h, way, d):
            w.wait((h, way, e), landing.at[e], me, "pack")
        return [landing[e] for e in sources(h, way, d)]

    def hop(h, way, d):
        k = row_at(way, d)
        source = RED[h].at[k]
        if sources(h, way, d):
            SUMS[h, way][d] = total(*arrived(h, way, d), RED[h][k]).astype(BF16)
            source = SUMS[h, way].at[d]
        w.send((h, way, d), source, LAND[h, way].at[d], dev(z=zg + way * (d - TREES[h][d])), "pack")

    def finish(h, out):
        parts = arrived(h, 1, 0) + arrived(h, -1, 0)
        unpacked(total(RED[h][place[0]], *parts) * factor, out)

    def input_terms(j):
        part = lax.dot_general(
            CG[...], WG[NY * j : NY * j + NY].reshape(FEAT, COLS),
            (((1,), (1,)), ((), ())), preferred_element_type=F32,
        ) + lax.dot_general(
            CV[...], WV[NY * j : NY * j + NY].reshape(FEAT, COLS),
            (((1,), (1,)), ((), ())), preferred_element_type=F32,
        )
        IP[NX * (j % 2) + j // 2] = part.astype(BF16)

    def input_swap():
        for i in range(NX):
            w.send(("ip", i), IP.at[NX * (1 - c) + i], IR.at[i], partner, "tile")

    def input_sums():
        for i in range(NX):
            w.wait(("ip", i), IR.at[i], me, "tile")
            IS[i] = total(IP[NX * c + i], IR[i]).astype(BF16)
        for dx in (1, 3, 2):
            w.send(("is", dx), IS.at[lax.rem(x + dx, NX)], ISR.at[dx - 1], dev(x=x + dx), "tile")

    results = []

    def put_out(source, target):
        copy = pltpu.make_async_copy(source, target, local_sems.at[6 + len(results)])
        copy.start()
        results.append(copy)

    def input_done():
        for dx in (1, 3, 2):
            w.wait(("is", dx), ISR.at[dx - 1], me, "tile")
        DIN[...] = total(IP[NX * c + x], IR[x], ISR[0], ISR[1], ISR[2]).astype(BF16)
        put_out(DIN, din_hbm)

    def taps_y():
        for dy in (1, 2, 3):
            w.send(("ty",), TY.at[y], TY.at[y], dev(y=y + dy), "taps")

    def taps_z():
        w.wait(("ty",), TY.at[pl.ds(0, 3)], me, "taps")
        TZ1[zo] = TY[0] + TY[1] + TY[2] + TY[3]
        for k in (1, 2, 3):
            w.send(("tz",), TZ1.at[zo], TZ1.at[zo], z_near(k), "taps")

    def taps_pair(stage):
        if stage == 0:
            w.wait(("tz",), TZ1.at[pl.ds(0, 3)], me, "taps")
            TB[0] = TZ1[0] + TZ1[1] + TZ1[2] + TZ1[3]
            w.send(("tb", 0), TB.at[0], TB.at[1], dev(z=zg + side), "taps")
        else:
            w.wait(("tb", 0), TB.at[1], me, "taps")
            TB[2] = TB[0] + TB[1]
            w.send(("tb", 1), TB.at[2], TB.at[3], dev(z=zg - side), "taps")

    def taps_spread():
        w.wait(("tb", 1), TB.at[3], me, "taps")
        TT[tp] = (TB[2] + TB[3]) * factor
        for k in range(1, 8):
            w.send(("tt",), TT.at[tp], TT.at[tp], tp_peer(k), "taps")

    def taps_done():
        w.wait(("tt",), TT.at[pl.ds(0, 7)], me, "taps")
        put_out(TT, tout_hbm)

    ahead, lag, spacing = AHEAD, 3, SPACING
    row_step = {item: t + lag for t, item in enumerate(ITEMS)}
    hop_step = {}
    for h, way in ends:
        for d in range(start_of(h, way), 0, -1):
            steps = [hop_step[h, way, e] + spacing + e - d - 1 for e in sources(h, way, d)]
            hop_step[h, way, d] = max([row_step[h, row_at(way, d)], *steps])
    items = ITEMS
    extra = {4: [taps_z], 7: [input_swap], 8: [lambda: taps_pair(0)], 11: [input_sums], 13: [lambda: taps_pair(1)],
             19: [taps_spread]}
    for j in range(2, 8):
        extra.setdefault(j - 1, []).insert(0, functools.partial(input_terms, j))
    for item in items[:ahead]:
        make_blocks(*item)
    back_all(KV, CV, v0, v1, v2)
    taps_own()
    taps_y()
    for j in range(2):
        input_terms(j)
    for step in range(max(hop_step.values()) + 1):
        if step < len(items):
            pass_on(*items[step])
        if step + ahead < len(items):
            make_blocks(*items[step + ahead])
        if 0 <= step - lag < len(items):
            row_done(*items[step - lag])
        for key in sorted(hop_step, key=hop_step.get):
            if hop_step[key] == step:
                hop(*key)
        for run in extra.get(step, ()):
            run()
    input_done()
    taps_done()
    finish("g", DG)
    put_out(DG, dg_hbm)
    finish("v", DV)
    put_out(DV, dv_hbm)
    w.drain(
        {
            "unit": lambda n: U.at[pl.ds(0, n)],
            "pack": lambda n: Q.at[pl.ds(0, n)],
            "tile": lambda n: XB.at[pl.ds(0, n)],
            "edge": lambda n: X.at[0, pl.ds(0, n * EDGE)],
            "og": lambda n: OG.at[pl.ds(0, n * EDGE)],
            "taps": lambda n: TS.at[pl.ds(0, n)],
        },
        me,
    )
    for copy in results:
        copy.wait()
    if len(w.index) > RECEIVES:
        raise ValueError(str(len(w.index)))


RECEIVES = 168


def finisher(din_ref, dg_ref, dv_ref, tt_ref, din_out, dg_out, dv_out, tg_out, tv_out):
    din_out[...] = din_ref[...]
    dg_out[...] = dg_ref[...]
    dv_out[...] = dv_ref[...]
    taps = jnp.concatenate([tt_ref[i] for i in range(8)], axis=1)
    tg_out[...] = taps[0:3]
    tv_out[...] = taps[3:6]


def shards(inputs, gate_proj, value_proj, gate_taps, value_taps, out_grad):
    unit = gate_proj.shape
    cols = unit[1]
    factor = float(TOK * NY * NZ) ** (-0.5)
    vm = pltpu.VMEM
    scratch = [
        vm((8, EXT, FEAT), BF16),
        vm((64, *unit), BF16),
        vm((216, PACK, 128), BF16),
        vm((4 * NX + 3, TOK, FEAT), BF16),
        vm((20, 8, cols), F32),
        vm(gate_taps.shape, F32),
        vm(gate_taps.shape, F32),
        vm((384, TOK), BF16),
        vm((EXT, cols), BF16),
        vm((EXT + 16, cols), F32),
        vm((EXT + 16, cols), F32),
        vm((EXT + 16, cols), F32),
        vm((EXT + 16, cols), F32),
        vm((TOK, cols), BF16),
        vm((TOK, cols), BF16),
        vm((TOK, FEAT), BF16),
        vm(unit, F32),
        vm(unit, F32),
        pltpu.SemaphoreType.DMA((6,)),
        pltpu.SemaphoreType.DMA((RECEIVES,)),
        pltpu.SemaphoreType.DMA((10,)),
    ]
    anywhere = pl.BlockSpec(memory_space=pl.ANY)
    vmem = pl.BlockSpec(memory_space=pltpu.VMEM)
    tile = jax.ShapeDtypeStruct((TOK, FEAT), BF16)
    grad = jax.ShapeDtypeStruct(unit, F32)
    tap = jax.ShapeDtypeStruct(gate_taps.shape, F32)
    sums = pl.pallas_call(
        functools.partial(kernel, factor),
        out_shape=(tile, grad, grad, jax.ShapeDtypeStruct((8, 8, cols), F32)),
        in_specs=[anywhere] * 6,
        out_specs=(anywhere,) * 4,
        scratch_shapes=scratch,
        compiler_params=pltpu.CompilerParams(
            collective_id=0, has_side_effects=True, vmem_limit_bytes=65000 * 1024
        ),
    )(inputs[0], gate_proj, value_proj, gate_taps, value_taps, jnp.swapaxes(out_grad[0], 0, 1))
    din, dg, dv, tg, tv = pl.pallas_call(
        finisher,
        out_shape=(tile, grad, grad, tap, tap),
        in_specs=[vmem] * 4,
        out_specs=(vmem,) * 5,
    )(*sums)
    return din[None], dg, dv, tg, tv


def solution(mesh):
    return jax.shard_map(
        shards,
        mesh=mesh,
        in_specs=(P("rep", "fs", "tp"), P("fs", "tp"), P("fs", "tp"), P(), P(), P("rep", "fs", "tp")),
        out_specs=(P("rep", "fs", "tp"), P("fs", "tp"), P("fs", "tp"), P(), P()),
        check_vma=False,
    )
```

```python
import functools

import jax
import jax.numpy as jnp
from jax import lax
from jax.experimental import pallas as pl
from jax.experimental.pallas import tpu as pltpu
from jax.sharding import PartitionSpec as P

MESH = pl.DeviceIdType.MESH
BF16 = jnp.bfloat16
F32 = jnp.float32

NX, NC, NY, NZ = 4, 2, 4, 16
ZL = 8
TOK = 384
COLS = 352
FEAT = 256
EDGE = 16
EXT = TOK + 2 * EDGE
PACK = 176


def right_reach(r):
    return 4 if r < 2 else 3


TREES = {
    "g": {8: 7, 7: 6, 6: 5, 5: 4, 4: 3, 3: 2, 2: 1, 1: 0},
    "v": {8: 7, 7: 6, 6: 5, 5: 4, 4: 0, 3: 2, 2: 1, 1: 0},
}
ITEMS = [(h, k) for h in "gv" for k in range(ZL)]
AHEAD, SPACING = 5, 3


class Wires:
    def __init__(self, send_sems, recv_sems):
        self.send_sems, self.recv_sems = send_sems, recv_sems
        self.index = {}
        self.count = dict.fromkeys(("unit", "pack", "tile", "edge", "og", "taps"), 0)

    def at(self, key):
        return self.index.setdefault(key, len(self.index))

    def copy(self, key, src, dst, to, kind):
        return pltpu.make_async_remote_copy(
            src_ref=src,
            dst_ref=dst,
            send_sem=self.send_sems.at[list(self.count).index(kind)],
            recv_sem=self.recv_sems.at[self.at(key)],
            device_id=to,
            device_id_type=MESH,
        )

    def send(self, key, src, dst, to, kind="unit", amount=1):
        self.count[kind] += amount
        self.copy(key, src, dst, to, kind).start()

    def wait(self, key, dst, to, kind="unit"):
        self.copy(key, dst, dst, to, kind).wait_recv()

    def drain(self, spans, to):
        for kind, span in spans.items():
            whole = span(int(self.count[kind]))
            self.copy(("drain",), whole, whole, to, kind).wait_send()


def kernel(
    factor,
    x_hbm, wg_hbm, wv_hbm, gt_hbm, vt_hbm, ogt_hbm,
    din_hbm, dg_hbm, dv_hbm, tout_hbm,
    X, U, Q, XB, TS, GT, VT, OGT, OG, PG, PV, KG, KV, CG, CV, DIN, DG, DV,
    send_sems, recv_sems, local_sems,
):
    def parts_of(pool, sizes):
        first, parts = 0, []
        for size in sizes:
            parts.append(pool.at[pl.ds(first, size)])
            first += size
        return parts

    WG, WV = parts_of(U, [32] * 2)
    GG, GV, *rest = parts_of(Q, [32] * 2 + [8] * 10 + [9] * 8)
    FAR, DIR, MID, END, RED = ({"g": rest[2 * i], "v": rest[2 * i + 1]} for i in range(5))
    ends = [(h, way) for h in "gv" for way in (1, -1)]
    LAND, SUMS = dict(zip(ends, rest[10:14])), dict(zip(ends, rest[14:18]))
    IP, IR, IS, ISR = parts_of(XB, [2 * NX, NX, NX, 3])
    TY, TZ1, TB, TT = parts_of(TS, [4, 4, 4, 8])
    rep, fs, tp = lax.axis_index("rep"), lax.axis_index("fs"), lax.axis_index("tp")
    zl, y = lax.div(fs, NY), lax.rem(fs, NY)
    x, c = lax.div(tp, NC), lax.rem(tp, NC)
    zg = rep * ZL + zl

    def dev(x=x, c=c, y=y, z=zg):
        z = lax.rem(z + NZ, NZ)
        return (
            lax.div(z, ZL),
            lax.rem(z, ZL) * NY + lax.rem(y + NY, NY),
            lax.rem(x + NX, NX) * NC + c,
        )

    def blk(dz, dy):
        return lax.rem(zl + dz + ZL, ZL) * NY + lax.rem(y + dy + NY, NY)

    def zrow(dz):
        return lax.rem(zl + dz + 2 * ZL, ZL)

    me = dev()
    right, left = dev(z=zg + 1), dev(z=zg - 1)
    up, down = dev(y=y + 1), dev(y=y - 1)
    partner = dev(c=1 - c)
    after_z = zg + lax.div(y + 1, NY)
    after = dev(y=y + 1, z=after_z)
    before_z = zg - 1 + lax.div(y + NY - 1, NY)
    before = dev(y=y - 1, z=before_z)

    def tp_peer(k):
        return (rep, fs, lax.rem(tp + k + 8, 8))

    zq, zo = lax.div(zg, 4), lax.rem(zg, 4)
    side = 4 * (1 - 2 * lax.rem(zq, 2))

    def z_near(k):
        return dev(z=zq * 4 + lax.rem(zo + k, 4))

    own = blk(0, 0)
    loads = [
        pltpu.make_async_copy(wg_hbm, WG.at[own], local_sems.at[0]),
        pltpu.make_async_copy(wv_hbm, WV.at[own], local_sems.at[1]),
        pltpu.make_async_copy(x_hbm, X.at[tp, pl.ds(EDGE, TOK)], local_sems.at[2]),
        pltpu.make_async_copy(ogt_hbm, OGT.at[pl.ds(0, COLS)], local_sems.at[3]),
        pltpu.make_async_copy(gt_hbm, GT, local_sems.at[4]),
        pltpu.make_async_copy(vt_hbm, VT, local_sems.at[5]),
    ]

    barrier = pltpu.get_barrier_semaphore()
    peers = [tp_peer(k) for k in range(1, 8)]
    peers += [dev(y=y + k) for k in (1, 2, 3)]
    peers += [right, left, after, before]
    for peer in peers:
        pl.semaphore_signal(barrier, inc=1, device_id=peer, device_id_type=MESH)
    for load in loads:
        load.start()
    pl.semaphore_wait(barrier, len(peers))

    w = Wires(send_sems, recv_sems)

    loads[0].wait()
    for dy in (1, 3, 2):
        w.send(("gy", dy), WG.at[own], WG.at[own], dev(y=y + dy))
    loads[1].wait()
    w.send(("vz", 1, 1), WV.at[own], WV.at[own], right)
    w.send(("vz", -1, 1), WV.at[own], WV.at[own], left)
    w.send(("gz", 0, 1, 1), WG.at[own], WG.at[own], right)
    w.send(("gz", 0, -1, 1), WG.at[own], WG.at[own], left)
    loads[2].wait()
    head, tail = X.at[tp, pl.ds(EDGE, EDGE)], X.at[tp, pl.ds(TOK, EDGE)]
    lo, hi = pl.ds(0, EDGE), pl.ds(TOK + EDGE, EDGE)
    w.send(("hx", 1), tail, X.at[tp, lo], after, "edge")
    w.send(("hx", -1), head, X.at[tp, hi], before, "edge")
    mine = X.at[tp, pl.ds(EDGE, TOK)]
    HALF = TOK // 2

    def half_of(dx, i):
        return X.at[lax.rem(x - dx + NX, NX) * NC + c, pl.ds(EDGE + HALF * i, HALF)]

    for i in (0, 1):
        for way, part in ((1, half_of(0, i)), (-1, half_of(0, 1 - i))):
            w.send(("x", way, i), part, part, dev(x=x + way), "tile", 0.5)
    w.send(("xp", 0), mine, mine, partner, "tile")
    w.send(("vy", 0, 1), WV.at[own], WV.at[own], up)
    w.send(("vy", 0, -1), WV.at[own], WV.at[own], down)

    def out_grad_rows():
        loads[3].wait()
        for i in range(3):
            for j in range(3):
                block = OGT[128 * i : 128 * i + 128, 128 * j : 128 * j + 128].astype(F32)
                cols = min(128, COLS - 128 * i)
                OG[EDGE + 128 * j : EDGE + 128 * j + 128, 128 * i : 128 * i + cols] = (
                    block.T[:, :cols].astype(BF16)
                )

    def rounded(value):
        return value.astype(BF16).astype(F32)

    def gate_chunk(z, first=False, last=False):
        part = jnp.dot(
            X[z],
            WG[pl.ds(z * NY, NY)].reshape(FEAT, COLS),
            preferred_element_type=F32,
        )
        if first:
            PG[8 : 8 + EXT] = part
        elif last:
            PG[8 : 8 + EXT] = rounded(PG[8 : 8 + EXT] + part)
        else:
            PG[8 : 8 + EXT] += part

    def value_chunk(z, first=False, last=False):
        part = jnp.dot(
            X[z],
            WV[pl.ds(z * NY, NY)].reshape(FEAT, COLS),
            preferred_element_type=F32,
        )
        if first:
            PV[8 : 8 + EXT] = part
        elif last:
            PV[8 : 8 + EXT] = rounded(PV[8 : 8 + EXT] + part)
        else:
            PV[8 : 8 + EXT] += part

    def x_first():
        for way in (1, -1):
            part = half_of(way, (1 - way) // 2)
            w.wait(("x", way, 0), part, me, "tile")
            w.send(("x2", way), part, part, dev(x=x + way), "tile", 0.5)

    def x_whole(dx):
        slot = X.at[lax.rem(x - dx + NX, NX) * NC + c, pl.ds(EDGE, TOK)]
        w.send(("xp", dx), slot, slot, partner, "tile")

    def x_near():
        for way in (1, -1):
            w.wait(("x", way, 1), half_of(way, (1 + way) // 2), me, "tile")
            x_whole(way)

    def x_far():
        for way in (1, -1):
            w.wait(("x2", way), half_of(2, (1 - way) // 2), me, "tile")
        x_whole(2)

    def xp_arrived(dx):
        slot = X.at[lax.rem(x - dx + NX, NX) * NC + 1 - c, pl.ds(EDGE, TOK)]
        w.wait(("xp", dx), slot, me, "tile")

    def edges_spread():
        w.wait(("hx", 1), X.at[tp, lo], me, "edge")
        w.wait(("hx", -1), X.at[tp, hi], me, "edge")
        for k in range(1, 8):
            w.send(("hl",), X.at[tp, lo], X.at[tp, lo], tp_peer(k), "edge")
            w.send(("hl",), X.at[tp, hi], X.at[tp, hi], tp_peer(k), "edge")

    def edges_done():
        w.wait(("hl",), X.at[0, pl.ds(0, 14 * EDGE)], me, "edge")

    def gate_y(dy):
        unit = WG.at[blk(0, -dy)]
        w.wait(("gy", dy), unit, me)
        w.send(("gz", 4 - dy, 1, 1), unit, unit, right)
        w.send(("gz", 4 - dy, -1, 1), unit, unit, left)

    def gate_z(r, d):
        for way, reach, to in ((1, right_reach(r), right), (-1, 7 - right_reach(r), left)):
            if d <= reach:
                unit = WG.at[blk(-way * d, r)]
                w.wait(("gz", r, way, d), unit, me)
                if d < reach:
                    w.send(("gz", r, way, d + 1), unit, unit, to)

    def value_z(d):
        for way, reach, to in ((1, 4, right), (-1, 3, left)):
            if d <= reach:
                dz = -way * d
                unit = WV.at[blk(dz, 0)]
                w.wait(("vz", way, d), unit, me)
                if d < reach:
                    w.send(("vz", way, d + 1), unit, unit, to)
                w.send(("vy", dz, 1), unit, unit, up)
                w.send(("vy", dz, -1), unit, unit, down)
                if d == 4:
                    w.send(("vf", dz), unit, unit, dev(y=y + 2))

    def value_y(dz):
        from_down, from_up = WV.at[blk(dz, -1)], WV.at[blk(dz, 1)]
        w.wait(("vy", dz, 1), from_down, me)
        if dz % 2 == 0 and dz != -4:
            w.send(("vf", dz), from_down, from_down, up)
        w.wait(("vy", dz, -1), from_up, me)
        if dz % 2 == 1:
            w.send(("vf", dz), from_up, from_up, down)

    def value_row(dz, first=False, last=False):
        w.wait(("vf", dz), WV.at[blk(dz, 2)], me)
        value_chunk(zrow(dz), first, last)

    value_z(1)
    gate_y(1)
    gate_y(3)
    gate_y(2)
    gate_z(0, 1)
    value_y(0)
    value_z(2)
    gate_z(3, 1)
    x_first()
    gate_z(1, 1)
    edges_spread()
    gate_z(2, 1)
    value_y(1)
    value_y(-1)
    x_near()
    out_grad_rows()
    gate_z(0, 2)
    value_z(3)
    x_far()
    w.send(("og", 1), OG.at[pl.ds(TOK, EDGE)], OG.at[lo], after, "og")
    w.send(("og", -1), OG.at[pl.ds(EDGE, EDGE)], OG.at[hi], before, "og")
    gate_z(3, 2)
    value_y(2)
    value_y(-2)
    gate_z(1, 2)
    gate_z(2, 2)
    gate_z(0, 3)
    value_z(4)
    for dx in (0, 1, -1, 2):
        xp_arrived(dx)
    edges_done()
    gate_chunk(zrow(0), first=True)
    gate_chunk(zrow(1))
    gate_z(3, 3)
    gate_chunk(zrow(-1))
    value_y(3)
    value_y(-3)
    gate_z(1, 3)
    value_row(0, first=True)
    gate_chunk(zrow(2))
    gate_z(2, 3)
    gate_chunk(zrow(-2))
    value_row(1)
    gate_z(0, 4)
    value_row(-1)
    value_row(2)
    gate_chunk(zrow(3))
    gate_z(3, 4)
    value_row(-2)
    gate_chunk(zrow(-3))
    value_y(-4)
    value_row(3)
    gate_z(1, 4)
    value_row(-3)
    value_row(-4, last=True)
    gate_z(2, 4)
    gate_chunk(zrow(4), last=True)
    w.wait(("og", 1), OG.at[lo], me, "og")
    w.wait(("og", -1), OG.at[hi], me, "og")

    not_first, not_last = fs > 0, fs < NY * ZL - 1
    for ref in (PG, PV):
        ref[8 : 8 + EDGE] = jnp.where(not_first, ref[8 : 8 + EDGE], 0.0)
        ref[8 + EDGE + TOK : 8 + EXT] = jnp.where(not_last, ref[8 + EDGE + TOK : 8 + EXT], 0.0)
    OG[:EDGE] = jnp.where(not_first, OG[:EDGE].astype(F32), 0.0).astype(BF16)
    OG[EDGE + TOK :] = jnp.where(not_last, OG[EDGE + TOK :].astype(F32), 0.0).astype(BF16)

    loads[4].wait()
    loads[5].wait()
    taps = jnp.concatenate([GT[...], VT[...], jnp.zeros((2, 8 * COLS), F32)], axis=0)
    taps = pltpu.roll(taps, lax.rem((8 - tp) * COLS, 8 * COLS), axis=1)[:, :COLS]
    g0, g1, g2, v0, v1, v2 = (taps[k : k + 1] for k in range(6))

    def cot_rows(i):
        base = pl.multiple_of(i * 16, 16)
        gate = PG[pl.ds(base, 32)]
        value = PV[pl.ds(base, 32)]
        gm, gz, gp = gate[7:23], gate[8:24], gate[9:25]
        vm, vz, vp = value[7:23], value[8:24], value[9:25]
        gate_mix = g0 * gm + g1 * gz + g2 * gp
        value_mix = v0 * vm + v1 * vz + v2 * vp
        grad = OG[pl.ds(base, 16)].astype(F32)
        s = jax.nn.sigmoid(gate_mix)
        gate_cot = grad * value_mix * (s * (1.0 + gate_mix * (1.0 - s)))
        value_cot = grad * (gate_mix * s)
        KG[pl.ds(base + 8, 16)] = gate_cot
        KV[pl.ds(base + 8, 16)] = value_cot

    def all_cots(i, carry):
        cot_rows(i)
        return carry

    lax.fori_loop(0, TOK // 16 + 2, all_cots, 0)

    def tap_rows(i, sums):
        base = pl.multiple_of(i * 16, 16)
        terms = []
        for pre, cot in ((PG, KG), (PV, KV)):
            rows, cots = pre[pl.ds(base, 32)], cot[pl.ds(base + 8, 16)]
            terms += [(rows[7 + k : 23 + k] * cots).reshape(2, 8, COLS).sum(axis=0) for k in range(3)]
        return tuple(a + b for a, b in zip(sums, terms))

    def taps_own():
        sums = lax.fori_loop(1, TOK // 16 + 1, tap_rows, (jnp.zeros((8, COLS), F32),) * 6)
        rows = [jnp.sum(part, axis=0, keepdims=True) for part in sums]
        TY[y] = jnp.concatenate(rows + [jnp.zeros((2, COLS), F32)], axis=0)

    def back_all(source, target, t0, t1, t2):
        def back_rows(i, carry):
            cot = source[pl.ds(pl.multiple_of(i * 16, 16), 32)]
            out = pl.ds(pl.multiple_of(i * 16 - 16, 16), 16)
            target[out] = (t0 * cot[9:25] + t1 * cot[8:24] + t2 * cot[7:23]).astype(BF16)
            return carry

        lax.fori_loop(1, TOK // 16 + 1, back_rows, 0)

    back_all(KG, CG, g0, g1, g2)

    order = (0, 1, -1, 2, -2, 3, -3, 4)
    place = {dz % ZL: k for k, dz in enumerate(order)}
    COT, TERMS = {"g": CG, "v": CV}, {"g": GG, "v": GV}

    def turn(h, k):
        return (1, up, down) if (k % 2 == 0) == (h == "g") else (-1, down, up)

    def packed(block, out):
        out[0:64] = block[:, :128].astype(BF16)
        out[64:128] = block[:, 128:256].astype(BF16)
        rest = block[:, 256:]
        for j in range(3):
            row = jnp.concatenate([rest[16 * j : 16 * j + 16], rest[48:64, 32 * j : 32 * j + 32]], axis=1)
            out[128 + 16 * j : 144 + 16 * j] = row.astype(BF16)

    def unpacked(block, out):
        out[:, :128] = block[0:64]
        out[:, 128:256] = block[64:128]
        last = jnp.concatenate([block[128 + 16 * j : 144 + 16 * j, 96:] for j in range(3)], axis=1)
        out[:, 256:] = jnp.concatenate([block[128:, :96], last], axis=0)

    def make_blocks(h, k):
        dz = order[k]
        z = zrow(dz)
        block = lax.dot_general(
            X[z, EDGE : EDGE + TOK, :], COT[h][...],
            (((0,), (0,)), ((), ())), preferred_element_type=F32,
        )
        for i in range(NY):
            packed(block[64 * i : 64 * i + 64], TERMS[h].at[z * NY + i])
        way, onward, back = turn(h, k)
        w.send(("far", h, k), TERMS[h].at[blk(dz, 2)], FAR[h].at[k], onward, "pack")
        w.send(("dir", h, k), TERMS[h].at[blk(dz, -way)], DIR[h].at[k], back, "pack")

    def total(*parts):
        acc = parts[0].astype(F32)
        for part in parts[1:]:
            acc = acc + part.astype(F32)
        return acc

    def pass_on(h, k):
        way, onward, back = turn(h, k)
        w.wait(("far", h, k), FAR[h].at[k], me, "pack")
        MID[h][k] = total(FAR[h][k], TERMS[h][blk(order[k], way)]).astype(BF16)
        w.send(("mid", h, k), MID[h].at[k], END[h].at[k], onward, "pack")

    def row_done(h, k):
        w.wait(("dir", h, k), DIR[h].at[k], me, "pack")
        w.wait(("mid", h, k), END[h].at[k], me, "pack")
        RED[h][k] = total(TERMS[h][blk(order[k], 0)], DIR[h][k], END[h][k]).astype(BF16)

    def start_of(h, way):
        return 8 if (h == "g") == (way == 1) else 7

    def row_at(way, d):
        return place[(way * d) % ZL]

    def sources(h, way, d):
        return [e for e in range(start_of(h, way), d, -1) if TREES[h][e] == d]

    def arrived(h, way, d):
        landing = LAND[h, way]
        for e in sources(h, way, d):
            w.wait((h, way, e), landing.at[e], me, "pack")
        return [landing[e] for e in sources(h, way, d)]

    def hop(h, way, d):
        k = row_at(way, d)
        source = RED[h].at[k]
        if sources(h, way, d):
            SUMS[h, way][d] = total(*arrived(h, way, d), RED[h][k]).astype(BF16)
            source = SUMS[h, way].at[d]
        w.send((h, way, d), source, LAND[h, way].at[d], dev(z=zg + way * (d - TREES[h][d])), "pack")

    def finish(h, out):
        parts = arrived(h, 1, 0) + arrived(h, -1, 0)
        unpacked(total(RED[h][place[0]], *parts) * factor, out)

    def input_terms(j):
        part = lax.dot_general(
            CG[...], WG[NY * j : NY * j + NY].reshape(FEAT, COLS),
            (((1,), (1,)), ((), ())), preferred_element_type=F32,
        ) + lax.dot_general(
            CV[...], WV[NY * j : NY * j + NY].reshape(FEAT, COLS),
            (((1,), (1,)), ((), ())), preferred_element_type=F32,
        )
        IP[NX * (j % 2) + j // 2] = part.astype(BF16)

    def input_swap():
        for i in range(NX):
            w.send(("ip", i), IP.at[NX * (1 - c) + i], IR.at[i], partner, "tile")

    def input_sums():
        for i in range(NX):
            w.wait(("ip", i), IR.at[i], me, "tile")
            IS[i] = total(IP[NX * c + i], IR[i]).astype(BF16)
        for dx in (1, 3, 2):
            w.send(("is", dx), IS.at[lax.rem(x + dx, NX)], ISR.at[dx - 1], dev(x=x + dx), "tile")

    results = []

    def put_out(source, target):
        copy = pltpu.make_async_copy(source, target, local_sems.at[6 + len(results)])
        copy.start()
        results.append(copy)

    def input_done():
        for dx in (1, 3, 2):
            w.wait(("is", dx), ISR.at[dx - 1], me, "tile")
        DIN[...] = total(IP[NX * c + x], IR[x], ISR[0], ISR[1], ISR[2]).astype(BF16)
        put_out(DIN, din_hbm)

    def taps_y():
        for dy in (1, 2, 3):
            w.send(("ty",), TY.at[y], TY.at[y], dev(y=y + dy), "taps")

    def taps_z():
        w.wait(("ty",), TY.at[pl.ds(0, 3)], me, "taps")
        TZ1[zo] = TY[0] + TY[1] + TY[2] + TY[3]
        for k in (1, 2, 3):
            w.send(("tz",), TZ1.at[zo], TZ1.at[zo], z_near(k), "taps")

    def taps_pair(stage):
        if stage == 0:
            w.wait(("tz",), TZ1.at[pl.ds(0, 3)], me, "taps")
            TB[0] = TZ1[0] + TZ1[1] + TZ1[2] + TZ1[3]
            w.send(("tb", 0), TB.at[0], TB.at[1], dev(z=zg + side), "taps")
        else:
            w.wait(("tb", 0), TB.at[1], me, "taps")
            TB[2] = TB[0] + TB[1]
            w.send(("tb", 1), TB.at[2], TB.at[3], dev(z=zg - side), "taps")

    def taps_spread():
        w.wait(("tb", 1), TB.at[3], me, "taps")
        TT[tp] = (TB[2] + TB[3]) * factor
        for k in range(1, 8):
            w.send(("tt",), TT.at[tp], TT.at[tp], tp_peer(k), "taps")

    def taps_done():
        w.wait(("tt",), TT.at[pl.ds(0, 7)], me, "taps")
        put_out(TT, tout_hbm)

    ahead, lag, spacing = AHEAD, 3, SPACING
    row_step = {item: t + lag for t, item in enumerate(ITEMS)}
    hop_step = {}
    for h, way in ends:
        for d in range(start_of(h, way), 0, -1):
            steps = [hop_step[h, way, e] + spacing + e - d - 1 for e in sources(h, way, d)]
            hop_step[h, way, d] = max([row_step[h, row_at(way, d)], *steps])
    items = ITEMS
    extra = {4: [taps_z], 7: [input_swap], 8: [lambda: taps_pair(0)], 11: [input_sums], 13: [lambda: taps_pair(1)],
             19: [taps_spread]}
    for j in range(2, 8):
        extra.setdefault(j - 1, []).insert(0, functools.partial(input_terms, j))
    for item in items[:ahead]:
        make_blocks(*item)
    back_all(KV, CV, v0, v1, v2)
    taps_own()
    taps_y()
    for j in range(2):
        input_terms(j)
    for step in range(max(hop_step.values()) + 1):
        if step < len(items):
            pass_on(*items[step])
        if step + ahead < len(items):
            make_blocks(*items[step + ahead])
        if 0 <= step - lag < len(items):
            row_done(*items[step - lag])
        for key in sorted(hop_step, key=hop_step.get):
            if hop_step[key] == step:
                hop(*key)
        for run in extra.get(step, ()):
            run()
    input_done()
    taps_done()
    finish("g", DG)
    put_out(DG, dg_hbm)
    finish("v", DV)
    put_out(DV, dv_hbm)
    w.drain(
        {
            "unit": lambda n: U.at[pl.ds(0, n)],
            "pack": lambda n: Q.at[pl.ds(0, n)],
            "tile": lambda n: XB.at[pl.ds(0, n)],
            "edge": lambda n: X.at[0, pl.ds(0, n * EDGE)],
            "og": lambda n: OG.at[pl.ds(0, n * EDGE)],
            "taps": lambda n: TS.at[pl.ds(0, n)],
        },
        me,
    )
    for copy in results:
        copy.wait()
    if len(w.index) > RECEIVES:
        raise ValueError(str(len(w.index)))


RECEIVES = 168


def finisher(din_ref, dg_ref, dv_ref, tt_ref, din_out, dg_out, dv_out, tg_out, tv_out):
    din_out[...] = din_ref[...]
    dg_out[...] = dg_ref[...]
    dv_out[...] = dv_ref[...]
    taps = jnp.concatenate([tt_ref[i] for i in range(8)], axis=1)
    tg_out[...] = taps[0:3]
    tv_out[...] = taps[3:6]


def shards(inputs, gate_proj, value_proj, gate_taps, value_taps, out_grad):
    unit = gate_proj.shape
    cols = unit[1]
    factor = float(TOK * NY * NZ) ** (-0.5)
    vm = pltpu.VMEM
    scratch = [
        vm((8, EXT, FEAT), BF16),
        vm((64, *unit), BF16),
        vm((216, PACK, 128), BF16),
        vm((4 * NX + 3, TOK, FEAT), BF16),
        vm((20, 8, cols), F32),
        vm(gate_taps.shape, F32),
        vm(gate_taps.shape, F32),
        vm((384, TOK), BF16),
        vm((EXT, cols), BF16),
        vm((EXT + 16, cols), F32),
        vm((EXT + 16, cols), F32),
        vm((EXT + 16, cols), F32),
        vm((EXT + 16, cols), F32),
        vm((TOK, cols), BF16),
        vm((TOK, cols), BF16),
        vm((TOK, FEAT), BF16),
        vm(unit, F32),
        vm(unit, F32),
        pltpu.SemaphoreType.DMA((6,)),
        pltpu.SemaphoreType.DMA((RECEIVES,)),
        pltpu.SemaphoreType.DMA((10,)),
    ]
    anywhere = pl.BlockSpec(memory_space=pl.ANY)
    vmem = pl.BlockSpec(memory_space=pltpu.VMEM)
    tile = jax.ShapeDtypeStruct((TOK, FEAT), BF16)
    grad = jax.ShapeDtypeStruct(unit, F32)
    tap = jax.ShapeDtypeStruct(gate_taps.shape, F32)
    sums = pl.pallas_call(
        functools.partial(kernel, factor),
        out_shape=(tile, grad, grad, jax.ShapeDtypeStruct((8, 8, cols), F32)),
        in_specs=[anywhere] * 6,
        out_specs=(anywhere,) * 4,
        scratch_shapes=scratch,
        compiler_params=pltpu.CompilerParams(
            collective_id=0, has_side_effects=True, vmem_limit_bytes=65000 * 1024
        ),
    )(inputs[0], gate_proj, value_proj, gate_taps, value_taps, jnp.swapaxes(out_grad[0], 0, 1))
    din, dg, dv, tg, tv = pl.pallas_call(
        finisher,
        out_shape=(tile, grad, grad, tap, tap),
        in_specs=[vmem] * 4,
        out_specs=(vmem,) * 5,
    )(*sums)
    return din[None], dg, dv, tg, tv


def solution(mesh):
    return jax.shard_map(
        shards,
        mesh=mesh,
        in_specs=(P("rep", "fs", "tp"), P("fs", "tp"), P("fs", "tp"), P(), P(), P("rep", "fs", "tp")),
        out_specs=(P("rep", "fs", "tp"), P("fs", "tp"), P("fs", "tp"), P(), P()),
        check_vma=False,
    )
```
